32 devices in a mesh: kv: 16 (over z, x, core), tp: 2 (over y).
Axes of the slice: x: 2, y: 2, z: 4, core: 2. Of those that a mesh axis runs over, the one named last changes fastest.
Arguments:
- hidden_in: bfloat16 [4, 1024, 2048], P(None, 'kv'), may hold values from -84 to 84
- w_query: bfloat16 [2048, 1024], P(None, 'tp'), may hold values from -0.125 to 0.125
- w_cmp_key: bfloat16 [2048, 256], P(None, 'tp'), may hold values from -0.125 to 0.125
- w_cmp_value: bfloat16 [2048, 256], P(None, 'tp'), may hold values from -0.8838835 to 0.8838835
- w_sel_key: bfloat16 [2048, 256], P(None, 'tp'), may hold values from -0.125 to 0.125
- w_sel_value: bfloat16 [2048, 256], P(None, 'tp'), may hold values from -0.8838835 to 0.8838835
- w_gate: bfloat16 [2048, 2, 16], replicated, may hold values from -0.125 to 0.125
- cmp_key_in: bfloat16 [2048, 128], replicated, may hold values from -0.125 to 0.125
- cmp_key_out: bfloat16 [128, 64], replicated, may hold values from -0.5 to 0.5
- cmp_value_in: bfloat16 [2048, 128], replicated, may hold values from -0.125 to 0.125
- cmp_value_out: bfloat16 [128, 64], replicated, may hold values from -0.5 to 0.5
- out_gain: float32 [1024], replicated, may hold values from 0.1 to 1.9
- w_out: bfloat16 [1024, 2048], replicated, may hold values from -0.1875 to 0.1875
- seq_lengths: int32 [4], replicated, may hold values from 1 to 1024, 1638 in all
- chosen: int32 [4, 16, 4, 16], P(None, 'kv', 'tp'), may hold values from -1 to 15, as said below
Outputs:
- attended: bfloat16 [4, 1024, 2048], P(None, 'kv', 'tp')
The draws below stay inside these ranges and needn't reach their ends.
Inputs may be any that keep to these rules, and one draw needn't show every extreme that they name: chosen[s, b, g, 0] is b itself. Every other entry is -1 or a block index below b, and the entries of one list that are not -1 are distinct. For each block index and key group, the entries after the first slot that name that index all lie in the lists of a single sequence.
All inputs are finite; a program needn't handle non-finite values.
Results may differ from the reference program's by a relative error of at most 0.012.
The reference program's roundings to bfloat16 on the way count: a program that leaves them out, or rounds other values in their place, can miss the bound.
Values may be sent and summed in bfloat16 or wider, within the bound.
A program may use at most 64 MiB of HBM per device.

```python
import math
import jax
import jax.numpy as jnp
import numpy as np
from jax import lax

D = 2048
HEADS = 16
GROUPS = 4
HEAD_DIM = 64
CMP_STRIDE = 16
CMP_BLOCK = 32
CMP_HIDDEN = 128
SLC_BLOCK = 64
TOPK = 16
SEQS = 4
SEQ_LEN = 1024
BLOCKS = 16


def rising_columns(key):
    base = jnp.clip(jax.random.normal(key, (D, GROUPS * HEAD_DIM), jnp.float32), -4.0, 4.0) * D ** (-0.5)
    group = (jnp.arange(GROUPS * HEAD_DIM) // HEAD_DIM).astype(jnp.float32)
    factor = 3.0 ** (group / (GROUPS - 1))
    return (base * factor[None, :]).astype(jnp.bfloat16)


def draw_w_cmp_value(key, part):
    return rising_columns(jax.random.fold_in(key, 31))


def draw_w_sel_value(key, part):
    return rising_columns(jax.random.fold_in(key, 32))


def draw_hidden_in(key, part):
    shape = (SEQS, SEQ_LEN, D)
    base = jnp.clip(jax.random.normal(jax.random.fold_in(key, 41), shape, jnp.float32), -6.0, 6.0)
    return base.astype(jnp.bfloat16)


def draw_chosen(key, part):
    block_list = SEQ_LEN // SLC_BLOCK
    owner_seq = jax.random.randint(jax.random.fold_in(key, 51), (block_list, GROUPS), 0, SEQS)
    heat = jax.random.randint(jax.random.fold_in(key, 52), (block_list,), 0, 4)
    random_jitter = jax.random.randint(jax.random.fold_in(key, 53), (SEQS, block_list, GROUPS, block_list), 0, 4096)
    local_block = jnp.arange(block_list)[None, :, None, None]
    remote_block = jnp.arange(block_list)[None, None, None, :]
    seq_ids = jnp.arange(SEQS)[:, None, None, None]
    owner = jnp.transpose(owner_seq)[None, None, :, :]
    valid = (remote_block < local_block) & (owner == seq_ids)
    closest_block = jnp.max(jnp.where(valid, remote_block, -1), axis=-1, keepdims=True)
    extra_score = jnp.where(remote_block == closest_block, 1 << 20, 0) + jnp.where(remote_block == local_block - block_list // 2, 1 << 19, 0)
    weight_matrix = heat * heat * 4096
    block_score = (weight_matrix[None, None, None, :] + random_jitter + extra_score) * block_list + remote_block
    block_score = jnp.where(valid, block_score, -1 - remote_block)
    values, indices = lax.top_k(block_score, TOPK - 1)
    picked = jnp.where(values >= 0, indices, -1)
    own = jnp.broadcast_to(local_block, (SEQS, block_list, GROUPS, 1))
    return jnp.concatenate([own, picked], axis=-1).astype(jnp.int32)


def levels(rng, extent, pieces, low, top_value):
    def one(axis_at, blocks):
        draws = jax.random.uniform(jax.random.fold_in(jax.random.fold_in(rng, 6), axis_at), (blocks,), jnp.float32, low / len(pieces), top_value / len(pieces))
        return jnp.repeat(jnp.exp(draws), extent[axis_at] // blocks).reshape((-1,) + (1,) * (len(extent) - axis_at - 1))

    factor_of = one(*pieces[0])
    for cut in pieces[1:]:
        factor_of = factor_of * one(*cut)
    return factor_of


def length_profile(amount, total, limit, skew):
    loads = [(1 << 20) // math.isqrt(rank ** skew) + 1 for rank in range(2, amount + 1)]
    rest, holding = total - limit - (amount - 1), [1] * (amount - 1)
    while rest > 0:
        movable = [i for i in range(amount - 1) if holding[i] < limit]
        pool, left = sum([loads[i] for i in movable]), rest
        for i in movable:
            addition = min(limit - holding[i], max(1, left * loads[i] // pool), rest)
            holding[i] = holding[i] + addition
            rest = rest - addition
    return np.array([limit] + holding)


def ragged(own_key, amount, total, limit, slope):
    if amount == 2:
        one = jax.random.randint(own_key, (), max(1, total - limit), min(limit, total - 1) + 1)
        return jnp.stack([one, total - one])
    lengths = jnp.asarray(length_profile(amount, total, limit, slope), jnp.int32)
    couples = (amount - 1) // 2
    donor, taker = lengths[1:1 + 2 * couples:2], lengths[2:2 + 2 * couples:2]
    margin = jnp.minimum(donor - 1, limit - taker)
    moved = jax.random.randint(jax.random.fold_in(own_key, 1), (couples,), 0, 1 << 20) % (margin + 1)
    lengths = lengths.at[1:1 + 2 * couples:2].set(donor - moved).at[2:2 + 2 * couples:2].set(taker + moved)
    return lengths[jax.random.permutation(jax.random.fold_in(own_key, 2), amount)]


def normal_values(own_key, extent, deviation, most, shards=(), kind=jnp.bfloat16):
    values = jax.random.normal(own_key, extent, jnp.float32) * deviation
    if len(shards) > 0:
        values = levels(own_key, extent, shards, -0.22, 0.18) * values
    return jnp.clip(values, min=-most, max=most).astype(kind)


def setup_inputs(seed: int = 0) -> dict:
    splits = jax.random.split(jax.random.key(seed), 16)
    hidden_in = draw_hidden_in(jax.random.fold_in(splits[15], 71), 0)
    w_query = normal_values(splits[1], (D, HEADS * HEAD_DIM), D ** -0.5, 0.125, ((1, 2),))
    w_cmp_key = normal_values(splits[2], (D, GROUPS * HEAD_DIM), D ** -0.5, 0.125, ((1, 2),))
    w_cmp_value = draw_w_cmp_value(jax.random.fold_in(splits[15], 71), 0)
    w_sel_key = normal_values(splits[4], (D, GROUPS * HEAD_DIM), D ** -0.5, 0.125, ((1, 2),))
    w_sel_value = draw_w_sel_value(jax.random.fold_in(splits[15], 71), 0)
    w_gate = normal_values(splits[6], (D, 2, HEADS), D ** -0.5, 0.125)
    cmp_key_in = normal_values(splits[7], (CMP_BLOCK * HEAD_DIM, CMP_HIDDEN), (CMP_BLOCK * HEAD_DIM) ** -0.5, 0.125)
    cmp_key_out = normal_values(splits[8], (CMP_HIDDEN, HEAD_DIM), CMP_HIDDEN ** -0.5, 0.5)
    cmp_value_in = normal_values(splits[9], (CMP_BLOCK * HEAD_DIM, CMP_HIDDEN), (CMP_BLOCK * HEAD_DIM) ** -0.5, 0.125)
    cmp_value_out = normal_values(splits[10], (CMP_HIDDEN, HEAD_DIM), CMP_HIDDEN ** -0.5, 0.5)
    out_gain = jnp.clip(1.0 + 0.18 * jax.random.normal(splits[11], (HEADS * HEAD_DIM,), jnp.float32), 0.1, 1.9)
    w_out = normal_values(splits[12], (HEADS * HEAD_DIM, D), (HEADS * HEAD_DIM) ** -0.5, 0.1875)
    seq_lengths = ragged(splits[13], SEQS, SEQ_LEN + (SEQS - 1) * SEQ_LEN // 5, SEQ_LEN, 2).astype(jnp.int32)
    chosen = draw_chosen(jax.random.fold_in(splits[15], 71), 0)
    return {"hidden_in": hidden_in, "w_query": w_query, "w_cmp_key": w_cmp_key, "w_cmp_value": w_cmp_value, "w_sel_key": w_sel_key, "w_sel_value": w_sel_value, "w_gate": w_gate, "cmp_key_in": cmp_key_in, "cmp_key_out": cmp_key_out, "cmp_value_in": cmp_value_in, "cmp_value_out": cmp_value_out, "out_gain": out_gain, "w_out": w_out, "seq_lengths": seq_lengths, "chosen": chosen}


theta_base = 500000.0
norm_eps = 1e-06

def rotate(values, positions):
    width = values.shape[-1]
    half = width // 2
    inverse = jnp.exp(-jnp.log(jnp.float32(theta_base)) * jnp.arange(0, width, 2).astype(jnp.float32) / width)
    angle = positions.astype(jnp.float32)[:, None] * inverse[None, :]
    cosine = jnp.cos(angle)[:, None, :]
    sine = jnp.sin(angle)[:, None, :]
    first = values[..., :half]
    second = values[..., half:]
    return jnp.concatenate([first * cosine - second * sine, second * cosine + first * sine], axis=-1)

def masked_weights(scores, valid):
    top = lax.optimization_barrier(jnp.max(jnp.where(valid, scores, -1e+30), axis=-1, keepdims=True))
    expd = jnp.where(valid, jnp.exp(scores - top), 0.0)
    total = lax.optimization_barrier(jnp.sum(expd, axis=-1, keepdims=True))
    return (expd / jnp.maximum(total, 1.0)).astype(jnp.bfloat16)

def compress(raw, weight_in, weight_out):
    length, groups, width = raw.shape
    block_count = length // SLC_BLOCK
    per_block = SLC_BLOCK // CMP_STRIDE
    blocked = raw.reshape(block_count, SLC_BLOCK, groups, width)
    padded = jnp.concatenate([jnp.zeros((block_count, CMP_STRIDE, groups, width), raw.dtype), blocked], axis=1)
    count = block_count * per_block
    front = padded[:, :SLC_BLOCK].reshape(count, CMP_STRIDE, groups, width)
    back = padded[:, CMP_STRIDE:].reshape(count, CMP_STRIDE, groups, width)
    window = jnp.concatenate([front, back], axis=1).transpose(0, 2, 1, 3).reshape(count * groups, CMP_BLOCK * width)
    inner = jax.nn.gelu(jnp.dot(window, weight_in, preferred_element_type=jnp.float32)).astype(jnp.bfloat16)
    return jnp.dot(inner, weight_out, preferred_element_type=jnp.float32).reshape(count, groups, width)

def reference(hidden_in, w_query, w_cmp_key, w_cmp_value, w_sel_key, w_sel_value, w_gate, cmp_key_in, cmp_key_out, cmp_value_in, cmp_value_out, out_gain, w_out, seq_lengths, chosen):
    count = SEQ_LEN // CMP_STRIDE
    per_group = HEADS // GROUPS
    scale = HEAD_DIM ** (-0.5)
    entry = jnp.arange(count).astype(jnp.int32)
    ends = entry * CMP_STRIDE + CMP_STRIDE - 1

    def one_sequence(args):
        tokens, length, picks = args
        positions = jnp.arange(SEQ_LEN).astype(jnp.int32)

        def project(weight_matrix, heads):
            return jnp.dot(tokens, weight_matrix, preferred_element_type=jnp.float32).reshape(SEQ_LEN, heads, HEAD_DIM)
        queries = rotate(project(w_query, HEADS), positions).astype(jnp.bfloat16)
        sel_keys = rotate(project(w_sel_key, GROUPS), positions).astype(jnp.bfloat16)
        sel_values = project(w_sel_value, GROUPS).astype(jnp.bfloat16)
        raw_keys = project(w_cmp_key, GROUPS).astype(jnp.bfloat16)
        raw_values = project(w_cmp_value, GROUPS).astype(jnp.bfloat16)
        cmp_keys = rotate(compress(raw_keys, cmp_key_in, cmp_key_out), ends).astype(jnp.bfloat16)
        cmp_values = compress(raw_values, cmp_value_in, cmp_value_out).astype(jnp.bfloat16)
        gate_logits = jnp.dot(tokens, w_gate.reshape(D, 2 * HEADS), preferred_element_type=jnp.float32)
        gates = jax.nn.sigmoid(gate_logits).reshape(SEQ_LEN, 2, HEADS)
        cmp_key_wide = cmp_keys.astype(jnp.float32)
        cmp_value_wide = cmp_values.astype(jnp.float32)
        sel_key_wide = sel_keys.astype(jnp.float32)
        sel_value_wide = sel_values.astype(jnp.float32)
        group_ids = jnp.arange(GROUPS).astype(jnp.int32)[:, None]

        def one_block(index):
            index = index.astype(jnp.int32)
            start = index * SLC_BLOCK
            block_q = lax.dynamic_slice_in_dim(queries, start, SLC_BLOCK, 0).astype(jnp.float32)
            block_q = block_q.reshape(SLC_BLOCK, GROUPS, per_group, HEAD_DIM)
            query_pos = start + jnp.arange(SLC_BLOCK).astype(jnp.int32)
            scores = jnp.einsum('qghd,egd->ghqe', block_q, cmp_key_wide) * scale
            valid = ((entry >= 1)[None, :] & (ends[None, :] <= query_pos[:, None]))[None, None]
            weights = masked_weights(scores, valid)
            cmp_out = jnp.einsum('ghqe,egd->qghd', weights.astype(jnp.float32), cmp_value_wide)
            lists = lax.dynamic_index_in_dim(picks, index, axis=0, keepdims=False)
            safe = jnp.maximum(lists, 0)
            token = safe[:, :, None] * SLC_BLOCK + jnp.arange(SLC_BLOCK).astype(jnp.int32)[None, None, :]
            token = token.reshape(GROUPS, TOPK * SLC_BLOCK)
            keys = sel_key_wide[token, group_ids]
            values = sel_value_wide[token, group_ids]
            live = jnp.repeat(lists >= 0, SLC_BLOCK, axis=1)
            valid_s = (live[:, None, :] & (token[:, None, :] <= query_pos[None, :, None]))[:, None]
            scores_s = jnp.einsum('qghd,gmd->ghqm', block_q, keys) * scale
            weights_s = masked_weights(scores_s, valid_s)
            sel_out = jnp.einsum('ghqm,gmd->qghd', weights_s.astype(jnp.float32), values)
            block_gates = lax.dynamic_slice_in_dim(gates, start, SLC_BLOCK, 0).reshape(SLC_BLOCK, 2, GROUPS, per_group, 1)
            mixed = block_gates[:, 0] * cmp_out + block_gates[:, 1] * sel_out
            mixed = jnp.where((query_pos < length)[:, None, None, None], mixed, 0.0)
            return mixed.reshape(SLC_BLOCK, HEADS * HEAD_DIM).astype(jnp.bfloat16)
        mixed = lax.map(one_block, jnp.arange(BLOCKS).astype(jnp.int32)).reshape(SEQ_LEN, HEADS * HEAD_DIM)
        wide = mixed.astype(jnp.float32)
        scaled = (wide * out_gain[None, :]).astype(jnp.bfloat16)
        row_scale = lax.rsqrt(lax.optimization_barrier(jnp.mean(wide * wide, axis=-1, keepdims=True)) + norm_eps)
        projected = jnp.dot(scaled, w_out, preferred_element_type=jnp.float32)
        return (projected * row_scale).astype(jnp.bfloat16)
    return lax.map(one_sequence, (hidden_in, seq_lengths, chosen))
```

```python
import functools
import math

import jax
import jax.numpy as jnp
from jax import lax
from jax.experimental import pallas as pl
from jax.experimental.pallas import tpu as pltpu
from jax.sharding import PartitionSpec as P

HEADS = 16
HEAD_DIM = 64
CMP_STRIDE = 16
CMP_BLOCK = 32
TOPK = 16


theta_base = 500000.0
norm_eps = 1e-06


def rotate(values, positions):
    width = values.shape[-1]
    half = width // 2
    inverse = jnp.exp(
        -jnp.log(jnp.float32(theta_base)) * jnp.arange(0, width, 2).astype(jnp.float32) / width
    )
    angle = positions.astype(jnp.float32)[:, None] * inverse[None, :]
    cosine = jnp.cos(angle)[:, None, :]
    sine = jnp.sin(angle)[:, None, :]
    first = values[..., :half]
    second = values[..., half:]
    return jnp.concatenate(
        [first * cosine - second * sine, second * cosine + first * sine], axis=-1
    )


def masked_weights(scores, valid):
    top = jnp.max(jnp.where(valid, scores, -1e30), axis=-1, keepdims=True)
    expd = jnp.where(valid, jnp.exp(scores - top), 0.0)
    total = jnp.sum(expd, axis=-1, keepdims=True)
    return (expd / jnp.maximum(total, 1.0)).astype(jnp.bfloat16)


def compress(raw, prior, weight_in, weight_out):
    seqs, span, groups, width = raw.shape
    extended = jnp.concatenate([prior, raw], axis=1)
    count = span // CMP_STRIDE
    front = extended[:, :span].reshape(seqs, count, CMP_STRIDE, groups, width)
    back = extended[:, CMP_STRIDE:].reshape(seqs, count, CMP_STRIDE, groups, width)
    window = jnp.concatenate([front, back], axis=2).transpose(0, 1, 3, 2, 4)
    window = window.reshape(seqs * count * groups, CMP_BLOCK * width)
    inner = jax.nn.gelu(jnp.dot(window, weight_in, preferred_element_type=jnp.float32)).astype(
        jnp.bfloat16
    )
    return jnp.dot(inner, weight_out, preferred_element_type=jnp.float32).reshape(
        seqs, count, groups, width
    )


def shards(
    hidden_in,
    w_query,
    w_cmp_key,
    w_cmp_value,
    w_sel_key,
    w_sel_value,
    w_gate,
    cmp_key_in,
    cmp_key_out,
    cmp_value_in,
    cmp_value_out,
    out_gain,
    w_out,
    seq_lengths,
    chosen,
):
    seqs, span, width = hidden_in.shape
    block_list = lax.axis_size("kv")
    place = lax.axis_index("kv")
    column = lax.axis_index("tp")
    local_heads = w_query.shape[1] // HEAD_DIM
    local_groups = w_sel_key.shape[1] // HEAD_DIM
    per_group = local_heads // local_groups
    count = span // CMP_STRIDE
    scale = HEAD_DIM ** (-0.5)
    rows = hidden_in.reshape(seqs * span, width)
    positions = place * span + jnp.arange(span, dtype=jnp.int32)

    def project(weight_matrix, heads):
        return jnp.dot(rows, weight_matrix, preferred_element_type=jnp.float32).reshape(
            seqs, span, heads, HEAD_DIM
        )

    queries = rotate(project(w_query, local_heads), positions).astype(jnp.bfloat16)
    sel_pairs = jnp.concatenate(
        [rotate(project(w_sel_key, local_groups), positions), project(w_sel_value, local_groups)],
        axis=-1,
    ).astype(jnp.bfloat16)
    raw_pairs = jnp.concatenate(
        [project(w_cmp_key, local_groups), project(w_cmp_value, local_groups)], axis=-1
    ).astype(jnp.bfloat16)
    prior = jnp.zeros((seqs, CMP_STRIDE, local_groups, HEAD_DIM), jnp.bfloat16)
    ends = place * span + jnp.arange(count, dtype=jnp.int32) * CMP_STRIDE + CMP_STRIDE - 1
    cmp_keys = rotate(compress(raw_pairs[..., :HEAD_DIM], prior, cmp_key_in, cmp_key_out), ends)
    cmp_values = compress(raw_pairs[..., HEAD_DIM:], prior, cmp_value_in, cmp_value_out)
    cmp_piece = jnp.concatenate(
        [cmp_keys.astype(jnp.bfloat16), cmp_values.astype(jnp.bfloat16)], axis=-1
    )[:, None]
    picks = chosen[:, 0]
    every_list = lax.all_gather(picks[None, :, :, 1:], "kv", axis=0, tiled=True)
    named = jnp.any(every_list == place, axis=(0, 3)).astype(jnp.int32)
    seq_ids = jnp.arange(seqs, dtype=jnp.int32)[:, None]
    exported_seq = jnp.sum(named * seq_ids, axis=0)
    selector = seq_ids == exported_seq[None, :]
    export = jnp.sum(
        jnp.where(selector[:, None, :, None], sel_pairs, jnp.zeros((), jnp.bfloat16)), axis=0
    )
    export = export[None]
    remote_pairs, remote_entries = (
        lax.all_gather(export, "kv", axis=0, tiled=True),
        lax.all_gather(cmp_piece, "kv", axis=1, tiled=True),
    )
    gate_all = jnp.dot(rows, w_gate.reshape(width, 2 * HEADS), preferred_element_type=jnp.float32)
    gate_all = gate_all.reshape(seqs, span, 2, HEADS)
    gates = jax.nn.sigmoid(lax.dynamic_slice_in_dim(gate_all, column * local_heads, local_heads, 3))
    entry = jnp.arange(block_list * count, dtype=jnp.int32)
    entry_end = entry * CMP_STRIDE + CMP_STRIDE - 1
    cmp_valid = ((entry >= 1)[None, :] & (entry_end[None, :] <= positions[:, None]))[None, None]
    key_pos = jnp.arange(span, dtype=jnp.int32)
    own_valid = key_pos[None, :] <= key_pos[:, None]

    def one_sequence(args):
        seq_queries, seq_entries, seq_picks, seq_pairs, seq_gates, seq_length = args
        block_q = seq_queries.reshape(span, local_groups, per_group, HEAD_DIM)
        entries = seq_entries.reshape(block_list * count, local_groups, 2 * HEAD_DIM)
        scores = (
            jnp.einsum(
                "qghd,egd->ghqe",
                block_q,
                entries[..., :HEAD_DIM],
                preferred_element_type=jnp.float32,
            )
            * scale
        )
        weights = masked_weights(scores, cmp_valid)
        cmp_out = jnp.einsum(
            "ghqe,egd->qghd", weights, entries[..., HEAD_DIM:], preferred_element_type=jnp.float32
        )
        far = jnp.maximum(seq_picks[:, 1:], 0)
        fetched = jax.vmap(lambda table, index: table[index], in_axes=(2, 0))(remote_pairs, far)
        near = jnp.transpose(seq_pairs, (1, 0, 2))[:, None]
        pairs = jnp.concatenate([near, fetched], axis=1).reshape(
            local_groups, TOPK * span, 2 * HEAD_DIM
        )
        far_live = jnp.broadcast_to(
            (seq_picks[:, 1:] >= 0)[:, None, :, None], (local_groups, span, TOPK - 1, span)
        )
        near_live = jnp.broadcast_to(own_valid[None, :, None, :], (local_groups, span, 1, span))
        sel_valid = jnp.concatenate([near_live, far_live], axis=2).reshape(
            local_groups, 1, span, TOPK * span
        )
        scores_s = (
            jnp.einsum(
                "qghd,gmd->ghqm", block_q, pairs[..., :HEAD_DIM], preferred_element_type=jnp.float32
            )
            * scale
        )
        weights_s = masked_weights(scores_s, sel_valid)
        sel_out = jnp.einsum(
            "ghqm,gmd->qghd", weights_s, pairs[..., HEAD_DIM:], preferred_element_type=jnp.float32
        )
        split = seq_gates.reshape(span, 2, local_groups, per_group, 1)
        mixed = split[:, 0] * cmp_out + split[:, 1] * sel_out
        mixed = jnp.where((positions < seq_length)[:, None, None, None], mixed, 0.0)
        return mixed.reshape(span, local_heads * HEAD_DIM).astype(jnp.bfloat16)

    mixed = lax.map(one_sequence, (queries, remote_entries, picks, sel_pairs, gates, seq_lengths))
    mixed = mixed.reshape(seqs * span, local_heads * HEAD_DIM)
    out_width = width // lax.axis_size("tp")
    own_columns = lax.dynamic_slice_in_dim(w_out, column * out_width, out_width, 1)
    piece_wide = lax.all_gather(mixed, "tp", axis=1, tiled=True).astype(jnp.float32)
    scaled_piece = (piece_wide * out_gain[None, :]).astype(jnp.bfloat16)
    total = jnp.dot(scaled_piece, own_columns, preferred_element_type=jnp.float32)
    squares = jnp.sum(piece_wide * piece_wide, axis=-1)
    row_scale = lax.rsqrt(squares / (HEADS * HEAD_DIM) + norm_eps)
    return (total * row_scale[:, None]).astype(jnp.bfloat16).reshape(seqs, span, out_width)


FAR = -1e30
PLANE = 4
VMEM_BYTES = 60 * 1024 * 1024
f32 = jnp.float32
bf16 = jnp.bfloat16


def dot(a, b):
    return jnp.dot(a, b, preferred_element_type=f32)


def dot_t(a, b):
    return lax.dot_general(a, b, (((1,), (1,)), ((), ())), preferred_element_type=f32)


def turn(values, cosine, sine):
    lane = lax.broadcasted_iota(jnp.int32, values.shape, 1)
    other = jnp.where(
        lane % HEAD_DIM < HEAD_DIM // 2,
        pltpu.roll(values, 128 - HEAD_DIM // 2, 1),
        pltpu.roll(values, HEAD_DIM // 2, 1),
    )
    return values * cosine + other * sine


def gelu(x):
    return 0.5 * x * (1.0 + jnp.tanh(0.7978845608028654 * (x + 0.044715 * (x * x * x))))


def layer_kernel(
    n, seqs, span, heads,
    lens_ref, picks_ref, gain_ref, kout_ref, vout_ref,
    rows_ref, wq_ref, wck_ref, wcv_ref, wsk_ref, wsv_ref, wg_ref, kin_ref, vin_ref, wout_ref,
    out_ref,
    rows, wq, ws, wg, kin, vin, weight,
    q_buf, sk_buf, sv_buf, raw, gate_buf, lists, blobs, own, other, bias, near, partial,
    load_sem, pick_send, pick_recv, blob_send, blob_recv, half_send, half_recv,
):
    me = lax.axis_index("kv")
    column = lax.axis_index("tp")
    planes = n // PLANE
    z, x, c = me // PLANE, (me // 2) % 2, me % 2
    depth = heads * HEAD_DIM
    wide = out_ref.shape[1]
    count = span // CMP_STRIDE
    entries = seqs * count
    half = heads // 2
    mesh_id = pl.DeviceIdType.MESH

    pairs = [(rows_ref, rows)]
    for i, ref in enumerate((wsk_ref, wsv_ref, wck_ref, wcv_ref)):
        pairs.append((ref, ws.at[:, i * 128 : (i + 1) * 128]))
    pairs += [(kin_ref, kin), (vin_ref, vin), (wq_ref, wq), (wg_ref, wg)]
    for i in range(2):
        side = column if i == 0 else 1 - column
        block = wout_ref.at[
            pl.ds(pl.multiple_of(side * depth, depth), depth),
            pl.ds(pl.multiple_of(column * wide, wide), wide),
        ]
        pairs.append((block, weight.at[i]))
    loads = [pltpu.make_async_copy(a, b, load_sem.at[i]) for i, (a, b) in enumerate(pairs)]
    for load in loads:
        load.start()

    barrier = pltpu.get_barrier_semaphore()
    for d in range(1, n):
        pl.semaphore_signal(
            barrier, inc=1, device_id={"kv": (me + d) % n}, device_id_type=mesh_id
        )
    pl.semaphore_signal(barrier, inc=1, device_id={"tp": 1 - column}, device_id_type=mesh_id)

    lane = lax.broadcasted_iota(jnp.int32, (span, 128), 1)
    low = lane < HEAD_DIM
    low_e = low[:entries]
    at = lax.broadcasted_iota(jnp.int32, (span, 128), 0)
    sign = jnp.where(lane % HEAD_DIM < HEAD_DIM // 2, -1.0, 1.0)
    power = (lane % (HEAD_DIM // 2) * 2).astype(f32)
    freq = jnp.exp(-math.log(theta_base) * power / HEAD_DIM)
    angle = (me * span + at).astype(f32) * freq
    cosine = jnp.cos(angle)
    sine = jnp.sin(angle) * sign
    end = me * span + (at[:entries] % count) * CMP_STRIDE + CMP_STRIDE - 1
    angle = end.astype(f32) * freq[:entries]
    cosine_e = jnp.cos(angle)
    sine_e = jnp.sin(angle) * sign[:entries]
    row_q = lax.broadcasted_iota(jnp.int32, (span, span), 0)
    near[...] = jnp.where(
        lax.broadcasted_iota(jnp.int32, (span, span), 1) <= row_q, 0.0, FAR
    )
    far_keys = n * span
    block = lax.broadcasted_iota(jnp.int32, (2, far_keys), 1) // span
    for s in range(seqs):
        listed = picks_ref[s]
        hit = jnp.zeros((2, far_keys), jnp.int32)
        for j in range(1, TOPK):
            hit = jnp.where(block == listed[:, j : j + 1], 1, hit)
        bias[s] = jnp.where(hit > 0, 0.0, FAR)

    pl.semaphore_wait(barrier, n)
    sent = []
    for d in range(1, n):
        copy = pltpu.make_async_remote_copy(
            src_ref=picks_ref, dst_ref=lists.at[me], send_sem=pick_send.at[d - 1],
            recv_sem=pick_recv.at[me], device_id={"kv": (me + d) % n}, device_id_type=mesh_id,
        )
        copy.start()
        sent.append(copy)

    for load in loads[:5]:
        load.wait()
    made = dot(rows[...], ws[...])
    for s in range(seqs):
        part = slice(s * span, (s + 1) * span)
        sk_buf[part, :] = turn(made[part, :128], cosine, sine).astype(bf16)
    sv_buf[...] = made[:, 128:256].astype(bf16)
    raw[0] = made[:, 256:384].astype(bf16).astype(f32)
    raw[1] = made[:, 384:512].astype(bf16).astype(f32)
    first = at[:entries] % count == 0
    mid = CMP_STRIDE * HEAD_DIM
    for branch, inner_weight, outer in ((0, kin, kout_ref), (1, vin, vout_ref)):
        loads[5 + branch].wait()
        left, right = [], []
        for j in range(0, CMP_STRIDE, 2):
            a = raw[branch, pl.ds(j, entries, stride=CMP_STRIDE), :]
            b = raw[branch, pl.ds(j + 1, entries, stride=CMP_STRIDE), :]
            left.append(jnp.where(low_e, a, pltpu.roll(b, HEAD_DIM, 1)))
            right.append(jnp.where(low_e, pltpu.roll(a, HEAD_DIM, 1), b))
        window = jnp.concatenate(
            [jnp.concatenate(left, axis=1), jnp.concatenate(right, axis=1)], axis=0
        ).astype(bf16)
        front = dot(window, inner_weight[:mid])
        back = dot(window, inner_weight[mid:])
        parts = []
        for g in range(2):
            shifted = pltpu.roll(front[g * entries : (g + 1) * entries], 1, 0)
            parts.append(back[g * entries : (g + 1) * entries] + jnp.where(first, 0.0, shifted))
        inner = gelu(jnp.concatenate(parts, axis=0)).astype(bf16)
        outer = jnp.concatenate([outer[...], outer[...]], axis=0)
        result = dot_t(inner, outer)
        result = jnp.where(low_e, result[:entries], result[entries:])
        if branch == 0:
            result = turn(result, cosine_e, sine_e)
        start = 2 * span + branch * entries
        blobs[me, start : start + entries, :] = result.astype(bf16)

    loads[7].wait()
    loads[8].wait()
    hidden = rows[...]
    for i in range(half):
        made = dot(hidden, wq[:, i * 128 : (i + 1) * 128])
        for s in range(seqs):
            v = turn(made[s * span : (s + 1) * span], cosine, sine) * (HEAD_DIM**-0.5)
            y = pltpu.roll(v, HEAD_DIM, 1)
            if 2 * i < half:
                even, odd = jnp.where(low, v, 0.0), jnp.where(low, y, 0.0)
            else:
                even, odd = jnp.where(low, 0.0, y), jnp.where(low, 0.0, v)
            base = (s * heads + 2 * i) * span
            q_buf[base : base + span, :] = even.astype(bf16)
            q_buf[base + span : base + 2 * span, :] = odd.astype(bf16)
    spread = 2 * wg_ref.shape[1]
    gate_buf[...] = jnp.zeros_like(gate_buf)
    gate_buf[:, :spread] = jax.nn.sigmoid(dot_t(hidden, wg[...].reshape(spread, rows.shape[1])))

    named = jnp.zeros((seqs, 2, TOPK), jnp.int32)
    for d in range(1, n):
        origin = (me + d) % n
        pltpu.make_async_remote_copy(
            src_ref=picks_ref, dst_ref=lists.at[origin], send_sem=pick_send.at[d - 1],
            recv_sem=pick_recv.at[origin], device_id={"kv": origin}, device_id_type=mesh_id,
        ).wait_recv()
        named = jnp.maximum(named, (lists[origin] == me).astype(jnp.int32))
    slot_at = lax.broadcasted_iota(jnp.int32, (seqs, 2, TOPK), 2)
    named = jnp.max(jnp.where(slot_at == 0, 0, named), axis=2, keepdims=True)
    key = jnp.zeros((span, 128), f32)
    value = jnp.zeros((span, 128), f32)
    for s in range(seqs):
        flag = jnp.where(low, named[s, 0:1, :], named[s, 1:2, :]) > 0
        key = jnp.where(flag, sk_buf[s * span : (s + 1) * span, :].astype(f32), key)
        value = jnp.where(flag, sv_buf[s * span : (s + 1) * span, :].astype(f32), value)
    blobs[me, 0:span, :] = key.astype(bf16)
    blobs[me, span : 2 * span, :] = value.astype(bf16)

    def pass_on(slot, dst, number):
        copy = pltpu.make_async_remote_copy(
            src_ref=blobs.at[slot], dst_ref=blobs.at[slot], send_sem=blob_send.at[number],
            recv_sem=blob_recv.at[slot], device_id={"kv": dst}, device_id_type=mesh_id,
        )
        copy.start()
        sent.append(copy)

    def arrived(slot):
        pltpu.make_async_remote_copy(
            src_ref=blobs.at[slot], dst_ref=blobs.at[slot], send_sem=blob_send.at[0],
            recv_sem=blob_recv.at[slot], device_id={"kv": (me + 1) % n}, device_id_type=mesh_id,
        ).wait_recv()

    across = z * PLANE + (1 - x) * 2 + c
    beside = z * PLANE + x * 2 + (1 - c)
    order = sorted(range(1, planes), key=lambda d: (min(d, planes - d), d))
    number = 0
    for d in order:
        pass_on(me, ((z + d) % planes) * PLANE + x * 2 + c, number)
        number += 1
    pass_on(me, across, number)
    pass_on(me, beside, number + 1)
    number += 2

    for d in order:
        slot = ((z + planes - d) % planes) * PLANE + x * 2 + c
        arrived(slot)
        pass_on(slot, across, number)
        pass_on(slot, beside, number + 1)
        number += 2
    for d in [0] + order:
        slot = ((z + planes - d) % planes) * PLANE + (1 - x) * 2 + c
        arrived(slot)
        pass_on(slot, beside, number)
        number += 1
    for d in [0] + order:
        origin = ((z + planes - d) % planes) * PLANE
        arrived(origin + x * 2 + (1 - c))
        arrived(origin + (1 - x) * 2 + (1 - c))

    slot = lax.broadcasted_iota(jnp.int32, (span, n * entries), 1)
    entry = (slot // entries) * count + slot % count
    entry_seq = (slot % entries) // count
    query_at = me * span + lax.broadcasted_iota(jnp.int32, (span, n * entries), 0)
    entry_ok = (entry >= 1) & (entry * CMP_STRIDE + CMP_STRIDE - 1 <= query_at)
    row_at = me * span + at
    far_k = blobs[:, 0:span, :].reshape(far_keys, 128)
    far_v = blobs[:, span : 2 * span, :].reshape(far_keys, 128)
    cmp_k = blobs[:, 2 * span : 2 * span + entries, :].reshape(n * entries, 128)
    cmp_v = blobs[:, 2 * span + entries :, :].reshape(n * entries, 128)

    def piece(s):
        return pltpu.make_async_remote_copy(
            src_ref=own.at[s], dst_ref=other.at[s], send_sem=half_send.at[s],
            recv_sem=half_recv.at[s], device_id={"tp": 1 - column}, device_id_type=mesh_id,
        )

    def one_sequence(s, carry):
        part = pl.ds(pl.multiple_of(s * span, span), span)
        near_k = sk_buf[part, :]
        near_v = sv_buf[part, :]
        gates = gate_buf[part, :]
        gates = jnp.where(column == 0, gates, pltpu.roll(gates, 128 - heads, 1))
        live = row_at < lens_ref[s]
        entry_bias = jnp.where(entry_ok & (entry_seq == s), 0.0, FAR)
        for g in range(2):
            start = pl.multiple_of((s * heads + g * half) * span, span)
            q = q_buf[pl.ds(start, half * span), :]
            sc = dot_t(q, cmp_k).reshape(half, span, n * entries) + entry_bias[None]
            top = jnp.maximum(jnp.max(sc, axis=-1, keepdims=True), -1e29)
            e = jnp.exp(sc - top)
            total = jnp.maximum(jnp.sum(e, axis=-1, keepdims=True), 1.0)
            w = (e * (1.0 / total)).astype(bf16).reshape(half * span, n * entries)
            cmp_out = dot(w, cmp_v)
            sf = dot_t(q, far_k) + bias[s, g : g + 1, :]
            sn = (dot_t(q, near_k).reshape(half, span, span) + near[...][None]).reshape(
                half * span, span
            )
            top = jnp.maximum(
                jnp.max(sf, axis=-1, keepdims=True), jnp.max(sn, axis=-1, keepdims=True)
            )
            ef = jnp.exp(sf - top)
            en = jnp.exp(sn - top)
            total = jnp.sum(ef, axis=-1, keepdims=True) + jnp.sum(en, axis=-1, keepdims=True)
            inverse = 1.0 / total
            sel_out = dot((ef * inverse).astype(bf16), far_v) + dot(
                (en * inverse).astype(bf16), near_v
            )
            mixed = []
            for h in range(half):
                span_h = slice(h * span, (h + 1) * span)
                head = g * half + h
                behind = spread // 2 + head
                mixed.append(
                    gates[:, head : head + 1] * cmp_out[span_h]
                    + gates[:, behind : behind + 1] * sel_out[span_h]
                )
            for h in range(0, half, 2):
                if g == 0:
                    pair = jnp.where(low, mixed[h], pltpu.roll(mixed[h + 1], HEAD_DIM, 1))
                else:
                    pair = jnp.where(low, pltpu.roll(mixed[h], HEAD_DIM, 1), mixed[h + 1])
                pair = jnp.where(live, pair, 0.0).astype(bf16)
                lanes = (g * half + h) * HEAD_DIM
                own[s, :, lanes : lanes + 128] = pair
        piece(s).start()
        return carry

    lax.fori_loop(0, seqs, one_sequence, 0)
    for load in loads[9:]:
        load.wait()
    gain_own = gain_ref[:, pl.ds(pl.multiple_of(column * depth, depth), depth)]
    gain_other = gain_ref[:, pl.ds(pl.multiple_of((1 - column) * depth, depth), depth)]

    def begin(s, carry):
        partial[s] = dot((own[s].astype(f32) * gain_own).astype(bf16), weight[0])
        return carry

    lax.fori_loop(0, seqs, begin, 0)

    def finish(s, carry):
        piece(s).wait_recv()
        a = own[s].astype(f32)
        b = other[s].astype(f32)
        squares = jnp.sum(a * a, axis=-1, keepdims=True) + jnp.sum(b * b, axis=-1, keepdims=True)
        row_scale = lax.rsqrt(squares / (2 * depth) + norm_eps)
        total = partial[s] + dot((b * gain_other).astype(bf16), weight[1])
        out_ref[pl.ds(pl.multiple_of(s * span, span), span), :] = (total * row_scale).astype(bf16)
        return carry

    lax.fori_loop(0, seqs, finish, 0)

    def close(s, carry):
        piece(s).wait_send()
        return carry

    lax.fori_loop(0, seqs, close, 0)
    for copy in sent:
        copy.wait_send()


def fused_shards(
    hidden_in,
    w_query,
    w_cmp_key,
    w_cmp_value,
    w_sel_key,
    w_sel_value,
    w_gate,
    cmp_key_in,
    cmp_key_out,
    cmp_value_in,
    cmp_value_out,
    out_gain,
    w_out,
    seq_lengths,
    chosen,
):
    seqs, span, width = hidden_in.shape
    n = lax.axis_size("kv")
    heads = w_query.shape[1] // HEAD_DIM
    total = seqs * span
    entries = total // CMP_STRIDE
    out_width = width // lax.axis_size("tp")
    small = w_sel_key.shape[1]
    vmem = pl.BlockSpec(memory_space=pltpu.VMEM)
    anywhere = pl.BlockSpec(memory_space=pl.ANY)
    gate_rows = jnp.transpose(w_gate, (1, 2, 0))
    out = pl.pallas_call(
        functools.partial(layer_kernel, n, seqs, span, heads),
        in_specs=[pl.BlockSpec(memory_space=pltpu.SMEM)] + [vmem] * 4 + [anywhere] * 10,
        out_specs=vmem,
        out_shape=pltpu.VMEM((total, out_width), bf16),
        scratch_shapes=[
            pltpu.VMEM((total, width), bf16),
            pltpu.VMEM(w_query.shape, bf16),
            pltpu.VMEM((width, 4 * small), bf16),
            pltpu.VMEM(gate_rows.shape, bf16),
            pltpu.VMEM(cmp_key_in.shape, bf16),
            pltpu.VMEM(cmp_value_in.shape, bf16),
            pltpu.VMEM((2, heads * HEAD_DIM, out_width), bf16),
            pltpu.VMEM((heads * total, 128), bf16),
            pltpu.VMEM((total, small), bf16),
            pltpu.VMEM((total, small), bf16),
            pltpu.VMEM((2, total, small), f32),
            pltpu.VMEM((total, 128), f32),
            pltpu.VMEM((n, seqs, 2, TOPK), jnp.int32),
            pltpu.VMEM((n, 2 * span + 2 * entries, small), bf16),
            pltpu.VMEM((seqs, span, heads * HEAD_DIM), bf16),
            pltpu.VMEM((seqs, span, heads * HEAD_DIM), bf16),
            pltpu.VMEM((seqs, 2, n * span), f32),
            pltpu.VMEM((span, span), f32),
            pltpu.VMEM((seqs, span, out_width), f32),
            pltpu.SemaphoreType.DMA((11,)),
            pltpu.SemaphoreType.DMA((n,)),
            pltpu.SemaphoreType.DMA((n,)),
            pltpu.SemaphoreType.DMA((n,)),
            pltpu.SemaphoreType.DMA((n,)),
            pltpu.SemaphoreType.DMA((seqs,)),
            pltpu.SemaphoreType.DMA((seqs,)),
        ],
        compiler_params=pltpu.CompilerParams(
            collective_id=0, has_side_effects=True, vmem_limit_bytes=VMEM_BYTES
        ),
        name="layer",
    )(
        seq_lengths, chosen[:, 0], out_gain[None],
        jnp.transpose(cmp_key_out), jnp.transpose(cmp_value_out),
        hidden_in.reshape(total, width), w_query, w_cmp_key, w_cmp_value, w_sel_key,
        w_sel_value, gate_rows, cmp_key_in, cmp_value_in, w_out,
    )
    return out.reshape(seqs, span, out_width)


def fits(mesh):
    n = mesh.shape["kv"]
    return mesh.shape["tp"] == 2 and n % PLANE == 0 and n <= 32


def solution(mesh):
    placed = (
        P(None, "kv", None),
        P(None, "tp"),
        P(None, "tp"),
        P(None, "tp"),
        P(None, "tp"),
        P(None, "tp"),
        P(),
        P(),
        P(),
        P(),
        P(),
        P(),
        P(),
        P(),
        P(None, "kv", "tp", None),
    )
    return jax.shard_map(
        fused_shards if fits(mesh) else shards, mesh=mesh, in_specs=placed, out_specs=P(None, "kv", "tp"), check_vma=False
    )
```

```python
import functools
import math

import jax
import jax.numpy as jnp
from jax import lax
from jax.experimental import pallas as pl
from jax.experimental.pallas import tpu as pltpu
from jax.sharding import PartitionSpec as P

HEADS = 16
HEAD_DIM = 64
CMP_STRIDE = 16
CMP_BLOCK = 32
TOPK = 16


theta_base = 500000.0
norm_eps = 1e-06


def rotate(values, positions):
    width = values.shape[-1]
    half = width // 2
    inverse = jnp.exp(
        -jnp.log(jnp.float32(theta_base)) * jnp.arange(0, width, 2).astype(jnp.float32) / width
    )
    angle = positions.astype(jnp.float32)[:, None] * inverse[None, :]
    cosine = jnp.cos(angle)[:, None, :]
    sine = jnp.sin(angle)[:, None, :]
    first = values[..., :half]
    second = values[..., half:]
    return jnp.concatenate(
        [first * cosine - second * sine, second * cosine + first * sine], axis=-1
    )


def masked_weights(scores, valid):
    top = jnp.max(jnp.where(valid, scores, -1e30), axis=-1, keepdims=True)
    expd = jnp.where(valid, jnp.exp(scores - top), 0.0)
    total = jnp.sum(expd, axis=-1, keepdims=True)
    return (expd / jnp.maximum(total, 1.0)).astype(jnp.bfloat16)


def compress(raw, prior, weight_in, weight_out):
    seqs, span, groups, width = raw.shape
    extended = jnp.concatenate([prior, raw], axis=1)
    count = span // CMP_STRIDE
    front = extended[:, :span].reshape(seqs, count, CMP_STRIDE, groups, width)
    back = extended[:, CMP_STRIDE:].reshape(seqs, count, CMP_STRIDE, groups, width)
    window = jnp.concatenate([front, back], axis=2).transpose(0, 1, 3, 2, 4)
    window = window.reshape(seqs * count * groups, CMP_BLOCK * width)
    inner = jax.nn.gelu(jnp.dot(window, weight_in, preferred_element_type=jnp.float32)).astype(
        jnp.bfloat16
    )
    return jnp.dot(inner, weight_out, preferred_element_type=jnp.float32).reshape(
        seqs, count, groups, width
    )


def shards(
    hidden_in,
    w_query,
    w_cmp_key,
    w_cmp_value,
    w_sel_key,
    w_sel_value,
    w_gate,
    cmp_key_in,
    cmp_key_out,
    cmp_value_in,
    cmp_value_out,
    out_gain,
    w_out,
    seq_lengths,
    chosen,
):
    seqs, span, width = hidden_in.shape
    block_list = lax.axis_size("kv")
    place = lax.axis_index("kv")
    column = lax.axis_index("tp")
    local_heads = w_query.shape[1] // HEAD_DIM
    local_groups = w_sel_key.shape[1] // HEAD_DIM
    per_group = local_heads // local_groups
    count = span // CMP_STRIDE
    scale = HEAD_DIM ** (-0.5)
    rows = hidden_in.reshape(seqs * span, width)
    positions = place * span + jnp.arange(span, dtype=jnp.int32)

    def project(weight_matrix, heads):
        return jnp.dot(rows, weight_matrix, preferred_element_type=jnp.float32).reshape(
            seqs, span, heads, HEAD_DIM
        )

    queries = rotate(project(w_query, local_heads), positions).astype(jnp.bfloat16)
    sel_pairs = jnp.concatenate(
        [rotate(project(w_sel_key, local_groups), positions), project(w_sel_value, local_groups)],
        axis=-1,
    ).astype(jnp.bfloat16)
    raw_pairs = jnp.concatenate(
        [project(w_cmp_key, local_groups), project(w_cmp_value, local_groups)], axis=-1
    ).astype(jnp.bfloat16)
    prior = jnp.zeros((seqs, CMP_STRIDE, local_groups, HEAD_DIM), jnp.bfloat16)
    ends = place * span + jnp.arange(count, dtype=jnp.int32) * CMP_STRIDE + CMP_STRIDE - 1
    cmp_keys = rotate(compress(raw_pairs[..., :HEAD_DIM], prior, cmp_key_in, cmp_key_out), ends)
    cmp_values = compress(raw_pairs[..., HEAD_DIM:], prior, cmp_value_in, cmp_value_out)
    cmp_piece = jnp.concatenate(
        [cmp_keys.astype(jnp.bfloat16), cmp_values.astype(jnp.bfloat16)], axis=-1
    )[:, None]
    picks = chosen[:, 0]
    every_list = lax.all_gather(picks[None, :, :, 1:], "kv", axis=0, tiled=True)
    named = jnp.any(every_list == place, axis=(0, 3)).astype(jnp.int32)
    seq_ids = jnp.arange(seqs, dtype=jnp.int32)[:, None]
    exported_seq = jnp.sum(named * seq_ids, axis=0)
    selector = seq_ids == exported_seq[None, :]
    export = jnp.sum(
        jnp.where(selector[:, None, :, None], sel_pairs, jnp.zeros((), jnp.bfloat16)), axis=0
    )
    export = export[None]
    remote_pairs, remote_entries = (
        lax.all_gather(export, "kv", axis=0, tiled=True),
        lax.all_gather(cmp_piece, "kv", axis=1, tiled=True),
    )
    gate_all = jnp.dot(rows, w_gate.reshape(width, 2 * HEADS), preferred_element_type=jnp.float32)
    gate_all = gate_all.reshape(seqs, span, 2, HEADS)
    gates = jax.nn.sigmoid(lax.dynamic_slice_in_dim(gate_all, column * local_heads, local_heads, 3))
    entry = jnp.arange(block_list * count, dtype=jnp.int32)
    entry_end = entry * CMP_STRIDE + CMP_STRIDE - 1
    cmp_valid = ((entry >= 1)[None, :] & (entry_end[None, :] <= positions[:, None]))[None, None]
    key_pos = jnp.arange(span, dtype=jnp.int32)
    own_valid = key_pos[None, :] <= key_pos[:, None]

    def one_sequence(args):
        seq_queries, seq_entries, seq_picks, seq_pairs, seq_gates, seq_length = args
        block_q = seq_queries.reshape(span, local_groups, per_group, HEAD_DIM)
        entries = seq_entries.reshape(block_list * count, local_groups, 2 * HEAD_DIM)
        scores = (
            jnp.einsum(
                "qghd,egd->ghqe",
                block_q,
                entries[..., :HEAD_DIM],
                preferred_element_type=jnp.float32,
            )
            * scale
        )
        weights = masked_weights(scores, cmp_valid)
        cmp_out = jnp.einsum(
            "ghqe,egd->qghd", weights, entries[..., HEAD_DIM:], preferred_element_type=jnp.float32
        )
        far = jnp.maximum(seq_picks[:, 1:], 0)
        fetched = jax.vmap(lambda table, index: table[index], in_axes=(2, 0))(remote_pairs, far)
        near = jnp.transpose(seq_pairs, (1, 0, 2))[:, None]
        pairs = jnp.concatenate([near, fetched], axis=1).reshape(
            local_groups, TOPK * span, 2 * HEAD_DIM
        )
        far_live = jnp.broadcast_to(
            (seq_picks[:, 1:] >= 0)[:, None, :, None], (local_groups, span, TOPK - 1, span)
        )
        near_live = jnp.broadcast_to(own_valid[None, :, None, :], (local_groups, span, 1, span))
        sel_valid = jnp.concatenate([near_live, far_live], axis=2).reshape(
            local_groups, 1, span, TOPK * span
        )
        scores_s = (
            jnp.einsum(
                "qghd,gmd->ghqm", block_q, pairs[..., :HEAD_DIM], preferred_element_type=jnp.float32
            )
            * scale
        )
        weights_s = masked_weights(scores_s, sel_valid)
        sel_out = jnp.einsum(
            "ghqm,gmd->qghd", weights_s, pairs[..., HEAD_DIM:], preferred_element_type=jnp.float32
        )
        split = seq_gates.reshape(span, 2, local_groups, per_group, 1)
        mixed = split[:, 0] * cmp_out + split[:, 1] * sel_out
        mixed = jnp.where((positions < seq_length)[:, None, None, None], mixed, 0.0)
        return mixed.reshape(span, local_heads * HEAD_DIM).astype(jnp.bfloat16)

    mixed = lax.map(one_sequence, (queries, remote_entries, picks, sel_pairs, gates, seq_lengths))
    mixed = mixed.reshape(seqs * span, local_heads * HEAD_DIM)
    out_width = width // lax.axis_size("tp")
    own_columns = lax.dynamic_slice_in_dim(w_out, column * out_width, out_width, 1)
    piece_wide = lax.all_gather(mixed, "tp", axis=1, tiled=True).astype(jnp.float32)
    scaled_piece = (piece_wide * out_gain[None, :]).astype(jnp.bfloat16)
    total = jnp.dot(scaled_piece, own_columns, preferred_element_type=jnp.float32)
    squares = jnp.sum(piece_wide * piece_wide, axis=-1)
    row_scale = lax.rsqrt(squares / (HEADS * HEAD_DIM) + norm_eps)
    return (total * row_scale[:, None]).astype(jnp.bfloat16).reshape(seqs, span, out_width)


FAR = -1e30
PLANE = 4
VMEM_BYTES = 60 * 1024 * 1024
f32 = jnp.float32
bf16 = jnp.bfloat16


def dot(a, b):
    return jnp.dot(a, b, preferred_element_type=f32)


def dot_t(a, b):
    return lax.dot_general(a, b, (((1,), (1,)), ((), ())), preferred_element_type=f32)


def swap(values):
    return pltpu.roll(values, HEAD_DIM, 1)


def turn(values, cosine, sine):
    lane = lax.broadcasted_iota(jnp.int32, values.shape, 1)
    other = jnp.where(
        lane % HEAD_DIM < HEAD_DIM // 2,
        pltpu.roll(values, 128 - HEAD_DIM // 2, 1),
        pltpu.roll(values, HEAD_DIM // 2, 1),
    )
    return values * cosine + other * sine


def gelu(x):
    return 0.5 * x * (1.0 + jnp.tanh(0.7978845608028654 * (x + 0.044715 * (x * x * x))))


def layer_kernel(
    n, seqs, span, heads,
    picks_ref, rows_ref, wsk_ref, wsv_ref, wck_ref, wcv_ref, kout_ref, vout_ref, kin_ref, vin_ref,
    wq_ref, wg_ref, lens_ref, gain_ref, wout_ref,
    out_ref,
    picks, rows, ws, kout, vout, kin, vin, wq, wg, lens, gain, weight,
    qn, sk_buf, svt, raw, gate_buf, hits, lists, ents, blobs, near_s, far_s, probs, vals,
    mix, own, other, partial,
    load_sem, pick_send, pick_recv, ent_send, ent_recv, blob_send, blob_recv, half_send, half_recv,
):
    me = lax.axis_index("kv")
    column = lax.axis_index("tp")
    planes = n // PLANE
    z, x, c = me // PLANE, (me // 2) % 2, me % 2
    depth = heads * HEAD_DIM
    wide = out_ref.shape[1]
    count = span // CMP_STRIDE
    entries = seqs * count
    half = heads // 2
    stack = seqs * HEAD_DIM
    across_q = half * span
    pairs = seqs // 2
    mesh_id = pl.DeviceIdType.MESH

    barrier = pltpu.get_barrier_semaphore()
    for d in range(1, n):
        pl.semaphore_signal(
            barrier, inc=1, device_id={"kv": (me + d) % n}, device_id_type=mesh_id
        )
    pl.semaphore_signal(barrier, inc=1, device_id={"tp": 1 - column}, device_id_type=mesh_id)

    jobs = [(picks_ref, picks), (rows_ref, rows)]
    for i, ref in enumerate((wsk_ref, wsv_ref, wck_ref, wcv_ref)):
        jobs.append((ref, ws.at[:, i * 128 : (i + 1) * 128]))
    jobs += [(kout_ref, kout), (vout_ref, vout), (kin_ref, kin), (vin_ref, vin)]
    jobs += [(wq_ref, wq), (wg_ref, wg), (lens_ref, lens), (gain_ref, gain)]
    for i in range(2):
        side = column if i == 0 else 1 - column
        block = wout_ref.at[
            pl.ds(pl.multiple_of(side * depth, depth), depth),
            pl.ds(pl.multiple_of(column * wide, wide), wide),
        ]
        jobs.append((block, weight.at[i]))
    loads = [pltpu.make_async_copy(a, b, load_sem.at[i]) for i, (a, b) in enumerate(jobs)]
    for load in loads:
        load.start()

    lane = lax.broadcasted_iota(jnp.int32, (span, 128), 1)
    low = lane < HEAD_DIM
    low_e = low[:entries]
    low_row = low[:1]
    at = lax.broadcasted_iota(jnp.int32, (span, 128), 0)
    sign = jnp.where(lane % HEAD_DIM < HEAD_DIM // 2, -1.0, 1.0)
    power = (lane % (HEAD_DIM // 2) * 2).astype(f32)
    freq = jnp.exp(-math.log(theta_base) * power / HEAD_DIM)
    angle = (me * span + at).astype(f32) * freq
    cosine = jnp.cos(angle)
    sine = jnp.sin(angle) * sign
    end = me * span + (at[:entries] % count) * CMP_STRIDE + CMP_STRIDE - 1
    angle = end.astype(f32) * freq[:entries]
    cosine_e = jnp.cos(angle)
    sine_e = jnp.sin(angle) * sign[:entries]

    for plane in range(1, planes):
        @pl.when(plane > z)
        def _():
            for g in range(2):
                for i in range(PLANE):
                    blobs[g, plane * PLANE + i] = jnp.zeros((span, 128), bf16)

    for d in range(1, n):
        @pl.when(d > me)
        def _():
            ents[d] = jnp.zeros((2 * entries, 128), bf16)

    loads[0].wait()
    slot_at = lax.broadcasted_iota(jnp.int32, (2 * seqs, TOPK), 1)
    listed = jnp.where(slot_at == 0, -1, picks[...])
    for b in range(n):
        hit = jnp.max(jnp.where(listed == b, 1.0, 0.0), axis=1, keepdims=True)
        hits[b] = jnp.broadcast_to(hit, (2 * seqs, 128))

    pl.semaphore_wait(barrier, n)
    sent = []

    def send(src, dst, ssem, rsem, target, when=None):
        copy = pltpu.make_async_remote_copy(
            src_ref=src, dst_ref=dst, send_sem=ssem, recv_sem=rsem,
            device_id=target, device_id_type=mesh_id,
        )
        if when is None:
            copy.start()
        else:
            pl.when(when)(copy.start)
        sent.append((copy, when))

    for d in range(1, n):
        send(picks, lists.at[me], pick_send.at[d - 1], pick_recv.at[me], {"kv": (me + d) % n})

    for load in loads[1:6]:
        load.wait()
    made = dot(rows[...], ws[...])
    sv = []
    for s in range(seqs):
        part = slice(s * span, (s + 1) * span)
        sk_buf[part, :] = turn(made[part, :128], cosine, sine).astype(bf16)
    svt[...] = jnp.transpose(made[:, 128:256]).astype(bf16)
    raw[0] = made[:, 256:384].astype(bf16).astype(f32)
    raw[1] = made[:, 384:512].astype(bf16).astype(f32)
    first = at[:entries] % count == 0
    mid = CMP_STRIDE * HEAD_DIM
    results = []
    for load in loads[6:10]:
        load.wait()
    for branch, inner_weight, outer in ((0, kin, kout), (1, vin, vout)):
        left, right = [], []
        for j in range(0, CMP_STRIDE, 2):
            a = raw[branch, pl.ds(j, entries, stride=CMP_STRIDE), :]
            b = raw[branch, pl.ds(j + 1, entries, stride=CMP_STRIDE), :]
            left.append(jnp.where(low_e, a, swap(b)))
            right.append(jnp.where(low_e, swap(a), b))
        window = jnp.concatenate(
            [jnp.concatenate(left, axis=1), jnp.concatenate(right, axis=1)], axis=0
        ).astype(bf16)
        front = dot(window, inner_weight[:mid])
        back = dot(window, inner_weight[mid:])
        parts = []
        for g in range(2):
            shifted = pltpu.roll(front[g * entries : (g + 1) * entries], 1, 0)
            parts.append(back[g * entries : (g + 1) * entries] + jnp.where(first, 0.0, shifted))
        inner = gelu(jnp.concatenate(parts, axis=0)).astype(bf16)
        results.append(dot_t(inner, jnp.concatenate([outer[...], outer[...]], axis=0)))
    for g in range(2):
        part = slice(g * entries, (g + 1) * entries)
        key = turn(results[0][part], cosine_e, sine_e)
        ents[me, part, :] = jnp.where(low_e, key, results[1][part]).astype(bf16)
    for d in range(1, n):
        send(
            ents.at[me], ents.at[me], ent_send.at[d - 1], ent_recv.at[me],
            {"kv": (me + d) % n}, me + d < n,
        )

    for load in loads[10:14]:
        load.wait()
    hidden = rows[...]
    for i in range(half):
        made = dot(hidden, wq[:, i * 128 : (i + 1) * 128])
        g, h = (2 * i) // half, (2 * i) % half
        turned = [
            turn(made[s * span : (s + 1) * span], cosine, sine) * (HEAD_DIM**-0.5)
            for s in range(seqs)
        ]
        for p in range(pairs):
            a, b = turned[2 * p], turned[2 * p + 1]
            even, odd = jnp.where(low, a, swap(b)), jnp.where(low, swap(a), b)
            lanes = slice(p * 128, (p + 1) * 128)
            qn[g, h * span : (h + 1) * span, lanes] = even.astype(bf16)
            qn[g, (h + 1) * span : (h + 2) * span, lanes] = odd.astype(bf16)
    spread = 2 * wg_ref.shape[1]
    logits = dot_t(wg[...].reshape(spread, rows.shape[1]), hidden)
    wide_at = lax.broadcasted_iota(jnp.int32, (1, seqs * span), 1)
    limit = jnp.zeros((1, seqs * span), jnp.int32)
    for s in range(seqs):
        limit = jnp.where(wide_at // span == s, lens[:, s : s + 1], limit)
    live = me * span + wide_at % span < limit
    for branch in range(2):
        base = branch * (spread // 2)
        mine = jnp.where(
            column == 0, logits[base : base + heads], logits[base + heads : base + 2 * heads]
        )
        mine = jnp.where(live, jax.nn.sigmoid(mine), 0.0)
        turned = [mine[:, p * 128 : (p + 1) * 128] for p in range(pairs)]
        swapped = [swap(t) for t in turned]
        for g in range(2):
            for s in range(seqs):
                for j in range(half // 2):
                    one = slice(g * half + 2 * j, g * half + 2 * j + 1)
                    two = slice(g * half + 2 * j + 1, g * half + 2 * j + 2)
                    t, w = turned[s // 2], swapped[s // 2]
                    if s % 2 == 0:
                        row = jnp.where(low_row, t[one], w[two])
                    else:
                        row = jnp.where(low_row, w[one], t[two])
                    number = (branch * 2 + g) * seqs + s
                    gate_buf[number : number + 1, j * 128 : (j + 1) * 128] = row

    named = jnp.zeros((2 * seqs, TOPK), f32)
    for d in range(1, n):
        origin = (me + d) % n
        pltpu.make_async_remote_copy(
            src_ref=picks, dst_ref=lists.at[origin], send_sem=pick_send.at[d - 1],
            recv_sem=pick_recv.at[origin], device_id={"kv": origin}, device_id_type=mesh_id,
        ).wait_recv()
        named = jnp.where(lists[origin] == me, 1.0, named)
    named = jnp.max(jnp.where(slot_at == 0, 0.0, named), axis=1, keepdims=True)
    named = jnp.broadcast_to(named, (2 * seqs, 128))
    key = jnp.zeros((span, 128), f32)
    for s in range(seqs):
        flag = jnp.where(low_row, named[2 * s : 2 * s + 1], named[2 * s + 1 : 2 * s + 2])
        key = key + flag * sk_buf[s * span : (s + 1) * span, :].astype(f32)
    for g in range(2):
        value = jnp.zeros((HEAD_DIM, 128), f32)
        for p in range(pairs):
            r0, r1 = 4 * p + g, 4 * p + 2 + g
            flag = jnp.where(low_row, named[r0 : r0 + 1], named[r1 : r1 + 1])
            block = svt[g * HEAD_DIM : (g + 1) * HEAD_DIM, p * 128 : (p + 1) * 128]
            value = value + flag * block.astype(f32)
        value = value + swap(value)
        blobs[g, me] = jnp.where(low, key if g == 0 else swap(key), value).astype(bf16)

    number = [0]

    def pass_on(g, slot, dst, when=None):
        ref = blobs.at[g, slot]
        send(ref, ref, blob_send.at[number[0]], blob_recv.at[g, slot], {"kv": dst}, when)
        number[0] += 1

    def arrived(g, slot):
        ref = blobs.at[g, slot]
        pltpu.make_async_remote_copy(
            src_ref=ref, dst_ref=ref, send_sem=blob_send.at[0],
            recv_sem=blob_recv.at[g, slot], device_id={"kv": (me + 1) % n}, device_id_type=mesh_id,
        ).wait_recv()

    across = z * PLANE + (1 - x) * 2 + c
    beside = z * PLANE + x * 2 + (1 - c)
    side_slot = x * 2 + c
    across_slot = (1 - x) * 2 + c
    for g in range(2):
        for d in range(planes - 1, 0, -1):
            pass_on(g, me, me + d * PLANE, z + d < planes)
        pass_on(g, me, across)
        pass_on(g, me, beside)

    def from_below(g, d):
        slot = jnp.maximum(z - d, 0) * PLANE + side_slot
        pl.when(z >= d)(lambda: arrived(g, slot))
        pass_on(g, slot, across, z >= d)
        pass_on(g, slot, beside, z >= d)

    def from_across(g, d):
        slot = jnp.maximum(z - d, 0) * PLANE + across_slot
        if d == 0:
            arrived(g, slot)
            pass_on(g, slot, beside)
        else:
            pl.when(z >= d)(lambda: arrived(g, slot))
            pass_on(g, slot, beside, z >= d)

    def from_beside(g):
        for d in range(planes):
            for column_x in (x, 1 - x):
                slot = jnp.maximum(z - d, 0) * PLANE + column_x * 2 + (1 - c)
                if d == 0:
                    arrived(g, slot)
                else:
                    pl.when(z >= d)(functools.partial(arrived, g, slot))

    key_at = lax.broadcasted_iota(jnp.int32, (span, across_q), 0)
    query_at = lax.broadcasted_iota(jnp.int32, (span, across_q), 1) % span
    near_bias = jnp.where(key_at <= query_at, 0.0, FAR)
    seq_lane = lax.broadcasted_iota(jnp.int32, (HEAD_DIM, seqs * span), 1) // span
    ones_at = lax.broadcasted_iota(jnp.int32, (16, seqs * span), 0)
    ones_lane = lax.broadcasted_iota(jnp.int32, (16, seqs * span), 1) // span
    near_keys = seqs * span
    near_top = {}

    def near_part(g):
        for s in range(seqs):
            block = sk_buf[s * span : (s + 1) * span, :].astype(f32)
            if g != s % 2:
                block = swap(block)
            block = jnp.where(low if s % 2 == 0 else ~low, block, 0.0).astype(bf16)
            lanes = slice((s // 2) * 128, (s // 2 + 1) * 128)
            score = dot_t(block, qn[g, :, lanes]) + near_bias
            near_s[g, s * span : (s + 1) * span, :] = score
            near_top[g, s] = jnp.max(score.reshape(span // 8, 8, across_q), axis=0)
            value = svt[g * HEAD_DIM : (g + 1) * HEAD_DIM, :].astype(f32)
            vals[g, s * HEAD_DIM : (s + 1) * HEAD_DIM, 0:near_keys] = jnp.where(
                seq_lane == s, value, 0.0
            ).astype(bf16)
        vals[g, stack : stack + 16, 0:near_keys] = jnp.where(
            ones_at == ones_lane, 1.0, 0.0
        ).astype(bf16)

    slots = n * entries
    entry_row = lax.broadcasted_iota(jnp.int32, (slots, 128), 0)
    entry_half = lax.broadcasted_iota(jnp.int32, (slots, 128), 1) // HEAD_DIM
    entry_seq = (entry_row % entries) // count
    slot_row = lax.broadcasted_iota(jnp.int32, (slots, across_q), 0)
    slot_query = lax.broadcasted_iota(jnp.int32, (slots, across_q), 1) % span
    slot_entry = (slot_row // entries) * count + slot_row % count
    entry_ok = (slot_entry >= 1) & (
        slot_entry * CMP_STRIDE + CMP_STRIDE - 1 <= me * span + slot_query
    )
    entry_bias = jnp.where(entry_ok, 0.0, FAR)
    value_lane = (lax.broadcasted_iota(jnp.int32, (HEAD_DIM, slots), 1) % entries) // count
    total_row = lax.broadcasted_iota(jnp.int32, (16, slots), 0)
    total_lane = (lax.broadcasted_iota(jnp.int32, (16, slots), 1) % entries) // count
    group_row = lax.broadcasted_iota(jnp.int32, (entries, across_q), 0)

    def wait_entries():
        for b in range(n):
            @pl.when(b < me)
            def _():
                pltpu.make_async_remote_copy(
                    src_ref=ents.at[b], dst_ref=ents.at[b], send_sem=ent_send.at[0],
                    recv_sem=ent_recv.at[b], device_id={"kv": (me + 1) % n},
                    device_id_type=mesh_id,
                ).wait_recv()

    def cmp_part(g):
        part = slice(g * entries, (g + 1) * entries)
        both = ents[:, part, :].reshape(slots, 128).astype(f32)
        twice = jnp.where(entry_half == 0, both, swap(both))
        keys = jnp.concatenate(
            [jnp.where(entry_seq == 2 * p + entry_half, twice, 0.0) for p in range(pairs)], axis=1
        ).astype(bf16)
        score = (dot_t(keys, qn[g]) + entry_bias).reshape(n, entries, across_q)
        top = jnp.max(score, axis=0)
        for step in (1, 2):
            top = jnp.maximum(
                top,
                jnp.where(
                    (group_row // step) % 2 == 0,
                    pltpu.roll(top, entries - step, 0),
                    pltpu.roll(top, step, 0),
                ),
            )
        top = jnp.maximum(top, -1e29)
        w = jnp.exp(score - top[None]).reshape(slots, across_q).astype(bf16)
        value = jnp.transpose(both)[HEAD_DIM:]
        left = [jnp.where(value_lane == s, value, 0.0) for s in range(seqs)]
        left.append(jnp.where(total_row == total_lane, 1.0, 0.0))
        made = dot(jnp.concatenate(left, axis=0).astype(bf16), w)
        for s in range(seqs):
            total = jnp.maximum(made[stack + s : stack + s + 1], 1.0)
            row = g * seqs + s
            factor = gate_buf[row : row + 1, :] / total
            block = slice(s * HEAD_DIM, (s + 1) * HEAD_DIM)
            mix[g, block, :] = made[block] * factor

    def far_part(g):
        tops = []
        for plane in range(planes):
            left = []
            for i in range(PLANE):
                b = plane * PLANE + i
                block = blobs[g, b].astype(f32)
                turned = swap(block)
                twice = jnp.where(low, block, turned)
                tiles = []
                for p in range(pairs):
                    r0, r1 = 4 * p + g, 4 * p + 2 + g
                    flag = jnp.where(low_row, hits[b, r0 : r0 + 1], hits[b, r1 : r1 + 1])
                    tiles.append(twice * flag)
                left.append(jnp.concatenate(tiles, axis=1))
                if i % 2 == 0:
                    before = turned
                else:
                    value = jnp.where(low, before, block)
                    lanes = slice(near_keys + (b - 1) * span, near_keys + (b + 1) * span)
                    for s in range(seqs):
                        r = 2 * s + g
                        flag = jnp.where(low_row, hits[b - 1, r : r + 1], hits[b, r : r + 1])
                        vals[g, s * HEAD_DIM : (s + 1) * HEAD_DIM, lanes] = (value * flag).astype(
                            bf16
                        )
                    flags = [
                        jnp.where(low_row, hits[b - 1, r : r + 1], hits[b, r : r + 1])
                        for r in range(g, 2 * seqs, 2)
                    ]
                    flags.append(jnp.zeros((16 - seqs, 128), f32))
                    vals[g, stack : stack + 16, lanes] = jnp.concatenate(flags, axis=0).astype(bf16)
            score = dot_t(jnp.concatenate(left, axis=0).astype(bf16), qn[g])
            far_s[plane * PLANE * span : (plane + 1) * PLANE * span, :] = score
            for i in range(PLANE):
                block = score[i * span : (i + 1) * span].reshape(span // 8, 8, across_q)
                tops.append(jnp.max(block, axis=0))
        wide_hits = [jnp.concatenate([hits[b], hits[b]], axis=1) for b in range(n)]
        refs = [jnp.full((1, across_q), 1e30, f32) for _ in range(n)]
        for s in range(seqs):
            r = 2 * s + g
            top = near_top[g, s]
            for b in range(n):
                top = jnp.maximum(top, jnp.where(wide_hits[b][r : r + 1] > 0, tops[b], FAR))
            top = jnp.max(top, axis=0, keepdims=True)
            for b in range(n):
                refs[b] = jnp.where(wide_hits[b][r : r + 1] > 0, top, refs[b])
            part = slice(s * span, (s + 1) * span)
            probs[part, :] = jnp.exp(near_s[g, part, :] - top).astype(bf16)
        for b in range(n):
            part = slice(b * span, (b + 1) * span)
            block = jnp.exp(far_s[part, :] - refs[b]).astype(bf16)
            probs[near_keys + b * span : near_keys + (b + 1) * span, :] = block
        made = dot(vals[g], probs[...])
        for p in range(pairs):
            tiles = []
            for s in (2 * p, 2 * p + 1):
                row = (2 + g) * seqs + s
                total = jnp.maximum(made[stack + s : stack + s + 1], 1.0)
                factor = gate_buf[row : row + 1, :] / total
                block = slice(s * HEAD_DIM, (s + 1) * HEAD_DIM)
                tiles.append(mix[g, block, :] + made[block] * factor)
            both = jnp.concatenate(tiles, axis=0)
            for j in range(half // 2):
                lanes = slice(j * 128, (j + 1) * 128)
                flipped = jnp.transpose(both[:, lanes])
                a, b = flipped[:span], flipped[span:]
                part = slice(2 * p * span, (2 * p + 1) * span)
                own[g, part, lanes] = jnp.where(low, a, swap(b)).astype(bf16)
                part = slice((2 * p + 1) * span, (2 * p + 2) * span)
                own[g, part, lanes] = jnp.where(low, swap(a), b).astype(bf16)
            for s in (2 * p, 2 * p + 1):
                piece(g, s).start()

    def piece(g, s):
        part = pl.ds(s * span, span)
        return pltpu.make_async_remote_copy(
            src_ref=own.at[g, part], dst_ref=other.at[g, part], send_sem=half_send.at[g, s],
            recv_sem=half_recv.at[g, s], device_id={"tp": 1 - column}, device_id_type=mesh_id,
        )

    for g in range(2):
        near_part(g)
    from_across(0, 0)
    if planes > 1:
        from_below(0, 1)
    from_across(1, 0)
    for d in range(2, planes):
        from_below(0, d)
        from_below(1, d - 1)
    wait_entries()
    cmp_part(0)
    for d in range(1, planes):
        from_across(0, d)
        if d == planes - 2:
            from_below(1, planes - 1)
    for d in range(1, planes - 1):
        from_across(1, d)
    if planes == 2:
        from_below(1, 1)
    from_beside(0)
    far_part(0)
    from_across(1, planes - 1)
    for load in loads[14:]:
        load.wait()
    cmp_part(1)
    from_beside(1)
    far_part(1)

    squares = jnp.zeros((seqs * span, 1), f32)
    total = jnp.zeros((seqs * span, wide), f32)
    group = half * HEAD_DIM

    def gains(side, g):
        return gain[:, pl.ds(pl.multiple_of(side * depth + g * group, group), group)]

    for g in range(2):
        a = own[g].astype(f32)
        squares = squares + jnp.sum(a * a, axis=1, keepdims=True)
        scaled = (a * gains(column, g)).astype(bf16)
        total = total + dot(scaled, weight[0, g * group : (g + 1) * group, :])
    for s in range(seqs):
        piece(0, s).wait_recv()
    a = other[0].astype(f32)
    squares = squares + jnp.sum(a * a, axis=1, keepdims=True)
    scaled = (a * gains(1 - column, 0)).astype(bf16)
    partial[...] = total + dot(scaled, weight[1, :group, :])
    for s in range(seqs):
        piece(1, s).wait_recv()
        part = slice(s * span, (s + 1) * span)
        a = other[1, part, :].astype(f32)
        square = squares[part] + jnp.sum(a * a, axis=1, keepdims=True)
        row_scale = lax.rsqrt(square / (2 * depth) + norm_eps)
        scaled = (a * gains(1 - column, 1)).astype(bf16)
        done = partial[part, :] + dot(scaled, weight[1, group:, :])
        out_ref[part, :] = (done * row_scale).astype(bf16)

    for g in range(2):
        for s in range(seqs):
            piece(g, s).wait_send()
    for copy, when in sent:
        if when is None:
            copy.wait_send()
        else:
            pl.when(when)(copy.wait_send)


def fused_shards(
    hidden_in,
    w_query,
    w_cmp_key,
    w_cmp_value,
    w_sel_key,
    w_sel_value,
    w_gate,
    cmp_key_in,
    cmp_key_out,
    cmp_value_in,
    cmp_value_out,
    out_gain,
    w_out,
    seq_lengths,
    chosen,
):
    seqs, span, width = hidden_in.shape
    n = lax.axis_size("kv")
    heads = w_query.shape[1] // HEAD_DIM
    total = seqs * span
    entries = total // CMP_STRIDE
    out_width = width // lax.axis_size("tp")
    small = w_sel_key.shape[1]
    half = heads // 2
    stack = seqs * HEAD_DIM
    across_q = half * span
    planes = n // PLANE
    anywhere = pl.BlockSpec(memory_space=pl.ANY)
    gate_rows = jnp.transpose(w_gate, (1, 2, 0))
    picks = chosen[:, 0].reshape(2 * seqs, TOPK)
    key_out, value_out = jnp.transpose(cmp_key_out), jnp.transpose(cmp_value_out)
    lens = seq_lengths[None]
    gain = out_gain[None]
    blob_sends = 2 * (planes + 1) + 2 * (2 * (planes - 1) + planes)
    out = pl.pallas_call(
        functools.partial(layer_kernel, n, seqs, span, heads),
        in_specs=[anywhere] * 15,
        out_specs=pl.BlockSpec(memory_space=pltpu.VMEM),
        out_shape=pltpu.VMEM((total, out_width), bf16),
        scratch_shapes=[
            pltpu.VMEM(picks.shape, jnp.int32),
            pltpu.VMEM((total, width), bf16),
            pltpu.VMEM((width, 4 * small), bf16),
            pltpu.VMEM(key_out.shape, bf16),
            pltpu.VMEM(value_out.shape, bf16),
            pltpu.VMEM(cmp_key_in.shape, bf16),
            pltpu.VMEM(cmp_value_in.shape, bf16),
            pltpu.VMEM(w_query.shape, bf16),
            pltpu.VMEM(gate_rows.shape, bf16),
            pltpu.VMEM(lens.shape, jnp.int32),
            pltpu.VMEM(gain.shape, f32),
            pltpu.VMEM((2, heads * HEAD_DIM, out_width), bf16),
            pltpu.VMEM((2, across_q, stack), bf16),
            pltpu.VMEM((total, small), bf16),
            pltpu.VMEM((small, total), bf16),
            pltpu.VMEM((2, total, small), f32),
            pltpu.VMEM((4 * seqs, across_q), f32),
            pltpu.VMEM((n, 2 * seqs, 128), f32),
            pltpu.VMEM((n,) + picks.shape, jnp.int32),
            pltpu.VMEM((n, 2 * entries, 128), bf16),
            pltpu.VMEM((2, n, span, 128), bf16),
            pltpu.VMEM((2, total, across_q), f32),
            pltpu.VMEM((n * span, across_q), f32),
            pltpu.VMEM((total + n * span, across_q), bf16),
            pltpu.VMEM((2, stack + 16, total + n * span), bf16),
            pltpu.VMEM((2, stack, across_q), f32),
            pltpu.VMEM((2, total, half * HEAD_DIM), bf16),
            pltpu.VMEM((2, total, half * HEAD_DIM), bf16),
            pltpu.VMEM((total, out_width), f32),
            pltpu.SemaphoreType.DMA((16,)),
            pltpu.SemaphoreType.DMA((n,)),
            pltpu.SemaphoreType.DMA((n,)),
            pltpu.SemaphoreType.DMA((n,)),
            pltpu.SemaphoreType.DMA((n,)),
            pltpu.SemaphoreType.DMA((blob_sends,)),
            pltpu.SemaphoreType.DMA((2, n)),
            pltpu.SemaphoreType.DMA((2, seqs)),
            pltpu.SemaphoreType.DMA((2, seqs)),
        ],
        compiler_params=pltpu.CompilerParams(
            collective_id=0, has_side_effects=True, vmem_limit_bytes=VMEM_BYTES
        ),
        name="layer",
    )(
        picks, hidden_in.reshape(total, width), w_sel_key, w_sel_value, w_cmp_key, w_cmp_value,
        key_out, value_out, cmp_key_in, cmp_value_in, w_query, gate_rows, lens, gain, w_out,
    )
    return out.reshape(seqs, span, out_width)


def fits(mesh):
    n = mesh.shape["kv"]
    return mesh.shape["tp"] == 2 and n % PLANE == 0 and n <= 32


def solution(mesh):
    placed = (
        P(None, "kv", None),
        P(None, "tp"),
        P(None, "tp"),
        P(None, "tp"),
        P(None, "tp"),
        P(None, "tp"),
        P(),
        P(),
        P(),
        P(),
        P(),
        P(),
        P(),
        P(),
        P(None, "kv", "tp", None),
    )
    return jax.shard_map(
        fused_shards if fits(mesh) else shards, mesh=mesh, in_specs=placed, out_specs=P(None, "kv", "tp"), check_vma=False
    )
```

```python
import functools
import math

import jax
import jax.numpy as jnp
from jax import lax
from jax.experimental import pallas as pl
from jax.experimental.pallas import tpu as pltpu
from jax.sharding import PartitionSpec as P

HEADS = 16
HEAD_DIM = 64
CMP_STRIDE = 16
CMP_BLOCK = 32
TOPK = 16


theta_base = 500000.0
norm_eps = 1e-06


def rotate(values, positions):
    width = values.shape[-1]
    half = width // 2
    inverse = jnp.exp(
        -jnp.log(jnp.float32(theta_base)) * jnp.arange(0, width, 2).astype(jnp.float32) / width
    )
    angle = positions.astype(jnp.float32)[:, None] * inverse[None, :]
    cosine = jnp.cos(angle)[:, None, :]
    sine = jnp.sin(angle)[:, None, :]
    first = values[..., :half]
    second = values[..., half:]
    return jnp.concatenate(
        [first * cosine - second * sine, second * cosine + first * sine], axis=-1
    )


def masked_weights(scores, valid):
    top = jnp.max(jnp.where(valid, scores, -1e30), axis=-1, keepdims=True)
    expd = jnp.where(valid, jnp.exp(scores - top), 0.0)
    total = jnp.sum(expd, axis=-1, keepdims=True)
    return (expd / jnp.maximum(total, 1.0)).astype(jnp.bfloat16)


def compress(raw, prior, weight_in, weight_out):
    seqs, span, groups, width = raw.shape
    extended = jnp.concatenate([prior, raw], axis=1)
    count = span // CMP_STRIDE
    front = extended[:, :span].reshape(seqs, count, CMP_STRIDE, groups, width)
    back = extended[:, CMP_STRIDE:].reshape(seqs, count, CMP_STRIDE, groups, width)
    window = jnp.concatenate([front, back], axis=2).transpose(0, 1, 3, 2, 4)
    window = window.reshape(seqs * count * groups, CMP_BLOCK * width)
    inner = jax.nn.gelu(jnp.dot(window, weight_in, preferred_element_type=jnp.float32)).astype(
        jnp.bfloat16
    )
    return jnp.dot(inner, weight_out, preferred_element_type=jnp.float32).reshape(
        seqs, count, groups, width
    )


def shards(
    hidden_in,
    w_query,
    w_cmp_key,
    w_cmp_value,
    w_sel_key,
    w_sel_value,
    w_gate,
    cmp_key_in,
    cmp_key_out,
    cmp_value_in,
    cmp_value_out,
    out_gain,
    w_out,
    seq_lengths,
    chosen,
):
    seqs, span, width = hidden_in.shape
    block_list = lax.axis_size("kv")
    place = lax.axis_index("kv")
    column = lax.axis_index("tp")
    local_heads = w_query.shape[1] // HEAD_DIM
    local_groups = w_sel_key.shape[1] // HEAD_DIM
    per_group = local_heads // local_groups
    count = span // CMP_STRIDE
    scale = HEAD_DIM ** (-0.5)
    rows = hidden_in.reshape(seqs * span, width)
    positions = place * span + jnp.arange(span, dtype=jnp.int32)

    def project(weight_matrix, heads):
        return jnp.dot(rows, weight_matrix, preferred_element_type=jnp.float32).reshape(
            seqs, span, heads, HEAD_DIM
        )

    queries = rotate(project(w_query, local_heads), positions).astype(jnp.bfloat16)
    sel_pairs = jnp.concatenate(
        [rotate(project(w_sel_key, local_groups), positions), project(w_sel_value, local_groups)],
        axis=-1,
    ).astype(jnp.bfloat16)
    raw_pairs = jnp.concatenate(
        [project(w_cmp_key, local_groups), project(w_cmp_value, local_groups)], axis=-1
    ).astype(jnp.bfloat16)
    prior = jnp.zeros((seqs, CMP_STRIDE, local_groups, HEAD_DIM), jnp.bfloat16)
    ends = place * span + jnp.arange(count, dtype=jnp.int32) * CMP_STRIDE + CMP_STRIDE - 1
    cmp_keys = rotate(compress(raw_pairs[..., :HEAD_DIM], prior, cmp_key_in, cmp_key_out), ends)
    cmp_values = compress(raw_pairs[..., HEAD_DIM:], prior, cmp_value_in, cmp_value_out)
    cmp_piece = jnp.concatenate(
        [cmp_keys.astype(jnp.bfloat16), cmp_values.astype(jnp.bfloat16)], axis=-1
    )[:, None]
    picks = chosen[:, 0]
    every_list = lax.all_gather(picks[None, :, :, 1:], "kv", axis=0, tiled=True)
    named = jnp.any(every_list == place, axis=(0, 3)).astype(jnp.int32)
    seq_ids = jnp.arange(seqs, dtype=jnp.int32)[:, None]
    exported_seq = jnp.sum(named * seq_ids, axis=0)
    selector = seq_ids == exported_seq[None, :]
    export = jnp.sum(
        jnp.where(selector[:, None, :, None], sel_pairs, jnp.zeros((), jnp.bfloat16)), axis=0
    )
    export = export[None]
    remote_pairs, remote_entries = (
        lax.all_gather(export, "kv", axis=0, tiled=True),
        lax.all_gather(cmp_piece, "kv", axis=1, tiled=True),
    )
    gate_all = jnp.dot(rows, w_gate.reshape(width, 2 * HEADS), preferred_element_type=jnp.float32)
    gate_all = gate_all.reshape(seqs, span, 2, HEADS)
    gates = jax.nn.sigmoid(lax.dynamic_slice_in_dim(gate_all, column * local_heads, local_heads, 3))
    entry = jnp.arange(block_list * count, dtype=jnp.int32)
    entry_end = entry * CMP_STRIDE + CMP_STRIDE - 1
    cmp_valid = ((entry >= 1)[None, :] & (entry_end[None, :] <= positions[:, None]))[None, None]
    key_pos = jnp.arange(span, dtype=jnp.int32)
    own_valid = key_pos[None, :] <= key_pos[:, None]

    def one_sequence(args):
        seq_queries, seq_entries, seq_picks, seq_pairs, seq_gates, seq_length = args
        block_q = seq_queries.reshape(span, local_groups, per_group, HEAD_DIM)
        entries = seq_entries.reshape(block_list * count, local_groups, 2 * HEAD_DIM)
        scores = (
            jnp.einsum(
                "qghd,egd->ghqe",
                block_q,
                entries[..., :HEAD_DIM],
                preferred_element_type=jnp.float32,
            )
            * scale
        )
        weights = masked_weights(scores, cmp_valid)
        cmp_out = jnp.einsum(
            "ghqe,egd->qghd", weights, entries[..., HEAD_DIM:], preferred_element_type=jnp.float32
        )
        far = jnp.maximum(seq_picks[:, 1:], 0)
        fetched = jax.vmap(lambda table, index: table[index], in_axes=(2, 0))(remote_pairs, far)
        near = jnp.transpose(seq_pairs, (1, 0, 2))[:, None]
        pairs = jnp.concatenate([near, fetched], axis=1).reshape(
            local_groups, TOPK * span, 2 * HEAD_DIM
        )
        far_live = jnp.broadcast_to(
            (seq_picks[:, 1:] >= 0)[:, None, :, None], (local_groups, span, TOPK - 1, span)
        )
        near_live = jnp.broadcast_to(own_valid[None, :, None, :], (local_groups, span, 1, span))
        sel_valid = jnp.concatenate([near_live, far_live], axis=2).reshape(
            local_groups, 1, span, TOPK * span
        )
        scores_s = (
            jnp.einsum(
                "qghd,gmd->ghqm", block_q, pairs[..., :HEAD_DIM], preferred_element_type=jnp.float32
            )
            * scale
        )
        weights_s = masked_weights(scores_s, sel_valid)
        sel_out = jnp.einsum(
            "ghqm,gmd->qghd", weights_s, pairs[..., HEAD_DIM:], preferred_element_type=jnp.float32
        )
        split = seq_gates.reshape(span, 2, local_groups, per_group, 1)
        mixed = split[:, 0] * cmp_out + split[:, 1] * sel_out
        mixed = jnp.where((positions < seq_length)[:, None, None, None], mixed, 0.0)
        return mixed.reshape(span, local_heads * HEAD_DIM).astype(jnp.bfloat16)

    mixed = lax.map(one_sequence, (queries, remote_entries, picks, sel_pairs, gates, seq_lengths))
    mixed = mixed.reshape(seqs * span, local_heads * HEAD_DIM)
    out_width = width // lax.axis_size("tp")
    own_columns = lax.dynamic_slice_in_dim(w_out, column * out_width, out_width, 1)
    piece_wide = lax.all_gather(mixed, "tp", axis=1, tiled=True).astype(jnp.float32)
    scaled_piece = (piece_wide * out_gain[None, :]).astype(jnp.bfloat16)
    total = jnp.dot(scaled_piece, own_columns, preferred_element_type=jnp.float32)
    squares = jnp.sum(piece_wide * piece_wide, axis=-1)
    row_scale = lax.rsqrt(squares / (HEADS * HEAD_DIM) + norm_eps)
    return (total * row_scale[:, None]).astype(jnp.bfloat16).reshape(seqs, span, out_width)


FAR = -1e30
PLANE = 4
VMEM_BYTES = 60 * 1024 * 1024
f32 = jnp.float32
bf16 = jnp.bfloat16


def dot(a, b):
    return jnp.dot(a, b, preferred_element_type=f32)


def dot_t(a, b):
    return lax.dot_general(a, b, (((1,), (1,)), ((), ())), preferred_element_type=f32)


def swap(values):
    return pltpu.roll(values, HEAD_DIM, 1)


def turn(values, cosine, sine):
    lane = lax.broadcasted_iota(jnp.int32, values.shape, 1)
    other = jnp.where(
        lane % HEAD_DIM < HEAD_DIM // 2,
        pltpu.roll(values, 128 - HEAD_DIM // 2, 1),
        pltpu.roll(values, HEAD_DIM // 2, 1),
    )
    return values * cosine + other * sine


def gelu(x):
    return 0.5 * x * (1.0 + jnp.tanh(0.7978845608028654 * (x + 0.044715 * (x * x * x))))


def layer_kernel(
    n, seqs, span, heads,
    picks_ref, rows_ref, wsk_ref, wsv_ref, wck_ref, wcv_ref, kout_ref, vout_ref, kin_ref, vin_ref,
    wq_ref, wg_ref, lens_ref, gain_ref, wout_ref,
    out_ref,
    picks, rows, ws, kout, vout, kin, vin, wq, wg, lens, gain, weight,
    qn, sk_buf, svt, raw, gate_buf, hits, lists, named_buf, ents, blobs, near_s, far_s, tops, base_top,
    probs, base_sum, vals, mix, own, other, partial,
    load_sem, pick_send, pick_recv, ent_send, ent_recv, blob_send, blob_recv, half_send, half_recv,
):
    me = lax.axis_index("kv")
    column = lax.axis_index("tp")
    planes = n // PLANE
    z, x, c = me // PLANE, (me // 2) % 2, me % 2
    depth = heads * HEAD_DIM
    wide = out_ref.shape[1]
    count = span // CMP_STRIDE
    entries = seqs * count
    half = heads // 2
    stack = seqs * HEAD_DIM
    across_q = half * span
    pairs = seqs // 2
    mesh_id = pl.DeviceIdType.MESH

    barrier = pltpu.get_barrier_semaphore()
    for d in range(1, n):
        pl.semaphore_signal(
            barrier, inc=1, device_id={"kv": (me + d) % n}, device_id_type=mesh_id
        )
    pl.semaphore_signal(barrier, inc=1, device_id={"tp": 1 - column}, device_id_type=mesh_id)

    jobs = [(picks_ref, picks), (rows_ref, rows)]
    for i, ref in enumerate((wsk_ref, wsv_ref, wck_ref, wcv_ref)):
        jobs.append((ref, ws.at[:, i * 128 : (i + 1) * 128]))
    jobs += [(kout_ref, kout), (vout_ref, vout), (kin_ref, kin), (vin_ref, vin)]
    jobs += [(wq_ref, wq), (wg_ref, wg), (lens_ref, lens), (gain_ref, gain)]
    for i in range(2):
        side = column if i == 0 else 1 - column
        block = wout_ref.at[
            pl.ds(pl.multiple_of(side * depth, depth), depth),
            pl.ds(pl.multiple_of(column * wide, wide), wide),
        ]
        jobs.append((block, weight.at[i]))
    loads = [pltpu.make_async_copy(a, b, load_sem.at[i]) for i, (a, b) in enumerate(jobs)]
    for load in loads:
        load.start()

    lane = lax.broadcasted_iota(jnp.int32, (span, 128), 1)
    low = lane < HEAD_DIM
    low_e = low[:entries]
    low_row = low[:1]
    at = lax.broadcasted_iota(jnp.int32, (span, 128), 0)
    sign = jnp.where(lane % HEAD_DIM < HEAD_DIM // 2, -1.0, 1.0)
    power = (lane % (HEAD_DIM // 2) * 2).astype(f32)
    freq = jnp.exp(-math.log(theta_base) * power / HEAD_DIM)
    angle = (me * span + at).astype(f32) * freq
    cosine = jnp.cos(angle)
    sine = jnp.sin(angle) * sign
    end = me * span + (at[:entries] % count) * CMP_STRIDE + CMP_STRIDE - 1
    angle = end.astype(f32) * freq[:entries]
    cosine_e = jnp.cos(angle)
    sine_e = jnp.sin(angle) * sign[:entries]

    near_keys = seqs * span
    plane_keys = PLANE * span

    def value_lanes(plane):
        start = near_keys + (plane + planes - 1) % planes * plane_keys
        return slice(start, start + plane_keys)

    for plane in range(1, planes):
        @pl.when(plane > z)
        def _():
            for i in range(PLANE):
                ents[plane * PLANE + i] = jnp.zeros((2 * entries, 128), bf16)
            keys = slice(plane * plane_keys, (plane + 1) * plane_keys)
            lanes = value_lanes(plane)
            for g in range(2):
                far_s[g, keys, :] = jnp.zeros((plane_keys, across_q), f32)
                vals[g, :, lanes] = jnp.zeros((stack + 16, plane_keys), bf16)
                tops[g, plane * PLANE : (plane + 1) * PLANE] = jnp.zeros(
                    (PLANE, 8, across_q), f32
                )

    loads[0].wait()
    pl.semaphore_wait(barrier, n)
    sent = []

    def send(src, dst, ssem, rsem, target, when=None):
        copy = pltpu.make_async_remote_copy(
            src_ref=src, dst_ref=dst, send_sem=ssem, recv_sem=rsem,
            device_id=target, device_id_type=mesh_id,
        )
        if when is None:
            copy.start()
        else:
            pl.when(when)(copy.start)
        sent.append((copy, when))

    for d in range(n - 1, 0, -1):
        send(
            picks, lists.at[me], pick_send.at[d - 1], pick_recv.at[me],
            {"kv": (me + n - d) % n}, me >= d,
        )

    slot_at = lax.broadcasted_iota(jnp.int32, (2 * seqs, TOPK), 1)
    listed = jnp.where(slot_at == 0, -1, picks[...])
    for b in range(n):
        hit = jnp.max(jnp.where(listed == b, 1.0, 0.0), axis=1, keepdims=True)
        hits[b] = jnp.broadcast_to(hit, (2 * seqs, 128))
    named_buf[...] = jnp.zeros((2 * seqs, TOPK), f32)

    for load in loads[1:6]:
        load.wait()
    made = dot(rows[...], ws[...])
    sv = []
    for s in range(seqs):
        part = slice(s * span, (s + 1) * span)
        sk_buf[part, :] = turn(made[part, :128], cosine, sine).astype(bf16)
    svt[...] = jnp.transpose(made[:, 128:256]).astype(bf16)
    raw[0] = made[:, 256:384].astype(bf16).astype(f32)
    raw[1] = made[:, 384:512].astype(bf16).astype(f32)
    first = at[:entries] % count == 0
    mid = CMP_STRIDE * HEAD_DIM
    results = []
    for load in loads[6:10]:
        load.wait()
    for branch, inner_weight, outer in ((0, kin, kout), (1, vin, vout)):
        left, right = [], []
        for j in range(0, CMP_STRIDE, 2):
            a = raw[branch, pl.ds(j, entries, stride=CMP_STRIDE), :]
            b = raw[branch, pl.ds(j + 1, entries, stride=CMP_STRIDE), :]
            left.append(jnp.where(low_e, a, swap(b)))
            right.append(jnp.where(low_e, swap(a), b))
        window = jnp.concatenate(
            [jnp.concatenate(left, axis=1), jnp.concatenate(right, axis=1)], axis=0
        ).astype(bf16)
        front = dot(window, inner_weight[:mid])
        back = dot(window, inner_weight[mid:])
        parts = []
        for g in range(2):
            shifted = pltpu.roll(front[g * entries : (g + 1) * entries], 1, 0)
            parts.append(back[g * entries : (g + 1) * entries] + jnp.where(first, 0.0, shifted))
        inner = gelu(jnp.concatenate(parts, axis=0)).astype(bf16)
        results.append(dot_t(inner, jnp.concatenate([outer[...], outer[...]], axis=0)))
    for g in range(2):
        part = slice(g * entries, (g + 1) * entries)
        key = turn(results[0][part], cosine_e, sine_e)
        ents[me, part, :] = jnp.where(low_e, key, results[1][part]).astype(bf16)
    across = z * PLANE + (1 - x) * 2 + c
    beside = z * PLANE + x * 2 + (1 - c)
    side_slot = x * 2 + c
    across_slot = (1 - x) * 2 + c
    ent_number = [0]

    def pass_entries(slot, dst, when=None):
        ref = ents.at[slot]
        send(ref, ref, ent_send.at[ent_number[0]], ent_recv.at[slot], {"kv": dst}, when)
        ent_number[0] += 1

    def entries_arrived(slot):
        ref = ents.at[slot]
        pltpu.make_async_remote_copy(
            src_ref=ref, dst_ref=ref, send_sem=ent_send.at[0], recv_sem=ent_recv.at[slot],
            device_id={"kv": (me + 1) % n}, device_id_type=mesh_id,
        ).wait_recv()

    for d in range(planes - 1, 0, -1):
        up = jnp.minimum(z + d, planes - 1) * PLANE
        pass_entries(me, up + side_slot, z + d < planes)
        pass_entries(me, up + across_slot, z + d < planes)
    pass_entries(me, across)
    pass_entries(me, beside)

    for load in loads[10:14]:
        load.wait()
    hidden = rows[...]
    for i in range(half):
        made = dot(hidden, wq[:, i * 128 : (i + 1) * 128])
        g, h = (2 * i) // half, (2 * i) % half
        turned = [
            turn(made[s * span : (s + 1) * span], cosine, sine) * (HEAD_DIM**-0.5)
            for s in range(seqs)
        ]
        for p in range(pairs):
            a, b = turned[2 * p], turned[2 * p + 1]
            even, odd = jnp.where(low, a, swap(b)), jnp.where(low, swap(a), b)
            lanes = slice(p * 128, (p + 1) * 128)
            qn[g, h * span : (h + 1) * span, lanes] = even.astype(bf16)
            qn[g, (h + 1) * span : (h + 2) * span, lanes] = odd.astype(bf16)
    for b in range(1, n):
        @pl.when(b > me)
        def _():
            pltpu.make_async_remote_copy(
                src_ref=picks, dst_ref=lists.at[b], send_sem=pick_send.at[0],
                recv_sem=pick_recv.at[b], device_id={"kv": (me + 1) % n}, device_id_type=mesh_id,
            ).wait_recv()
            named_buf[...] = jnp.where(lists[b] == me, 1.0, named_buf[...])

    named = jnp.max(jnp.where(slot_at == 0, 0.0, named_buf[...]), axis=1, keepdims=True)
    named = jnp.broadcast_to(named, (2 * seqs, 128))
    key = jnp.zeros((span, 128), f32)
    for s in range(seqs):
        flag = jnp.where(low_row, named[2 * s : 2 * s + 1], named[2 * s + 1 : 2 * s + 2])
        key = key + flag * sk_buf[s * span : (s + 1) * span, :].astype(f32)
    for g in range(2):
        value = jnp.zeros((HEAD_DIM, 128), f32)
        for p in range(pairs):
            r0, r1 = 4 * p + g, 4 * p + 2 + g
            flag = jnp.where(low_row, named[r0 : r0 + 1], named[r1 : r1 + 1])
            block = svt[g * HEAD_DIM : (g + 1) * HEAD_DIM, p * 128 : (p + 1) * 128]
            value = value + flag * block.astype(f32)
        value = value + swap(value)
        blobs[g, me] = jnp.where(low, key if g == 0 else swap(key), value).astype(bf16)

    number = [0]

    def pass_on(g, slot, dst, when=None):
        ref = blobs.at[g, slot]
        send(ref, ref, blob_send.at[number[0]], blob_recv.at[g, slot], {"kv": dst}, when)
        number[0] += 1

    def arrived(g, slot):
        ref = blobs.at[g, slot]
        pltpu.make_async_remote_copy(
            src_ref=ref, dst_ref=ref, send_sem=blob_send.at[0],
            recv_sem=blob_recv.at[g, slot], device_id={"kv": (me + 1) % n}, device_id_type=mesh_id,
        ).wait_recv()

    def export(g):
        for d in range(1, planes):
            up = jnp.minimum(z + d, planes - 1) * PLANE
            pass_on(g, me, up + side_slot, z + d < planes)
            pass_on(g, me, up + across_slot, z + d < planes)
        pass_on(g, me, across)
        pass_on(g, me, beside)

    export(0)

    def entries_direct(d):
        base = jnp.maximum(z - d, 0) * PLANE
        if d == 0:
            entries_arrived(across)
            pass_entries(across, beside)
        else:
            for slot in (base + side_slot, base + across_slot):
                pl.when(z >= d)(functools.partial(entries_arrived, slot))
                pass_entries(slot, beside, z >= d)

    def entries_beside(d):
        base = jnp.maximum(z - d, 0) * PLANE

        def ready():
            for column_x in (x, 1 - x):
                entries_arrived(base + column_x * 2 + (1 - c))

        if d == 0:
            ready()
        else:
            pl.when(z >= d)(ready)

    def in_side(g, plane):
        slot = plane * PLANE + side_slot
        pl.when(z > plane)(lambda: arrived(g, slot))
        pass_on(g, slot, beside, z > plane)

    def in_cross(g, plane):
        slot = plane * PLANE + across_slot
        pl.when(z >= plane)(lambda: arrived(g, slot))
        pass_on(g, slot, beside, z >= plane)

    def plane_in(g, plane):
        @pl.when(z >= plane)
        def _():
            for column_x in (x, 1 - x):
                arrived(g, plane * PLANE + column_x * 2 + (1 - c))
            plane_scores(g, plane)

    key_at = lax.broadcasted_iota(jnp.int32, (span, across_q), 0)
    query_at = lax.broadcasted_iota(jnp.int32, (span, across_q), 1) % span
    near_bias = jnp.where(key_at <= query_at, 0.0, FAR)
    seq_lane = lax.broadcasted_iota(jnp.int32, (HEAD_DIM, seqs * span), 1) // span
    ones_at = lax.broadcasted_iota(jnp.int32, (16, seqs * span), 0)
    ones_lane = lax.broadcasted_iota(jnp.int32, (16, seqs * span), 1) // span

    def near_part(g):
        for s in range(seqs):
            block = sk_buf[s * span : (s + 1) * span, :].astype(f32)
            if g != s % 2:
                block = swap(block)
            block = jnp.where(low if s % 2 == 0 else ~low, block, 0.0).astype(bf16)
            lanes = slice((s // 2) * 128, (s // 2 + 1) * 128)
            score = dot_t(block, qn[g, :, lanes]) + near_bias
            near_s[g, s * span : (s + 1) * span, :] = score
            tops[g, n + s] = jnp.max(score.reshape(span // 8, 8, across_q), axis=0)
            value = svt[g * HEAD_DIM : (g + 1) * HEAD_DIM, :].astype(f32)
            vals[g, s * HEAD_DIM : (s + 1) * HEAD_DIM, 0:near_keys] = jnp.where(
                seq_lane == s, value, 0.0
            ).astype(bf16)
        vals[g, stack : stack + 16, 0:near_keys] = jnp.where(
            ones_at == ones_lane, 1.0, 0.0
        ).astype(bf16)

    slots = n * entries
    entry_row = lax.broadcasted_iota(jnp.int32, (slots, 128), 0)
    entry_half = lax.broadcasted_iota(jnp.int32, (slots, 128), 1) // HEAD_DIM
    entry_seq = (entry_row % entries) // count
    slot_row = lax.broadcasted_iota(jnp.int32, (slots, across_q), 0)
    slot_query = lax.broadcasted_iota(jnp.int32, (slots, across_q), 1) % span
    slot_entry = (slot_row // entries) * count + slot_row % count
    entry_ok = (slot_entry >= 1) & (
        slot_entry * CMP_STRIDE + CMP_STRIDE - 1 <= me * span + slot_query
    )
    entry_bias = jnp.where(entry_ok, 0.0, FAR)
    value_lane = (lax.broadcasted_iota(jnp.int32, (HEAD_DIM, slots), 1) % entries) // count
    total_row = lax.broadcasted_iota(jnp.int32, (16, slots), 0)
    total_lane = (lax.broadcasted_iota(jnp.int32, (16, slots), 1) % entries) // count
    group_row = lax.broadcasted_iota(jnp.int32, (entries, across_q), 0)

    def cmp_part(g):
        part = slice(g * entries, (g + 1) * entries)
        both = ents[:, part, :].reshape(slots, 128).astype(f32)
        twice = jnp.where(entry_half == 0, both, swap(both))
        keys = jnp.concatenate(
            [jnp.where(entry_seq == 2 * p + entry_half, twice, 0.0) for p in range(pairs)], axis=1
        ).astype(bf16)
        score = (dot_t(keys, qn[g]) + entry_bias).reshape(n, entries, across_q)
        top = jnp.max(score, axis=0)
        for step in (1, 2):
            top = jnp.maximum(
                top,
                jnp.where(
                    (group_row // step) % 2 == 0,
                    pltpu.roll(top, entries - step, 0),
                    pltpu.roll(top, step, 0),
                ),
            )
        top = jnp.maximum(top, -1e29)
        w = jnp.exp(score - top[None]).reshape(slots, across_q).astype(bf16)
        value = jnp.transpose(both)[HEAD_DIM:]
        left = [jnp.where(value_lane == s, value, 0.0) for s in range(seqs)]
        left.append(jnp.where(total_row == total_lane, 1.0, 0.0))
        made = dot(jnp.concatenate(left, axis=0).astype(bf16), w)
        for s in range(seqs):
            total = jnp.maximum(made[stack + s : stack + s + 1], 1.0)
            row = g * seqs + s
            factor = gate_buf[row : row + 1, :] / total
            block = slice(s * HEAD_DIM, (s + 1) * HEAD_DIM)
            mix[g, block, :] = made[block] * factor

    def plane_scores(g, plane):
        base = plane * PLANE
        first_lane = value_lanes(plane).start
        left = []
        for i in range(PLANE):
            block = blobs[g, base + i].astype(f32)
            turned = swap(block)
            twice = jnp.where(low, block, turned)
            tiles = []
            for p in range(pairs):
                r0, r1 = 4 * p + g, 4 * p + 2 + g
                flag = jnp.where(
                    low_row, hits[base + i, r0 : r0 + 1], hits[base + i, r1 : r1 + 1]
                )
                tiles.append(twice * flag)
            left.append(jnp.concatenate(tiles, axis=1))
            if i % 2 == 0:
                before = turned
            else:
                value = jnp.where(low, before, block)
                lanes = slice(first_lane + (i - 1) * span, first_lane + (i + 1) * span)
                flags = [
                    jnp.where(low_row, hits[base + i - 1, r : r + 1], hits[base + i, r : r + 1])
                    for r in range(g, 2 * seqs, 2)
                ]
                for s in range(seqs):
                    vals[g, s * HEAD_DIM : (s + 1) * HEAD_DIM, lanes] = (value * flags[s]).astype(
                        bf16
                    )
                flags.append(jnp.zeros((16 - seqs, 128), f32))
                vals[g, stack : stack + 16, lanes] = jnp.concatenate(flags, axis=0).astype(bf16)
        score = dot_t(jnp.concatenate(left, axis=0).astype(bf16), qn[g])
        far_s[g, base * span : base * span + plane_keys, :] = score
        for i in range(PLANE):
            block = score[i * span : (i + 1) * span].reshape(span // 8, 8, across_q)
            tops[g, base + i] = jnp.max(block, axis=0)

    def flag_of(b):
        return jnp.concatenate([hits[b], hits[b]], axis=1) > 0

    def far_base(g):
        blocks = range(PLANE, n)
        refs = {b: jnp.full((1, across_q), 1e30, f32) for b in blocks}
        flags = {b: flag_of(b) for b in blocks}
        for s in range(seqs):
            r = 2 * s + g
            top = tops[g, n + s]
            for b in blocks:
                top = jnp.maximum(top, jnp.where(flags[b][r : r + 1], tops[g, b], FAR))
            top = jnp.max(top, axis=0, keepdims=True)
            base_top[g, s : s + 1, :] = top
            for b in blocks:
                refs[b] = jnp.where(flags[b][r : r + 1], top, refs[b])
            part = slice(s * span, (s + 1) * span)
            probs[part, :] = jnp.exp(near_s[g, part, :] - top).astype(bf16)
        for b in blocks:
            block = jnp.exp(far_s[g, b * span : (b + 1) * span, :] - refs[b]).astype(bf16)
            start = near_keys + (b - PLANE) * span
            probs[start : start + span, :] = block
        known = n * span
        base_sum[g] = dot(vals[g, :, :known], probs[...])

    def far_part(g):
        refs = [jnp.full((1, across_q), 1e30, f32) for _ in range(PLANE)]
        flags = [flag_of(b) for b in range(PLANE)]
        scales = []
        for s in range(seqs):
            r = 2 * s + g
            top = jnp.where(flags[0][r : r + 1], tops[g, 0], FAR)
            for b in range(1, PLANE):
                top = jnp.maximum(top, jnp.where(flags[b][r : r + 1], tops[g, b], FAR))
            before = base_top[g, s : s + 1, :]
            top = jnp.maximum(jnp.max(top, axis=0, keepdims=True), before)
            scales.append(jnp.exp(before - top))
            for b in range(PLANE):
                refs[b] = jnp.where(flags[b][r : r + 1], top, refs[b])
        w = jnp.concatenate(
            [
                jnp.exp(far_s[g, b * span : (b + 1) * span, :] - refs[b]).astype(bf16)
                for b in range(PLANE)
            ],
            axis=0,
        )
        made = dot(vals[g, :, n * span :], w)
        for p in range(pairs):
            tiles = []
            for s in (2 * p, 2 * p + 1):
                row = (2 + g) * seqs + s
                line = slice(stack + s, stack + s + 1)
                total = jnp.maximum(base_sum[g, line, :] * scales[s] + made[line], 1.0)
                factor = gate_buf[row : row + 1, :] / total
                block = slice(s * HEAD_DIM, (s + 1) * HEAD_DIM)
                old = base_sum[g, block, :] * (scales[s] * factor)
                tiles.append(mix[g, block, :] + old + made[block] * factor)
            both = jnp.concatenate(tiles, axis=0)
            for j in range(half // 2):
                lanes = slice(j * 128, (j + 1) * 128)
                flipped = jnp.transpose(both[:, lanes])
                a, b = flipped[:span], flipped[span:]
                part = slice(2 * p * span, (2 * p + 1) * span)
                own[g, part, lanes] = jnp.where(low, a, swap(b)).astype(bf16)
                part = slice((2 * p + 1) * span, (2 * p + 2) * span)
                own[g, part, lanes] = jnp.where(low, swap(a), b).astype(bf16)
            for s in (2 * p, 2 * p + 1):
                piece(g, s).start()

    def piece(g, s):
        part = pl.ds(s * span, span)
        return pltpu.make_async_remote_copy(
            src_ref=own.at[g, part], dst_ref=other.at[g, part], send_sem=half_send.at[g, s],
            recv_sem=half_recv.at[g, s], device_id={"tp": 1 - column}, device_id_type=mesh_id,
        )

    spread = 2 * wg_ref.shape[1]
    logits = dot_t(wg[...].reshape(spread, rows.shape[1]), hidden)
    wide_at = lax.broadcasted_iota(jnp.int32, (1, seqs * span), 1)
    limit = jnp.zeros((1, seqs * span), jnp.int32)
    for s in range(seqs):
        limit = jnp.where(wide_at // span == s, lens[:, s : s + 1], limit)
    live = me * span + wide_at % span < limit
    for branch in range(2):
        base = branch * (spread // 2)
        mine = jnp.where(
            column == 0, logits[base : base + heads], logits[base + heads : base + 2 * heads]
        )
        mine = jnp.where(live, jax.nn.sigmoid(mine), 0.0)
        turned = [mine[:, p * 128 : (p + 1) * 128] for p in range(pairs)]
        swapped = [swap(t) for t in turned]
        for g in range(2):
            for s in range(seqs):
                for j in range(half // 2):
                    one = slice(g * half + 2 * j, g * half + 2 * j + 1)
                    two = slice(g * half + 2 * j + 1, g * half + 2 * j + 2)
                    t, w = turned[s // 2], swapped[s // 2]
                    if s % 2 == 0:
                        row = jnp.where(low_row, t[one], w[two])
                    else:
                        row = jnp.where(low_row, w[one], t[two])
                    line = (branch * 2 + g) * seqs + s
                    gate_buf[line : line + 1, j * 128 : (j + 1) * 128] = row

    for g in range(2):
        near_part(g)
    last = planes - 1
    for plane in range(last - 1, 0, -1):
        in_side(0, plane)
        in_cross(0, plane + 1)
    in_cross(0, 1)
    export(1)
    for d in range(planes):
        entries_direct(d)
    for plane in range(last, 1, -1):
        plane_in(0, plane)
    for d in range(planes):
        entries_beside(d)
    cmp_part(0)
    in_side(0, 0)
    plane_in(0, 1)
    in_cross(0, 0)
    for plane in range(last - 1, 0, -1):
        in_side(1, plane)
    in_cross(1, last)
    far_base(0)
    plane_in(0, 0)
    far_part(0)
    for plane in range(last - 1, 0, -1):
        in_cross(1, plane)
    in_side(1, 0)
    in_cross(1, 0)
    for load in loads[14:]:
        load.wait()
    cmp_part(1)
    for plane in range(last, 0, -1):
        plane_in(1, plane)
    far_base(1)
    plane_in(1, 0)
    far_part(1)

    squares = jnp.zeros((seqs * span, 1), f32)
    total = jnp.zeros((seqs * span, wide), f32)
    group = half * HEAD_DIM

    def gains(side, g):
        return gain[:, pl.ds(pl.multiple_of(side * depth + g * group, group), group)]

    for g in range(2):
        a = own[g].astype(f32)
        squares = squares + jnp.sum(a * a, axis=1, keepdims=True)
        scaled = (a * gains(column, g)).astype(bf16)
        total = total + dot(scaled, weight[0, g * group : (g + 1) * group, :])
    for s in range(seqs):
        piece(0, s).wait_recv()
    a = other[0].astype(f32)
    squares = squares + jnp.sum(a * a, axis=1, keepdims=True)
    scaled = (a * gains(1 - column, 0)).astype(bf16)
    partial[...] = total + dot(scaled, weight[1, :group, :])
    for s in range(seqs):
        piece(1, s).wait_recv()
        part = slice(s * span, (s + 1) * span)
        a = other[1, part, :].astype(f32)
        square = squares[part] + jnp.sum(a * a, axis=1, keepdims=True)
        row_scale = lax.rsqrt(square / (2 * depth) + norm_eps)
        scaled = (a * gains(1 - column, 1)).astype(bf16)
        done = partial[part, :] + dot(scaled, weight[1, group:, :])
        out_ref[part, :] = (done * row_scale).astype(bf16)

    for g in range(2):
        for s in range(seqs):
            piece(g, s).wait_send()
    for copy, when in sent:
        if when is None:
            copy.wait_send()
        else:
            pl.when(when)(copy.wait_send)


def fused_shards(
    hidden_in,
    w_query,
    w_cmp_key,
    w_cmp_value,
    w_sel_key,
    w_sel_value,
    w_gate,
    cmp_key_in,
    cmp_key_out,
    cmp_value_in,
    cmp_value_out,
    out_gain,
    w_out,
    seq_lengths,
    chosen,
):
    seqs, span, width = hidden_in.shape
    n = lax.axis_size("kv")
    heads = w_query.shape[1] // HEAD_DIM
    total = seqs * span
    entries = total // CMP_STRIDE
    out_width = width // lax.axis_size("tp")
    small = w_sel_key.shape[1]
    half = heads // 2
    stack = seqs * HEAD_DIM
    across_q = half * span
    planes = n // PLANE
    anywhere = pl.BlockSpec(memory_space=pl.ANY)
    gate_rows = jnp.transpose(w_gate, (1, 2, 0))
    picks = chosen[:, 0].reshape(2 * seqs, TOPK)
    key_out, value_out = jnp.transpose(cmp_key_out), jnp.transpose(cmp_value_out)
    lens = seq_lengths[None]
    gain = out_gain[None]
    blob_sends = 2 * (6 * planes)
    out = pl.pallas_call(
        functools.partial(layer_kernel, n, seqs, span, heads),
        in_specs=[anywhere] * 15,
        out_specs=pl.BlockSpec(memory_space=pltpu.VMEM),
        out_shape=pltpu.VMEM((total, out_width), bf16),
        scratch_shapes=[
            pltpu.VMEM(picks.shape, jnp.int32),
            pltpu.VMEM((total, width), bf16),
            pltpu.VMEM((width, 4 * small), bf16),
            pltpu.VMEM(key_out.shape, bf16),
            pltpu.VMEM(value_out.shape, bf16),
            pltpu.VMEM(cmp_key_in.shape, bf16),
            pltpu.VMEM(cmp_value_in.shape, bf16),
            pltpu.VMEM(w_query.shape, bf16),
            pltpu.VMEM(gate_rows.shape, bf16),
            pltpu.VMEM(lens.shape, jnp.int32),
            pltpu.VMEM(gain.shape, f32),
            pltpu.VMEM((2, heads * HEAD_DIM, out_width), bf16),
            pltpu.VMEM((2, across_q, stack), bf16),
            pltpu.VMEM((total, small), bf16),
            pltpu.VMEM((small, total), bf16),
            pltpu.VMEM((2, total, small), f32),
            pltpu.VMEM((4 * seqs, across_q), f32),
            pltpu.VMEM((n, 2 * seqs, 128), f32),
            pltpu.VMEM((n,) + picks.shape, jnp.int32),
            pltpu.VMEM(picks.shape, f32),
            pltpu.VMEM((n, 2 * entries, 128), bf16),
            pltpu.VMEM((2, n, span, 128), bf16),
            pltpu.VMEM((2, total, across_q), f32),
            pltpu.VMEM((2, n * span, across_q), f32),
            pltpu.VMEM((2, n + seqs, 8, across_q), f32),
            pltpu.VMEM((2, 8, across_q), f32),
            pltpu.VMEM((n * span, across_q), bf16),
            pltpu.VMEM((2, stack + 16, across_q), f32),
            pltpu.VMEM((2, stack + 16, total + n * span), bf16),
            pltpu.VMEM((2, stack, across_q), f32),
            pltpu.VMEM((2, total, half * HEAD_DIM), bf16),
            pltpu.VMEM((2, total, half * HEAD_DIM), bf16),
            pltpu.VMEM((total, out_width), f32),
            pltpu.SemaphoreType.DMA((16,)),
            pltpu.SemaphoreType.DMA((n,)),
            pltpu.SemaphoreType.DMA((n,)),
            pltpu.SemaphoreType.DMA((4 * planes,)),
            pltpu.SemaphoreType.DMA((n,)),
            pltpu.SemaphoreType.DMA((blob_sends,)),
            pltpu.SemaphoreType.DMA((2, n)),
            pltpu.SemaphoreType.DMA((2, seqs)),
            pltpu.SemaphoreType.DMA((2, seqs)),
        ],
        compiler_params=pltpu.CompilerParams(
            collective_id=0, has_side_effects=True, vmem_limit_bytes=VMEM_BYTES
        ),
        name="layer",
    )(
        picks, hidden_in.reshape(total, width), w_sel_key, w_sel_value, w_cmp_key, w_cmp_value,
        key_out, value_out, cmp_key_in, cmp_value_in, w_query, gate_rows, lens, gain, w_out,
    )
    return out.reshape(seqs, span, out_width)


def fits(mesh):
    n = mesh.shape["kv"]
    return mesh.shape["tp"] == 2 and n % PLANE == 0 and 3 * PLANE <= n <= 32


def solution(mesh):
    placed = (
        P(None, "kv", None),
        P(None, "tp"),
        P(None, "tp"),
        P(None, "tp"),
        P(None, "tp"),
        P(None, "tp"),
        P(),
        P(),
        P(),
        P(),
        P(),
        P(),
        P(),
        P(),
        P(None, "kv", "tp", None),
    )
    return jax.shard_map(
        fused_shards if fits(mesh) else shards, mesh=mesh, in_specs=placed, out_specs=P(None, "kv", "tp"), check_vma=False
    )
```

```python
import functools
import math

import jax
import jax.numpy as jnp
from jax import lax
from jax.experimental import pallas as pl
from jax.experimental.pallas import tpu as pltpu
from jax.sharding import PartitionSpec as P

HEADS = 16
HEAD_DIM = 64
CMP_STRIDE = 16
CMP_BLOCK = 32
TOPK = 16


theta_base = 500000.0
norm_eps = 1e-06


def rotate(values, positions):
    width = values.shape[-1]
    half = width // 2
    inverse = jnp.exp(
        -jnp.log(jnp.float32(theta_base)) * jnp.arange(0, width, 2).astype(jnp.float32) / width
    )
    angle = positions.astype(jnp.float32)[:, None] * inverse[None, :]
    cosine = jnp.cos(angle)[:, None, :]
    sine = jnp.sin(angle)[:, None, :]
    first = values[..., :half]
    second = values[..., half:]
    return jnp.concatenate(
        [first * cosine - second * sine, second * cosine + first * sine], axis=-1
    )


def masked_weights(scores, valid):
    top = jnp.max(jnp.where(valid, scores, -1e30), axis=-1, keepdims=True)
    expd = jnp.where(valid, jnp.exp(scores - top), 0.0)
    total = jnp.sum(expd, axis=-1, keepdims=True)
    return (expd / jnp.maximum(total, 1.0)).astype(jnp.bfloat16)


def compress(raw, prior, weight_in, weight_out):
    seqs, span, groups, width = raw.shape
    extended = jnp.concatenate([prior, raw], axis=1)
    count = span // CMP_STRIDE
    front = extended[:, :span].reshape(seqs, count, CMP_STRIDE, groups, width)
    back = extended[:, CMP_STRIDE:].reshape(seqs, count, CMP_STRIDE, groups, width)
    window = jnp.concatenate([front, back], axis=2).transpose(0, 1, 3, 2, 4)
    window = window.reshape(seqs * count * groups, CMP_BLOCK * width)
    inner = jax.nn.gelu(jnp.dot(window, weight_in, preferred_element_type=jnp.float32)).astype(
        jnp.bfloat16
    )
    return jnp.dot(inner, weight_out, preferred_element_type=jnp.float32).reshape(
        seqs, count, groups, width
    )


def shards(
    hidden_in,
    w_query,
    w_cmp_key,
    w_cmp_value,
    w_sel_key,
    w_sel_value,
    w_gate,
    cmp_key_in,
    cmp_key_out,
    cmp_value_in,
    cmp_value_out,
    out_gain,
    w_out,
    seq_lengths,
    chosen,
):
    seqs, span, width = hidden_in.shape
    block_list = lax.axis_size("kv")
    place = lax.axis_index("kv")
    column = lax.axis_index("tp")
    local_heads = w_query.shape[1] // HEAD_DIM
    local_groups = w_sel_key.shape[1] // HEAD_DIM
    per_group = local_heads // local_groups
    count = span // CMP_STRIDE
    scale = HEAD_DIM ** (-0.5)
    rows = hidden_in.reshape(seqs * span, width)
    positions = place * span + jnp.arange(span, dtype=jnp.int32)

    def project(weight_matrix, heads):
        return jnp.dot(rows, weight_matrix, preferred_element_type=jnp.float32).reshape(
            seqs, span, heads, HEAD_DIM
        )

    queries = rotate(project(w_query, local_heads), positions).astype(jnp.bfloat16)
    sel_pairs = jnp.concatenate(
        [rotate(project(w_sel_key, local_groups), positions), project(w_sel_value, local_groups)],
        axis=-1,
    ).astype(jnp.bfloat16)
    raw_pairs = jnp.concatenate(
        [project(w_cmp_key, local_groups), project(w_cmp_value, local_groups)], axis=-1
    ).astype(jnp.bfloat16)
    prior = jnp.zeros((seqs, CMP_STRIDE, local_groups, HEAD_DIM), jnp.bfloat16)
    ends = place * span + jnp.arange(count, dtype=jnp.int32) * CMP_STRIDE + CMP_STRIDE - 1
    cmp_keys = rotate(compress(raw_pairs[..., :HEAD_DIM], prior, cmp_key_in, cmp_key_out), ends)
    cmp_values = compress(raw_pairs[..., HEAD_DIM:], prior, cmp_value_in, cmp_value_out)
    cmp_piece = jnp.concatenate(
        [cmp_keys.astype(jnp.bfloat16), cmp_values.astype(jnp.bfloat16)], axis=-1
    )[:, None]
    picks = chosen[:, 0]
    every_list = lax.all_gather(picks[None, :, :, 1:], "kv", axis=0, tiled=True)
    named = jnp.any(every_list == place, axis=(0, 3)).astype(jnp.int32)
    seq_ids = jnp.arange(seqs, dtype=jnp.int32)[:, None]
    exported_seq = jnp.sum(named * seq_ids, axis=0)
    selector = seq_ids == exported_seq[None, :]
    export = jnp.sum(
        jnp.where(selector[:, None, :, None], sel_pairs, jnp.zeros((), jnp.bfloat16)), axis=0
    )
    export = export[None]
    remote_pairs, remote_entries = (
        lax.all_gather(export, "kv", axis=0, tiled=True),
        lax.all_gather(cmp_piece, "kv", axis=1, tiled=True),
    )
    gate_all = jnp.dot(rows, w_gate.reshape(width, 2 * HEADS), preferred_element_type=jnp.float32)
    gate_all = gate_all.reshape(seqs, span, 2, HEADS)
    gates = jax.nn.sigmoid(lax.dynamic_slice_in_dim(gate_all, column * local_heads, local_heads, 3))
    entry = jnp.arange(block_list * count, dtype=jnp.int32)
    entry_end = entry * CMP_STRIDE + CMP_STRIDE - 1
    cmp_valid = ((entry >= 1)[None, :] & (entry_end[None, :] <= positions[:, None]))[None, None]
    key_pos = jnp.arange(span, dtype=jnp.int32)
    own_valid = key_pos[None, :] <= key_pos[:, None]

    def one_sequence(args):
        seq_queries, seq_entries, seq_picks, seq_pairs, seq_gates, seq_length = args
        block_q = seq_queries.reshape(span, local_groups, per_group, HEAD_DIM)
        entries = seq_entries.reshape(block_list * count, local_groups, 2 * HEAD_DIM)
        scores = (
            jnp.einsum(
                "qghd,egd->ghqe",
                block_q,
                entries[..., :HEAD_DIM],
                preferred_element_type=jnp.float32,
            )
            * scale
        )
        weights = masked_weights(scores, cmp_valid)
        cmp_out = jnp.einsum(
            "ghqe,egd->qghd", weights, entries[..., HEAD_DIM:], preferred_element_type=jnp.float32
        )
        far = jnp.maximum(seq_picks[:, 1:], 0)
        fetched = jax.vmap(lambda table, index: table[index], in_axes=(2, 0))(remote_pairs, far)
        near = jnp.transpose(seq_pairs, (1, 0, 2))[:, None]
        pairs = jnp.concatenate([near, fetched], axis=1).reshape(
            local_groups, TOPK * span, 2 * HEAD_DIM
        )
        far_live = jnp.broadcast_to(
            (seq_picks[:, 1:] >= 0)[:, None, :, None], (local_groups, span, TOPK - 1, span)
        )
        near_live = jnp.broadcast_to(own_valid[None, :, None, :], (local_groups, span, 1, span))
        sel_valid = jnp.concatenate([near_live, far_live], axis=2).reshape(
            local_groups, 1, span, TOPK * span
        )
        scores_s = (
            jnp.einsum(
                "qghd,gmd->ghqm", block_q, pairs[..., :HEAD_DIM], preferred_element_type=jnp.float32
            )
            * scale
        )
        weights_s = masked_weights(scores_s, sel_valid)
        sel_out = jnp.einsum(
            "ghqm,gmd->qghd", weights_s, pairs[..., HEAD_DIM:], preferred_element_type=jnp.float32
        )
        split = seq_gates.reshape(span, 2, local_groups, per_group, 1)
        mixed = split[:, 0] * cmp_out + split[:, 1] * sel_out
        mixed = jnp.where((positions < seq_length)[:, None, None, None], mixed, 0.0)
        return mixed.reshape(span, local_heads * HEAD_DIM).astype(jnp.bfloat16)

    mixed = lax.map(one_sequence, (queries, remote_entries, picks, sel_pairs, gates, seq_lengths))
    mixed = mixed.reshape(seqs * span, local_heads * HEAD_DIM)
    out_width = width // lax.axis_size("tp")
    own_columns = lax.dynamic_slice_in_dim(w_out, column * out_width, out_width, 1)
    piece_wide = lax.all_gather(mixed, "tp", axis=1, tiled=True).astype(jnp.float32)
    scaled_piece = (piece_wide * out_gain[None, :]).astype(jnp.bfloat16)
    total = jnp.dot(scaled_piece, own_columns, preferred_element_type=jnp.float32)
    squares = jnp.sum(piece_wide * piece_wide, axis=-1)
    row_scale = lax.rsqrt(squares / (HEADS * HEAD_DIM) + norm_eps)
    return (total * row_scale[:, None]).astype(jnp.bfloat16).reshape(seqs, span, out_width)


FAR = -1e30
PLANE = 4
VMEM_BYTES = 60 * 1024 * 1024
f32 = jnp.float32
bf16 = jnp.bfloat16


def dot(a, b):
    return jnp.dot(a, b, preferred_element_type=f32)


def dot_t(a, b):
    return lax.dot_general(a, b, (((1,), (1,)), ((), ())), preferred_element_type=f32)


def swap(values):
    return pltpu.roll(values, HEAD_DIM, 1)


def turn(values, cosine, sine):
    lane = lax.broadcasted_iota(jnp.int32, values.shape, 1)
    other = jnp.where(
        lane % HEAD_DIM < HEAD_DIM // 2,
        pltpu.roll(values, 128 - HEAD_DIM // 2, 1),
        pltpu.roll(values, HEAD_DIM // 2, 1),
    )
    return values * cosine + other * sine


def gelu(x):
    return 0.5 * x * (1.0 + jnp.tanh(0.7978845608028654 * (x + 0.044715 * (x * x * x))))


def layer_kernel(
    n, seqs, span, heads,
    picks_ref, rows_ref, wsk_ref, wsv_ref, wck_ref, wcv_ref, kout_ref, vout_ref, kin_ref, vin_ref,
    wq_ref, wg_ref, lens_ref, gain_ref, wout_ref,
    out_ref,
    picks, rows, ws, kout, vout, kin, vin, wq, wg, lens, gain, weight,
    qn, sk_buf, svt, raw, gate_buf, hits, lists, ents, blobs, near_s, far_s, tops, base_top,
    probs, base_sum, vals, mix, own, other, partial,
    load_sem, pick_send, pick_recv, ent_send, ent_recv, blob_send, blob_recv, half_send, half_recv,
):
    me = lax.axis_index("kv")
    column = lax.axis_index("tp")
    planes = n // PLANE
    z, x, c = me // PLANE, (me // 2) % 2, me % 2
    depth = heads * HEAD_DIM
    wide = out_ref.shape[1]
    count = span // CMP_STRIDE
    entries = seqs * count
    half = heads // 2
    stack = seqs * HEAD_DIM
    across_q = half * span
    pairs = seqs // 2
    mesh_id = pl.DeviceIdType.MESH

    barrier = pltpu.get_barrier_semaphore()
    for d in range(1, n):
        pl.semaphore_signal(
            barrier, inc=1, device_id={"kv": (me + d) % n}, device_id_type=mesh_id
        )
    pl.semaphore_signal(barrier, inc=1, device_id={"tp": 1 - column}, device_id_type=mesh_id)

    jobs = [(picks_ref, picks), (rows_ref, rows)]
    for i, ref in enumerate((wsk_ref, wsv_ref, wck_ref, wcv_ref)):
        jobs.append((ref, ws.at[:, i * 128 : (i + 1) * 128]))
    jobs += [(kout_ref, kout), (vout_ref, vout), (kin_ref, kin), (vin_ref, vin)]
    jobs += [(wq_ref, wq), (wg_ref, wg), (lens_ref, lens), (gain_ref, gain)]
    for i in range(2):
        side = column if i == 0 else 1 - column
        block = wout_ref.at[
            pl.ds(pl.multiple_of(side * depth, depth), depth),
            pl.ds(pl.multiple_of(column * wide, wide), wide),
        ]
        jobs.append((block, weight.at[i]))
    shared = [0, 1, 2, 2, 2, 2, 3, 4, 5, 6, 7, 8, 9, 10, 11, 11]
    loads = [pltpu.make_async_copy(a, b, load_sem.at[i]) for i, (a, b) in zip(shared, jobs)]
    for load in loads:
        load.start()

    lane = lax.broadcasted_iota(jnp.int32, (span, 128), 1)
    low = lane < HEAD_DIM
    low_e = low[:entries]
    low_row = low[:1]
    at = lax.broadcasted_iota(jnp.int32, (span, 128), 0)
    sign = jnp.where(lane % HEAD_DIM < HEAD_DIM // 2, -1.0, 1.0)
    power = (lane % (HEAD_DIM // 2) * 2).astype(f32)
    freq = jnp.exp(-math.log(theta_base) * power / HEAD_DIM)
    angle = (me * span + at).astype(f32) * freq
    cosine = jnp.cos(angle)
    sine = jnp.sin(angle) * sign
    end = me * span + (at[:entries] % count) * CMP_STRIDE + CMP_STRIDE - 1
    angle = end.astype(f32) * freq[:entries]
    cosine_e = jnp.cos(angle)
    sine_e = jnp.sin(angle) * sign[:entries]

    near_keys = seqs * span
    plane_keys = PLANE * span

    def value_lanes(plane):
        start = near_keys + (plane + planes - 1) % planes * plane_keys
        return slice(start, start + plane_keys)

    for plane in range(1, planes):
        @pl.when(plane > z)
        def _():
            for i in range(PLANE):
                ents[plane * PLANE + i] = jnp.zeros((2 * entries, 128), bf16)
            keys = slice(plane * plane_keys, (plane + 1) * plane_keys)
            lanes = value_lanes(plane)
            for g in range(2):
                far_s[g, keys, :] = jnp.zeros((plane_keys, across_q), f32)
                vals[g, :, lanes] = jnp.zeros((stack + 16, plane_keys), bf16)
                tops[g, plane * PLANE : (plane + 1) * PLANE] = jnp.zeros(
                    (PLANE, 8, across_q), f32
                )

    loads[0].wait()
    pl.semaphore_wait(barrier, n)
    def send(src, dst, ssem, rsem, target, when=None):
        copy = pltpu.make_async_remote_copy(
            src_ref=src, dst_ref=dst, send_sem=ssem, recv_sem=rsem,
            device_id=target, device_id_type=mesh_id,
        )
        if when is None:
            copy.start()
        else:
            pl.when(when)(copy.start)

    for d in range(n - 1, 0, -1):
        send(
            picks, lists.at[me], pick_send.at[0], pick_recv.at[0], {"kv": (me + n - d) % n},
            me >= d,
        )

    def lists_copy(amount):
        ref = lists.at[pl.ds(0, amount)]
        return pltpu.make_async_remote_copy(
            src_ref=ref, dst_ref=ref, send_sem=pick_send.at[0], recv_sem=pick_recv.at[0],
            device_id={"kv": (me + 1) % n}, device_id_type=mesh_id,
        )

    slot_at = lax.broadcasted_iota(jnp.int32, (2 * seqs, TOPK), 1)
    listed = jnp.where(slot_at == 0, -1, picks[...])
    for b in range(n):
        hit = jnp.max(jnp.where(listed == b, 1.0, 0.0), axis=1, keepdims=True)
        hits[b] = jnp.broadcast_to(hit, (2 * seqs, 128))

    loads[1].wait()
    pltpu.make_async_copy(ws, ws, load_sem.at[2]).wait()
    made = dot(rows[...], ws[...])
    sv = []
    for s in range(seqs):
        part = slice(s * span, (s + 1) * span)
        sk_buf[part, :] = turn(made[part, :128], cosine, sine).astype(bf16)
    svt[...] = jnp.transpose(made[:, 128:256]).astype(bf16)
    raw[0] = made[:, 256:384].astype(bf16).astype(f32)
    raw[1] = made[:, 384:512].astype(bf16).astype(f32)
    first = at[:entries] % count == 0
    mid = CMP_STRIDE * HEAD_DIM
    results = []
    for load in loads[6:10]:
        load.wait()
    for branch, inner_weight, outer in ((0, kin, kout), (1, vin, vout)):
        left, right = [], []
        for j in range(0, CMP_STRIDE, 2):
            a = raw[branch, pl.ds(j, entries, stride=CMP_STRIDE), :]
            b = raw[branch, pl.ds(j + 1, entries, stride=CMP_STRIDE), :]
            left.append(jnp.where(low_e, a, swap(b)))
            right.append(jnp.where(low_e, swap(a), b))
        window = jnp.concatenate(
            [jnp.concatenate(left, axis=1), jnp.concatenate(right, axis=1)], axis=0
        ).astype(bf16)
        front = dot(window, inner_weight[:mid])
        back = dot(window, inner_weight[mid:])
        parts = []
        for g in range(2):
            shifted = pltpu.roll(front[g * entries : (g + 1) * entries], 1, 0)
            parts.append(back[g * entries : (g + 1) * entries] + jnp.where(first, 0.0, shifted))
        inner = gelu(jnp.concatenate(parts, axis=0)).astype(bf16)
        results.append(dot_t(inner, jnp.concatenate([outer[...], outer[...]], axis=0)))
    for g in range(2):
        part = slice(g * entries, (g + 1) * entries)
        key = turn(results[0][part], cosine_e, sine_e)
        ents[me, part, :] = jnp.where(low_e, key, results[1][part]).astype(bf16)
    across = z * PLANE + (1 - x) * 2 + c
    beside = z * PLANE + x * 2 + (1 - c)
    side_slot = x * 2 + c
    across_slot = (1 - x) * 2 + c
    def pass_entries(slot, dst, when=None):
        ref = ents.at[slot]
        send(ref, ref, ent_send.at[0], ent_recv.at[slot], {"kv": dst}, when)

    def entries_arrived(slot):
        ref = ents.at[slot]
        pltpu.make_async_remote_copy(
            src_ref=ref, dst_ref=ref, send_sem=ent_send.at[0], recv_sem=ent_recv.at[slot],
            device_id={"kv": (me + 1) % n}, device_id_type=mesh_id,
        ).wait_recv()

    for d in range(planes - 1, 0, -1):
        up = jnp.minimum(z + d, planes - 1) * PLANE
        pass_entries(me, up + side_slot, z + d < planes)
        pass_entries(me, up + across_slot, z + d < planes)
    pass_entries(me, across)
    pass_entries(me, beside)

    for load in loads[10:14]:
        load.wait()
    hidden = rows[...]
    for i in range(half):
        made = dot(hidden, wq[:, i * 128 : (i + 1) * 128])
        g, h = (2 * i) // half, (2 * i) % half
        turned = [
            turn(made[s * span : (s + 1) * span], cosine, sine) * (HEAD_DIM**-0.5)
            for s in range(seqs)
        ]
        for p in range(pairs):
            a, b = turned[2 * p], turned[2 * p + 1]
            even, odd = jnp.where(low, a, swap(b)), jnp.where(low, swap(a), b)
            lanes = slice(p * 128, (p + 1) * 128)
            qn[g, h * span : (h + 1) * span, lanes] = even.astype(bf16)
            qn[g, (h + 1) * span : (h + 2) * span, lanes] = odd.astype(bf16)
    for b in range(n - 1):
        pl.when(me == b)(lambda b=b: lists_copy(n - 1 - b).wait_recv())
    named = jnp.zeros((2 * seqs, TOPK), f32)
    for b in range(1, n):
        named = jnp.where((lists[b] == me) & (me < b), 1.0, named)
    named = jnp.max(jnp.where(slot_at == 0, 0.0, named), axis=1, keepdims=True)
    named = jnp.broadcast_to(named, (2 * seqs, 128))
    key = jnp.zeros((span, 128), f32)
    for s in range(seqs):
        flag = jnp.where(low_row, named[2 * s : 2 * s + 1], named[2 * s + 1 : 2 * s + 2])
        key = key + flag * sk_buf[s * span : (s + 1) * span, :].astype(f32)
    for g in range(2):
        value = jnp.zeros((HEAD_DIM, 128), f32)
        for p in range(pairs):
            r0, r1 = 4 * p + g, 4 * p + 2 + g
            flag = jnp.where(low_row, named[r0 : r0 + 1], named[r1 : r1 + 1])
            block = svt[g * HEAD_DIM : (g + 1) * HEAD_DIM, p * 128 : (p + 1) * 128]
            value = value + flag * block.astype(f32)
        value = value + swap(value)
        blobs[g, me] = jnp.where(low, key if g == 0 else swap(key), value).astype(bf16)

    def pass_on(g, slot, dst, when=None):
        ref = blobs.at[g, slot]
        send(ref, ref, blob_send.at[0], blob_recv.at[g, slot], {"kv": dst}, when)

    def arrived(g, slot):
        ref = blobs.at[g, slot]
        pltpu.make_async_remote_copy(
            src_ref=ref, dst_ref=ref, send_sem=blob_send.at[0],
            recv_sem=blob_recv.at[g, slot], device_id={"kv": (me + 1) % n}, device_id_type=mesh_id,
        ).wait_recv()

    def export(g):
        for d in range(1, planes):
            up = jnp.minimum(z + d, planes - 1) * PLANE
            pass_on(g, me, up + side_slot, z + d < planes)
            pass_on(g, me, up + across_slot, z + d < planes)
        pass_on(g, me, across)
        pass_on(g, me, beside)

    export(0)

    def entries_direct(d):
        base = jnp.maximum(z - d, 0) * PLANE
        if d == 0:
            entries_arrived(across)
            pass_entries(across, beside)
        else:
            for slot in (base + side_slot, base + across_slot):
                pl.when(z >= d)(functools.partial(entries_arrived, slot))
                pass_entries(slot, beside, z >= d)

    def entries_beside(d):
        base = jnp.maximum(z - d, 0) * PLANE

        def ready():
            for column_x in (x, 1 - x):
                entries_arrived(base + column_x * 2 + (1 - c))

        if d == 0:
            ready()
        else:
            pl.when(z >= d)(ready)

    def in_side(g, plane):
        slot = plane * PLANE + side_slot
        pl.when(z > plane)(lambda: arrived(g, slot))
        pass_on(g, slot, beside, z > plane)

    def in_cross(g, plane):
        slot = plane * PLANE + across_slot
        pl.when(z >= plane)(lambda: arrived(g, slot))
        pass_on(g, slot, beside, z >= plane)

    def plane_in(g, plane):
        @pl.when(z >= plane)
        def _():
            for column_x in (x, 1 - x):
                arrived(g, plane * PLANE + column_x * 2 + (1 - c))
            plane_scores(g, plane)

    key_at = lax.broadcasted_iota(jnp.int32, (span, across_q), 0)
    query_at = lax.broadcasted_iota(jnp.int32, (span, across_q), 1) % span
    near_bias = jnp.where(key_at <= query_at, 0.0, FAR)
    seq_lane = lax.broadcasted_iota(jnp.int32, (HEAD_DIM, seqs * span), 1) // span
    ones_at = lax.broadcasted_iota(jnp.int32, (16, seqs * span), 0)
    ones_lane = lax.broadcasted_iota(jnp.int32, (16, seqs * span), 1) // span

    def near_part(g):
        for s in range(seqs):
            block = sk_buf[s * span : (s + 1) * span, :].astype(f32)
            if g != s % 2:
                block = swap(block)
            block = jnp.where(low if s % 2 == 0 else ~low, block, 0.0).astype(bf16)
            lanes = slice((s // 2) * 128, (s // 2 + 1) * 128)
            score = dot_t(block, qn[g, :, lanes]) + near_bias
            near_s[g, s * span : (s + 1) * span, :] = score
            tops[g, n + s] = jnp.max(score.reshape(span // 8, 8, across_q), axis=0)
            value = svt[g * HEAD_DIM : (g + 1) * HEAD_DIM, :].astype(f32)
            vals[g, s * HEAD_DIM : (s + 1) * HEAD_DIM, 0:near_keys] = jnp.where(
                seq_lane == s, value, 0.0
            ).astype(bf16)
        vals[g, stack : stack + 16, 0:near_keys] = jnp.where(
            ones_at == ones_lane, 1.0, 0.0
        ).astype(bf16)

    slots = n * entries
    entry_row = lax.broadcasted_iota(jnp.int32, (slots, 128), 0)
    entry_half = lax.broadcasted_iota(jnp.int32, (slots, 128), 1) // HEAD_DIM
    entry_seq = (entry_row % entries) // count
    slot_row = lax.broadcasted_iota(jnp.int32, (slots, across_q), 0)
    slot_query = lax.broadcasted_iota(jnp.int32, (slots, across_q), 1) % span
    slot_entry = (slot_row // entries) * count + slot_row % count
    entry_ok = (slot_entry >= 1) & (
        slot_entry * CMP_STRIDE + CMP_STRIDE - 1 <= me * span + slot_query
    )
    entry_bias = jnp.where(entry_ok, 0.0, FAR)
    value_lane = (lax.broadcasted_iota(jnp.int32, (HEAD_DIM, slots), 1) % entries) // count
    total_row = lax.broadcasted_iota(jnp.int32, (16, slots), 0)
    total_lane = (lax.broadcasted_iota(jnp.int32, (16, slots), 1) % entries) // count
    group_row = lax.broadcasted_iota(jnp.int32, (entries, across_q), 0)

    def cmp_part(g):
        part = slice(g * entries, (g + 1) * entries)
        both = ents[:, part, :].reshape(slots, 128).astype(f32)
        twice = jnp.where(entry_half == 0, both, swap(both))
        keys = jnp.concatenate(
            [jnp.where(entry_seq == 2 * p + entry_half, twice, 0.0) for p in range(pairs)], axis=1
        ).astype(bf16)
        score = (dot_t(keys, qn[g]) + entry_bias).reshape(n, entries, across_q)
        top = jnp.max(score, axis=0)
        for step in (1, 2):
            top = jnp.maximum(
                top,
                jnp.where(
                    (group_row // step) % 2 == 0,
                    pltpu.roll(top, entries - step, 0),
                    pltpu.roll(top, step, 0),
                ),
            )
        top = jnp.maximum(top, -1e29)
        w = jnp.exp(score - top[None]).reshape(slots, across_q).astype(bf16)
        value = jnp.transpose(both)[HEAD_DIM:]
        left = [jnp.where(value_lane == s, value, 0.0) for s in range(seqs)]
        left.append(jnp.where(total_row == total_lane, 1.0, 0.0))
        made = dot(jnp.concatenate(left, axis=0).astype(bf16), w)
        for s in range(seqs):
            total = jnp.maximum(made[stack + s : stack + s + 1], 1.0)
            row = g * seqs + s
            factor = gate_buf[row : row + 1, :] / total
            block = slice(s * HEAD_DIM, (s + 1) * HEAD_DIM)
            mix[g, block, :] = made[block] * factor

    def plane_scores(g, plane):
        base = plane * PLANE
        first_lane = value_lanes(plane).start
        left = []
        for i in range(PLANE):
            block = blobs[g, base + i].astype(f32)
            turned = swap(block)
            twice = jnp.where(low, block, turned)
            tiles = []
            for p in range(pairs):
                r0, r1 = 4 * p + g, 4 * p + 2 + g
                flag = jnp.where(
                    low_row, hits[base + i, r0 : r0 + 1], hits[base + i, r1 : r1 + 1]
                )
                tiles.append(twice * flag)
            left.append(jnp.concatenate(tiles, axis=1))
            if i % 2 == 0:
                before = turned
            else:
                value = jnp.where(low, before, block)
                lanes = slice(first_lane + (i - 1) * span, first_lane + (i + 1) * span)
                flags = [
                    jnp.where(low_row, hits[base + i - 1, r : r + 1], hits[base + i, r : r + 1])
                    for r in range(g, 2 * seqs, 2)
                ]
                for s in range(seqs):
                    vals[g, s * HEAD_DIM : (s + 1) * HEAD_DIM, lanes] = (value * flags[s]).astype(
                        bf16
                    )
                flags.append(jnp.zeros((16 - seqs, 128), f32))
                vals[g, stack : stack + 16, lanes] = jnp.concatenate(flags, axis=0).astype(bf16)
        score = dot_t(jnp.concatenate(left, axis=0).astype(bf16), qn[g])
        far_s[g, base * span : base * span + plane_keys, :] = score
        for i in range(PLANE):
            block = score[i * span : (i + 1) * span].reshape(span // 8, 8, across_q)
            tops[g, base + i] = jnp.max(block, axis=0)

    def flag_of(b):
        return jnp.concatenate([hits[b], hits[b]], axis=1) > 0

    def far_base(g):
        blocks = range(PLANE, n)
        refs = {b: jnp.full((1, across_q), 1e30, f32) for b in blocks}
        flags = {b: flag_of(b) for b in blocks}
        for s in range(seqs):
            r = 2 * s + g
            top = tops[g, n + s]
            for b in blocks:
                top = jnp.maximum(top, jnp.where(flags[b][r : r + 1], tops[g, b], FAR))
            top = jnp.max(top, axis=0, keepdims=True)
            base_top[g, s : s + 1, :] = top
            for b in blocks:
                refs[b] = jnp.where(flags[b][r : r + 1], top, refs[b])
            part = slice(s * span, (s + 1) * span)
            probs[part, :] = jnp.exp(near_s[g, part, :] - top).astype(bf16)
        for b in blocks:
            block = jnp.exp(far_s[g, b * span : (b + 1) * span, :] - refs[b]).astype(bf16)
            start = near_keys + (b - PLANE) * span
            probs[start : start + span, :] = block
        known = n * span
        base_sum[g] = dot(vals[g, :, :known], probs[...])

    def far_part(g):
        refs = [jnp.full((1, across_q), 1e30, f32) for _ in range(PLANE)]
        flags = [flag_of(b) for b in range(PLANE)]
        scales = []
        for s in range(seqs):
            r = 2 * s + g
            top = jnp.where(flags[0][r : r + 1], tops[g, 0], FAR)
            for b in range(1, PLANE):
                top = jnp.maximum(top, jnp.where(flags[b][r : r + 1], tops[g, b], FAR))
            before = base_top[g, s : s + 1, :]
            top = jnp.maximum(jnp.max(top, axis=0, keepdims=True), before)
            scales.append(jnp.exp(before - top))
            for b in range(PLANE):
                refs[b] = jnp.where(flags[b][r : r + 1], top, refs[b])
        w = jnp.concatenate(
            [
                jnp.exp(far_s[g, b * span : (b + 1) * span, :] - refs[b]).astype(bf16)
                for b in range(PLANE)
            ],
            axis=0,
        )
        made = dot(vals[g, :, n * span :], w)
        for p in range(pairs):
            tiles = []
            for s in (2 * p, 2 * p + 1):
                row = (2 + g) * seqs + s
                line = slice(stack + s, stack + s + 1)
                total = jnp.maximum(base_sum[g, line, :] * scales[s] + made[line], 1.0)
                factor = gate_buf[row : row + 1, :] / total
                block = slice(s * HEAD_DIM, (s + 1) * HEAD_DIM)
                old = base_sum[g, block, :] * (scales[s] * factor)
                tiles.append(mix[g, block, :] + old + made[block] * factor)
            both = jnp.concatenate(tiles, axis=0)
            for j in range(half // 2):
                lanes = slice(j * 128, (j + 1) * 128)
                flipped = jnp.transpose(both[:, lanes])
                a, b = flipped[:span], flipped[span:]
                part = slice(2 * p * span, (2 * p + 1) * span)
                own[g, part, lanes] = jnp.where(low, a, swap(b)).astype(bf16)
                part = slice((2 * p + 1) * span, (2 * p + 2) * span)
                own[g, part, lanes] = jnp.where(low, swap(a), b).astype(bf16)
            for s in (2 * p, 2 * p + 1):
                piece(g, s).start()

    def piece(g, s):
        part = pl.ds(s * span, span)
        return pltpu.make_async_remote_copy(
            src_ref=own.at[g, part], dst_ref=other.at[g, part], send_sem=half_send.at[0],
            recv_sem=half_recv.at[g * (s + 1)], device_id={"tp": 1 - column}, device_id_type=mesh_id,
        )

    spread = 2 * wg_ref.shape[1]
    logits = dot_t(wg[...].reshape(spread, rows.shape[1]), hidden)
    wide_at = lax.broadcasted_iota(jnp.int32, (1, seqs * span), 1)
    limit = jnp.zeros((1, seqs * span), jnp.int32)
    for s in range(seqs):
        limit = jnp.where(wide_at // span == s, lens[:, s : s + 1], limit)
    live = me * span + wide_at % span < limit
    for branch in range(2):
        base = branch * (spread // 2)
        mine = jnp.where(
            column == 0, logits[base : base + heads], logits[base + heads : base + 2 * heads]
        )
        mine = jnp.where(live, jax.nn.sigmoid(mine), 0.0)
        turned = [mine[:, p * 128 : (p + 1) * 128] for p in range(pairs)]
        swapped = [swap(t) for t in turned]
        for g in range(2):
            for s in range(seqs):
                for j in range(half // 2):
                    one = slice(g * half + 2 * j, g * half + 2 * j + 1)
                    two = slice(g * half + 2 * j + 1, g * half + 2 * j + 2)
                    t, w = turned[s // 2], swapped[s // 2]
                    if s % 2 == 0:
                        row = jnp.where(low_row, t[one], w[two])
                    else:
                        row = jnp.where(low_row, w[one], t[two])
                    line = (branch * 2 + g) * seqs + s
                    gate_buf[line : line + 1, j * 128 : (j + 1) * 128] = row

    for g in range(2):
        near_part(g)
    last = planes - 1
    in_side(0, last - 1)
    in_cross(0, last)
    for d in range(planes):
        entries_direct(d)
    for plane in range(last - 2, 0, -1):
        in_side(0, plane)
        in_cross(0, plane + 1)
    in_cross(0, 1)
    export(1)
    plane_in(0, last)
    for d in range(planes):
        entries_beside(d)
    cmp_part(0)
    for plane in range(last - 1, 1, -1):
        plane_in(0, plane)
    in_side(0, 0)
    in_cross(0, 0)
    plane_in(0, 1)
    far_base(0)
    plane_in(0, 0)
    far_part(0)
    for plane in range(last - 1, 0, -1):
        in_side(1, plane)
    in_cross(1, last)
    for plane in range(last - 1, 0, -1):
        in_cross(1, plane)
    in_side(1, 0)
    in_cross(1, 0)
    pltpu.make_async_copy(weight, weight, load_sem.at[11]).wait()
    cmp_part(1)
    for plane in range(last, 0, -1):
        plane_in(1, plane)
    far_base(1)
    plane_in(1, 0)
    far_part(1)

    squares = jnp.zeros((seqs * span, 1), f32)
    total = jnp.zeros((seqs * span, wide), f32)
    group = half * HEAD_DIM

    def gains(side, g):
        return gain[:, pl.ds(pl.multiple_of(side * depth + g * group, group), group)]

    for g in range(2):
        a = own[g].astype(f32)
        squares = squares + jnp.sum(a * a, axis=1, keepdims=True)
        scaled = (a * gains(column, g)).astype(bf16)
        total = total + dot(scaled, weight[0, g * group : (g + 1) * group, :])
    def all_pieces(ref):
        return pltpu.make_async_remote_copy(
            src_ref=ref, dst_ref=ref, send_sem=half_send.at[0], recv_sem=half_recv.at[0],
            device_id={"tp": 1 - column}, device_id_type=mesh_id,
        )

    all_pieces(other.at[0]).wait_recv()
    a = other[0].astype(f32)
    squares = squares + jnp.sum(a * a, axis=1, keepdims=True)
    scaled = (a * gains(1 - column, 0)).astype(bf16)
    partial[...] = total + dot(scaled, weight[1, :group, :])
    for s in range(seqs):
        piece(1, s).wait_recv()
        part = slice(s * span, (s + 1) * span)
        a = other[1, part, :].astype(f32)
        square = squares[part] + jnp.sum(a * a, axis=1, keepdims=True)
        row_scale = lax.rsqrt(square / (2 * depth) + norm_eps)
        scaled = (a * gains(1 - column, 1)).astype(bf16)
        done = partial[part, :] + dot(scaled, weight[1, group:, :])
        out_ref[part, :] = (done * row_scale).astype(bf16)

    all_pieces(own).wait_send()
    for b in range(1, n):
        pl.when(me == b)(lambda b=b: lists_copy(b).wait_send())
    everyone = pl.ds(0, 2 * planes + 1)
    pltpu.make_async_remote_copy(
        src_ref=ents.at[everyone], dst_ref=ents.at[everyone], send_sem=ent_send.at[0],
        recv_sem=ent_recv.at[0], device_id={"kv": (me + 1) % n}, device_id_type=mesh_id,
    ).wait_send()
    pltpu.make_async_remote_copy(
        src_ref=blobs.at[:, everyone], dst_ref=blobs.at[:, everyone], send_sem=blob_send.at[0],
        recv_sem=blob_recv.at[0, 0], device_id={"kv": (me + 1) % n}, device_id_type=mesh_id,
    ).wait_send()


def fused_shards(
    hidden_in,
    w_query,
    w_cmp_key,
    w_cmp_value,
    w_sel_key,
    w_sel_value,
    w_gate,
    cmp_key_in,
    cmp_key_out,
    cmp_value_in,
    cmp_value_out,
    out_gain,
    w_out,
    seq_lengths,
    chosen,
):
    seqs, span, width = hidden_in.shape
    n = lax.axis_size("kv")
    heads = w_query.shape[1] // HEAD_DIM
    total = seqs * span
    entries = total // CMP_STRIDE
    out_width = width // lax.axis_size("tp")
    small = w_sel_key.shape[1]
    half = heads // 2
    stack = seqs * HEAD_DIM
    across_q = half * span
    planes = n // PLANE
    anywhere = pl.BlockSpec(memory_space=pl.ANY)
    gate_rows = jnp.transpose(w_gate, (1, 2, 0))
    picks = chosen[:, 0].reshape(2 * seqs, TOPK)
    key_out, value_out = jnp.transpose(cmp_key_out), jnp.transpose(cmp_value_out)
    lens = seq_lengths[None]
    gain = out_gain[None]
    out = pl.pallas_call(
        functools.partial(layer_kernel, n, seqs, span, heads),
        in_specs=[anywhere] * 15,
        out_specs=pl.BlockSpec(memory_space=pltpu.VMEM),
        out_shape=pltpu.VMEM((total, out_width), bf16),
        scratch_shapes=[
            pltpu.VMEM(picks.shape, jnp.int32),
            pltpu.VMEM((total, width), bf16),
            pltpu.VMEM((width, 4 * small), bf16),
            pltpu.VMEM(key_out.shape, bf16),
            pltpu.VMEM(value_out.shape, bf16),
            pltpu.VMEM(cmp_key_in.shape, bf16),
            pltpu.VMEM(cmp_value_in.shape, bf16),
            pltpu.VMEM(w_query.shape, bf16),
            pltpu.VMEM(gate_rows.shape, bf16),
            pltpu.VMEM(lens.shape, jnp.int32),
            pltpu.VMEM(gain.shape, f32),
            pltpu.VMEM((2, heads * HEAD_DIM, out_width), bf16),
            pltpu.VMEM((2, across_q, stack), bf16),
            pltpu.VMEM((total, small), bf16),
            pltpu.VMEM((small, total), bf16),
            pltpu.VMEM((2, total, small), f32),
            pltpu.VMEM((4 * seqs, across_q), f32),
            pltpu.VMEM((n, 2 * seqs, 128), f32),
            pltpu.VMEM((n,) + picks.shape, jnp.int32),
            pltpu.VMEM((n, 2 * entries, 128), bf16),
            pltpu.VMEM((2, n, span, 128), bf16),
            pltpu.VMEM((2, total, across_q), f32),
            pltpu.VMEM((2, n * span, across_q), f32),
            pltpu.VMEM((2, n + seqs, 8, across_q), f32),
            pltpu.VMEM((2, 8, across_q), f32),
            pltpu.VMEM((n * span, across_q), bf16),
            pltpu.VMEM((2, stack + 16, across_q), f32),
            pltpu.VMEM((2, stack + 16, total + n * span), bf16),
            pltpu.VMEM((2, stack, across_q), f32),
            pltpu.VMEM((2, total, half * HEAD_DIM), bf16),
            pltpu.VMEM((2, total, half * HEAD_DIM), bf16),
            pltpu.VMEM((total, out_width), f32),
            pltpu.SemaphoreType.DMA((12,)),
            pltpu.SemaphoreType.DMA((1,)),
            pltpu.SemaphoreType.DMA((1,)),
            pltpu.SemaphoreType.DMA((1,)),
            pltpu.SemaphoreType.DMA((n,)),
            pltpu.SemaphoreType.DMA((1,)),
            pltpu.SemaphoreType.DMA((2, n)),
            pltpu.SemaphoreType.DMA((1,)),
            pltpu.SemaphoreType.DMA((1 + seqs,)),
        ],
        compiler_params=pltpu.CompilerParams(
            collective_id=0, has_side_effects=True, vmem_limit_bytes=VMEM_BYTES
        ),
        name="layer",
    )(
        picks, hidden_in.reshape(total, width), w_sel_key, w_sel_value, w_cmp_key, w_cmp_value,
        key_out, value_out, cmp_key_in, cmp_value_in, w_query, gate_rows, lens, gain, w_out,
    )
    return out.reshape(seqs, span, out_width)


def fits(mesh):
    n = mesh.shape["kv"]
    return mesh.shape["tp"] == 2 and n % PLANE == 0 and 3 * PLANE <= n <= 32


def solution(mesh):
    placed = (
        P(None, "kv", None),
        P(None, "tp"),
        P(None, "tp"),
        P(None, "tp"),
        P(None, "tp"),
        P(None, "tp"),
        P(),
        P(),
        P(),
        P(),
        P(),
        P(),
        P(),
        P(),
        P(None, "kv", "tp", None),
    )
    return jax.shard_map(
        fused_shards if fits(mesh) else shards, mesh=mesh, in_specs=placed, out_specs=P(None, "kv", "tp"), check_vma=False
    )
```

```python
import functools
import math

import jax
import jax.numpy as jnp
from jax import lax
from jax.experimental import pallas as pl
from jax.experimental.pallas import tpu as pltpu
from jax.sharding import PartitionSpec as P

HEADS = 16
HEAD_DIM = 64
CMP_STRIDE = 16
CMP_BLOCK = 32
TOPK = 16


theta_base = 500000.0
norm_eps = 1e-06


def rotate(values, positions):
    width = values.shape[-1]
    half = width // 2
    inverse = jnp.exp(
        -jnp.log(jnp.float32(theta_base)) * jnp.arange(0, width, 2).astype(jnp.float32) / width
    )
    angle = positions.astype(jnp.float32)[:, None] * inverse[None, :]
    cosine = jnp.cos(angle)[:, None, :]
    sine = jnp.sin(angle)[:, None, :]
    first = values[..., :half]
    second = values[..., half:]
    return jnp.concatenate(
        [first * cosine - second * sine, second * cosine + first * sine], axis=-1
    )


def masked_weights(scores, valid):
    top = jnp.max(jnp.where(valid, scores, -1e30), axis=-1, keepdims=True)
    expd = jnp.where(valid, jnp.exp(scores - top), 0.0)
    total = jnp.sum(expd, axis=-1, keepdims=True)
    return (expd / jnp.maximum(total, 1.0)).astype(jnp.bfloat16)


def compress(raw, prior, weight_in, weight_out):
    seqs, span, groups, width = raw.shape
    extended = jnp.concatenate([prior, raw], axis=1)
    count = span // CMP_STRIDE
    front = extended[:, :span].reshape(seqs, count, CMP_STRIDE, groups, width)
    back = extended[:, CMP_STRIDE:].reshape(seqs, count, CMP_STRIDE, groups, width)
    window = jnp.concatenate([front, back], axis=2).transpose(0, 1, 3, 2, 4)
    window = window.reshape(seqs * count * groups, CMP_BLOCK * width)
    inner = jax.nn.gelu(jnp.dot(window, weight_in, preferred_element_type=jnp.float32)).astype(
        jnp.bfloat16
    )
    return jnp.dot(inner, weight_out, preferred_element_type=jnp.float32).reshape(
        seqs, count, groups, width
    )


def shards(
    hidden_in,
    w_query,
    w_cmp_key,
    w_cmp_value,
    w_sel_key,
    w_sel_value,
    w_gate,
    cmp_key_in,
    cmp_key_out,
    cmp_value_in,
    cmp_value_out,
    out_gain,
    w_out,
    seq_lengths,
    chosen,
):
    seqs, span, width = hidden_in.shape
    block_list = lax.axis_size("kv")
    place = lax.axis_index("kv")
    column = lax.axis_index("tp")
    local_heads = w_query.shape[1] // HEAD_DIM
    local_groups = w_sel_key.shape[1] // HEAD_DIM
    per_group = local_heads // local_groups
    count = span // CMP_STRIDE
    scale = HEAD_DIM ** (-0.5)
    rows = hidden_in.reshape(seqs * span, width)
    positions = place * span + jnp.arange(span, dtype=jnp.int32)

    def project(weight_matrix, heads):
        return jnp.dot(rows, weight_matrix, preferred_element_type=jnp.float32).reshape(
            seqs, span, heads, HEAD_DIM
        )

    queries = rotate(project(w_query, local_heads), positions).astype(jnp.bfloat16)
    sel_pairs = jnp.concatenate(
        [rotate(project(w_sel_key, local_groups), positions), project(w_sel_value, local_groups)],
        axis=-1,
    ).astype(jnp.bfloat16)
    raw_pairs = jnp.concatenate(
        [project(w_cmp_key, local_groups), project(w_cmp_value, local_groups)], axis=-1
    ).astype(jnp.bfloat16)
    prior = jnp.zeros((seqs, CMP_STRIDE, local_groups, HEAD_DIM), jnp.bfloat16)
    ends = place * span + jnp.arange(count, dtype=jnp.int32) * CMP_STRIDE + CMP_STRIDE - 1
    cmp_keys = rotate(compress(raw_pairs[..., :HEAD_DIM], prior, cmp_key_in, cmp_key_out), ends)
    cmp_values = compress(raw_pairs[..., HEAD_DIM:], prior, cmp_value_in, cmp_value_out)
    cmp_piece = jnp.concatenate(
        [cmp_keys.astype(jnp.bfloat16), cmp_values.astype(jnp.bfloat16)], axis=-1
    )[:, None]
    picks = chosen[:, 0]
    every_list = lax.all_gather(picks[None, :, :, 1:], "kv", axis=0, tiled=True)
    named = jnp.any(every_list == place, axis=(0, 3)).astype(jnp.int32)
    seq_ids = jnp.arange(seqs, dtype=jnp.int32)[:, None]
    exported_seq = jnp.sum(named * seq_ids, axis=0)
    selector = seq_ids == exported_seq[None, :]
    export = jnp.sum(
        jnp.where(selector[:, None, :, None], sel_pairs, jnp.zeros((), jnp.bfloat16)), axis=0
    )
    export = export[None]
    remote_pairs, remote_entries = (
        lax.all_gather(export, "kv", axis=0, tiled=True),
        lax.all_gather(cmp_piece, "kv", axis=1, tiled=True),
    )
    gate_all = jnp.dot(rows, w_gate.reshape(width, 2 * HEADS), preferred_element_type=jnp.float32)
    gate_all = gate_all.reshape(seqs, span, 2, HEADS)
    gates = jax.nn.sigmoid(lax.dynamic_slice_in_dim(gate_all, column * local_heads, local_heads, 3))
    entry = jnp.arange(block_list * count, dtype=jnp.int32)
    entry_end = entry * CMP_STRIDE + CMP_STRIDE - 1
    cmp_valid = ((entry >= 1)[None, :] & (entry_end[None, :] <= positions[:, None]))[None, None]
    key_pos = jnp.arange(span, dtype=jnp.int32)
    own_valid = key_pos[None, :] <= key_pos[:, None]

    def one_sequence(args):
        seq_queries, seq_entries, seq_picks, seq_pairs, seq_gates, seq_length = args
        block_q = seq_queries.reshape(span, local_groups, per_group, HEAD_DIM)
        entries = seq_entries.reshape(block_list * count, local_groups, 2 * HEAD_DIM)
        scores = (
            jnp.einsum(
                "qghd,egd->ghqe",
                block_q,
                entries[..., :HEAD_DIM],
                preferred_element_type=jnp.float32,
            )
            * scale
        )
        weights = masked_weights(scores, cmp_valid)
        cmp_out = jnp.einsum(
            "ghqe,egd->qghd", weights, entries[..., HEAD_DIM:], preferred_element_type=jnp.float32
        )
        far = jnp.maximum(seq_picks[:, 1:], 0)
        fetched = jax.vmap(lambda table, index: table[index], in_axes=(2, 0))(remote_pairs, far)
        near = jnp.transpose(seq_pairs, (1, 0, 2))[:, None]
        pairs = jnp.concatenate([near, fetched], axis=1).reshape(
            local_groups, TOPK * span, 2 * HEAD_DIM
        )
        far_live = jnp.broadcast_to(
            (seq_picks[:, 1:] >= 0)[:, None, :, None], (local_groups, span, TOPK - 1, span)
        )
        near_live = jnp.broadcast_to(own_valid[None, :, None, :], (local_groups, span, 1, span))
        sel_valid = jnp.concatenate([near_live, far_live], axis=2).reshape(
            local_groups, 1, span, TOPK * span
        )
        scores_s = (
            jnp.einsum(
                "qghd,gmd->ghqm", block_q, pairs[..., :HEAD_DIM], preferred_element_type=jnp.float32
            )
            * scale
        )
        weights_s = masked_weights(scores_s, sel_valid)
        sel_out = jnp.einsum(
            "ghqm,gmd->qghd", weights_s, pairs[..., HEAD_DIM:], preferred_element_type=jnp.float32
        )
        split = seq_gates.reshape(span, 2, local_groups, per_group, 1)
        mixed = split[:, 0] * cmp_out + split[:, 1] * sel_out
        mixed = jnp.where((positions < seq_length)[:, None, None, None], mixed, 0.0)
        return mixed.reshape(span, local_heads * HEAD_DIM).astype(jnp.bfloat16)

    mixed = lax.map(one_sequence, (queries, remote_entries, picks, sel_pairs, gates, seq_lengths))
    mixed = mixed.reshape(seqs * span, local_heads * HEAD_DIM)
    out_width = width // lax.axis_size("tp")
    own_columns = lax.dynamic_slice_in_dim(w_out, column * out_width, out_width, 1)
    piece_wide = lax.all_gather(mixed, "tp", axis=1, tiled=True).astype(jnp.float32)
    scaled_piece = (piece_wide * out_gain[None, :]).astype(jnp.bfloat16)
    total = jnp.dot(scaled_piece, own_columns, preferred_element_type=jnp.float32)
    squares = jnp.sum(piece_wide * piece_wide, axis=-1)
    row_scale = lax.rsqrt(squares / (HEADS * HEAD_DIM) + norm_eps)
    return (total * row_scale[:, None]).astype(jnp.bfloat16).reshape(seqs, span, out_width)


FAR = -1e30
PLANE = 4
VMEM_BYTES = 60 * 1024 * 1024
f32 = jnp.float32
bf16 = jnp.bfloat16


def dot(a, b):
    return jnp.dot(a, b, preferred_element_type=f32)


def dot_t(a, b):
    return lax.dot_general(a, b, (((1,), (1,)), ((), ())), preferred_element_type=f32)


def swap(values):
    return pltpu.roll(values, HEAD_DIM, 1)


def turn(values, cosine, sine):
    lane = lax.broadcasted_iota(jnp.int32, values.shape, 1)
    other = jnp.where(
        lane % HEAD_DIM < HEAD_DIM // 2,
        pltpu.roll(values, 128 - HEAD_DIM // 2, 1),
        pltpu.roll(values, HEAD_DIM // 2, 1),
    )
    return values * cosine + other * sine


def gelu(x):
    return 0.5 * x * (1.0 + jnp.tanh(0.7978845608028654 * (x + 0.044715 * (x * x * x))))


def layer_kernel(
    n, seqs, span, heads,
    picks_ref, rows_ref, wsk_ref, wsv_ref, wck_ref, wcv_ref, kout_ref, vout_ref, kin_ref, vin_ref,
    wq_ref, wg_ref, lens_ref, gain_ref, wout_ref,
    out_ref,
    picks, rows, ws, kout, vout, kin, vin, wq, wg, lens, gain, weight,
    qn, sk_buf, svt, raw, gate_buf, hits, lists, ents, blobs, near_s, far_s, tops, base_top,
    probs, base_sum, vals, mix, own, other, partial,
    load_sem, pick_send, pick_recv, ent_send, ent_recv, blob_send, blob_recv, half_send, half_recv,
):
    me = lax.axis_index("kv")
    column = lax.axis_index("tp")
    planes = n // PLANE
    z, x, c = me // PLANE, (me // 2) % 2, me % 2
    depth = heads * HEAD_DIM
    wide = out_ref.shape[1]
    count = span // CMP_STRIDE
    entries = seqs * count
    half = heads // 2
    stack = seqs * HEAD_DIM
    across_q = half * span
    pairs = seqs // 2
    mesh_id = pl.DeviceIdType.MESH

    barrier = pltpu.get_barrier_semaphore()
    for d in range(1, n):
        pl.semaphore_signal(
            barrier, inc=1, device_id={"kv": (me + d) % n}, device_id_type=mesh_id
        )
    pl.semaphore_signal(barrier, inc=1, device_id={"tp": 1 - column}, device_id_type=mesh_id)

    jobs = [(picks_ref, picks), (rows_ref, rows)]
    for i, ref in enumerate((wsk_ref, wsv_ref, wck_ref, wcv_ref)):
        jobs.append((ref, ws.at[:, i * 128 : (i + 1) * 128]))
    jobs += [(kout_ref, kout), (vout_ref, vout), (kin_ref, kin), (vin_ref, vin)]
    jobs += [(wq_ref, wq), (wg_ref, wg), (lens_ref, lens), (gain_ref, gain)]
    for i in range(2):
        side = column if i == 0 else 1 - column
        block = wout_ref.at[
            pl.ds(pl.multiple_of(side * depth, depth), depth),
            pl.ds(pl.multiple_of(column * wide, wide), wide),
        ]
        jobs.append((block, weight.at[i]))
    shared = [0, 1, 2, 2, 2, 2, 3, 4, 5, 6, 7, 8, 9, 10, 11, 11]
    loads = [pltpu.make_async_copy(a, b, load_sem.at[i]) for i, (a, b) in zip(shared, jobs)]
    for load in loads:
        load.start()

    lane = lax.broadcasted_iota(jnp.int32, (span, 128), 1)
    low = lane < HEAD_DIM
    low_e = low[:entries]
    low_row = low[:1]
    at = lax.broadcasted_iota(jnp.int32, (span, 128), 0)
    sign = jnp.where(lane % HEAD_DIM < HEAD_DIM // 2, -1.0, 1.0)
    power = (lane % (HEAD_DIM // 2) * 2).astype(f32)
    freq = jnp.exp(-math.log(theta_base) * power / HEAD_DIM)
    angle = (me * span + at).astype(f32) * freq
    cosine = jnp.cos(angle)
    sine = jnp.sin(angle) * sign
    end = me * span + (at[:entries] % count) * CMP_STRIDE + CMP_STRIDE - 1
    angle = end.astype(f32) * freq[:entries]
    cosine_e = jnp.cos(angle)
    sine_e = jnp.sin(angle) * sign[:entries]

    near_keys = seqs * span
    plane_keys = PLANE * span

    def value_lanes(plane):
        start = near_keys + (plane + planes - 1) % planes * plane_keys
        return slice(start, start + plane_keys)

    for plane in range(1, planes):
        @pl.when(plane > z)
        def _():
            for i in range(PLANE):
                ents[plane * PLANE + i] = jnp.zeros((2 * entries, 128), bf16)
            keys = slice(plane * plane_keys, (plane + 1) * plane_keys)
            lanes = value_lanes(plane)
            for g in range(2):
                far_s[g, keys, :] = jnp.zeros((plane_keys, across_q), f32)
                vals[g, :, lanes] = jnp.zeros((stack + 16, plane_keys), bf16)
                tops[g, plane * PLANE : (plane + 1) * PLANE] = jnp.zeros(
                    (PLANE, 8, across_q), f32
                )

    loads[0].wait()
    pl.semaphore_wait(barrier, n)
    def send(src, dst, ssem, rsem, target, when=None):
        copy = pltpu.make_async_remote_copy(
            src_ref=src, dst_ref=dst, send_sem=ssem, recv_sem=rsem,
            device_id=target, device_id_type=mesh_id,
        )
        if when is None:
            copy.start()
        else:
            pl.when(when)(copy.start)

    for d in range(n - 1, 0, -1):
        send(
            picks, lists.at[me], pick_send.at[0], pick_recv.at[0], {"kv": (me + n - d) % n},
            me >= d,
        )

    def lists_copy(amount):
        ref = lists.at[pl.ds(0, amount)]
        return pltpu.make_async_remote_copy(
            src_ref=ref, dst_ref=ref, send_sem=pick_send.at[0], recv_sem=pick_recv.at[0],
            device_id={"kv": (me + 1) % n}, device_id_type=mesh_id,
        )

    slot_at = lax.broadcasted_iota(jnp.int32, (2 * seqs, TOPK), 1)
    listed = jnp.where(slot_at == 0, -1, picks[...])
    for b in range(n):
        hit = jnp.max(jnp.where(listed == b, 1.0, 0.0), axis=1, keepdims=True)
        hits[b] = jnp.broadcast_to(hit, (2 * seqs, 128))

    loads[1].wait()
    pltpu.make_async_copy(ws, ws, load_sem.at[2]).wait()
    made = dot(rows[...], ws[...])
    sv = []
    for s in range(seqs):
        part = slice(s * span, (s + 1) * span)
        sk_buf[part, :] = turn(made[part, :128], cosine, sine).astype(bf16)
    svt[...] = jnp.transpose(made[:, 128:256]).astype(bf16)
    raw[0] = made[:, 256:384].astype(bf16).astype(f32)
    raw[1] = made[:, 384:512].astype(bf16).astype(f32)
    first = at[:entries] % count == 0
    mid = CMP_STRIDE * HEAD_DIM
    results = []
    for load in loads[6:10]:
        load.wait()
    for branch, inner_weight, outer in ((0, kin, kout), (1, vin, vout)):
        left, right = [], []
        for j in range(0, CMP_STRIDE, 2):
            a = raw[branch, pl.ds(j, entries, stride=CMP_STRIDE), :]
            b = raw[branch, pl.ds(j + 1, entries, stride=CMP_STRIDE), :]
            left.append(jnp.where(low_e, a, swap(b)))
            right.append(jnp.where(low_e, swap(a), b))
        window = jnp.concatenate(
            [jnp.concatenate(left, axis=1), jnp.concatenate(right, axis=1)], axis=0
        ).astype(bf16)
        front = dot(window, inner_weight[:mid])
        back = dot(window, inner_weight[mid:])
        parts = []
        for g in range(2):
            shifted = pltpu.roll(front[g * entries : (g + 1) * entries], 1, 0)
            parts.append(back[g * entries : (g + 1) * entries] + jnp.where(first, 0.0, shifted))
        inner = gelu(jnp.concatenate(parts, axis=0)).astype(bf16)
        results.append(dot_t(inner, jnp.concatenate([outer[...], outer[...]], axis=0)))
    for g in range(2):
        part = slice(g * entries, (g + 1) * entries)
        key = turn(results[0][part], cosine_e, sine_e)
        ents[me, part, :] = jnp.where(low_e, key, results[1][part]).astype(bf16)
    across = z * PLANE + (1 - x) * 2 + c
    beside = z * PLANE + x * 2 + (1 - c)
    side_slot = x * 2 + c
    across_slot = (1 - x) * 2 + c
    def pass_entries(slot, dst, kind, when=None):
        ref = ents.at[slot]
        send(ref, ref, ent_send.at[0], ent_recv.at[kind], {"kv": dst}, when)

    def entries_copy(amount, kind):
        ref = ents.at[pl.ds(0, amount)]
        return pltpu.make_async_remote_copy(
            src_ref=ref, dst_ref=ref, send_sem=ent_send.at[0], recv_sem=ent_recv.at[kind],
            device_id={"kv": (me + 1) % n}, device_id_type=mesh_id,
        )

    for d in range(planes - 1, 0, -1):
        up = jnp.minimum(z + d, planes - 1) * PLANE
        pass_entries(me, up + side_slot, 0, z + d < planes)
        pass_entries(me, up + across_slot, 0, z + d < planes)
    pass_entries(me, across, 0)
    pass_entries(me, beside, 1)

    for load in loads[10:14]:
        load.wait()
    hidden = rows[...]
    for i in range(half):
        made = dot(hidden, wq[:, i * 128 : (i + 1) * 128])
        g, h = (2 * i) // half, (2 * i) % half
        turned = [
            turn(made[s * span : (s + 1) * span], cosine, sine) * (HEAD_DIM**-0.5)
            for s in range(seqs)
        ]
        for p in range(pairs):
            a, b = turned[2 * p], turned[2 * p + 1]
            even, odd = jnp.where(low, a, swap(b)), jnp.where(low, swap(a), b)
            lanes = slice(p * 128, (p + 1) * 128)
            qn[g, h * span : (h + 1) * span, lanes] = even.astype(bf16)
            qn[g, (h + 1) * span : (h + 2) * span, lanes] = odd.astype(bf16)
    for b in range(n - 1):
        pl.when(me == b)(lambda b=b: lists_copy(n - 1 - b).wait_recv())
    named = jnp.zeros((2 * seqs, TOPK), f32)
    for b in range(1, n):
        named = jnp.where((lists[b] == me) & (me < b), 1.0, named)
    named = jnp.max(jnp.where(slot_at == 0, 0.0, named), axis=1, keepdims=True)
    named = jnp.broadcast_to(named, (2 * seqs, 128))
    key = jnp.zeros((span, 128), f32)
    for s in range(seqs):
        flag = jnp.where(low_row, named[2 * s : 2 * s + 1], named[2 * s + 1 : 2 * s + 2])
        key = key + flag * sk_buf[s * span : (s + 1) * span, :].astype(f32)
    for g in range(2):
        value = jnp.zeros((HEAD_DIM, 128), f32)
        for p in range(pairs):
            r0, r1 = 4 * p + g, 4 * p + 2 + g
            flag = jnp.where(low_row, named[r0 : r0 + 1], named[r1 : r1 + 1])
            block = svt[g * HEAD_DIM : (g + 1) * HEAD_DIM, p * 128 : (p + 1) * 128]
            value = value + flag * block.astype(f32)
        value = value + swap(value)
        blobs[g, me] = jnp.where(low, key if g == 0 else swap(key), value).astype(bf16)

    def pass_on(g, slot, dst, kind, when=None):
        ref = blobs.at[g, slot]
        send(ref, ref, blob_send.at[0], blob_recv.at[g, slot // PLANE, kind], {"kv": dst}, when)

    def arrived(g, plane, kind):
        ref = blobs.at[g, pl.ds(0, 2)] if kind == 2 else blobs.at[g, 0]
        pltpu.make_async_remote_copy(
            src_ref=ref, dst_ref=ref, send_sem=blob_send.at[0],
            recv_sem=blob_recv.at[g, plane, kind], device_id={"kv": (me + 1) % n},
            device_id_type=mesh_id,
        ).wait_recv()

    def export(g):
        for d in range(1, planes):
            up = jnp.minimum(z + d, planes - 1) * PLANE
            pass_on(g, me, up + side_slot, 0, z + d < planes)
            pass_on(g, me, up + across_slot, 1, z + d < planes)
        pass_on(g, me, across, 1)
        pass_on(g, me, beside, 2)

    export(0)

    def entries_direct():
        for v in range(planes):
            pl.when(z == v)(lambda v=v: entries_copy(2 * v + 1, 0).wait_recv())
        for plane in range(planes):
            pass_entries(plane * PLANE + side_slot, beside, 1, z > plane)
            pass_entries(plane * PLANE + across_slot, beside, 1, z >= plane)

    def entries_beside():
        for v in range(planes):
            pl.when(z == v)(lambda v=v: entries_copy(2 * v + 2, 1).wait_recv())

    def in_side(g, plane):
        slot = plane * PLANE + side_slot
        pl.when(z > plane)(lambda: arrived(g, plane, 0))
        pass_on(g, slot, beside, 2, z > plane)

    def in_cross(g, plane):
        slot = plane * PLANE + across_slot
        pl.when(z >= plane)(lambda: arrived(g, plane, 1))
        pass_on(g, slot, beside, 2, z >= plane)

    def plane_in(g, plane):
        @pl.when(z >= plane)
        def _():
            arrived(g, plane, 2)
            plane_scores(g, plane)

    key_at = lax.broadcasted_iota(jnp.int32, (span, across_q), 0)
    query_at = lax.broadcasted_iota(jnp.int32, (span, across_q), 1) % span
    near_bias = jnp.where(key_at <= query_at, 0.0, FAR)
    seq_lane = lax.broadcasted_iota(jnp.int32, (HEAD_DIM, seqs * span), 1) // span
    ones_at = lax.broadcasted_iota(jnp.int32, (16, seqs * span), 0)
    ones_lane = lax.broadcasted_iota(jnp.int32, (16, seqs * span), 1) // span

    def near_part(g):
        for s in range(seqs):
            block = sk_buf[s * span : (s + 1) * span, :].astype(f32)
            if g != s % 2:
                block = swap(block)
            block = jnp.where(low if s % 2 == 0 else ~low, block, 0.0).astype(bf16)
            lanes = slice((s // 2) * 128, (s // 2 + 1) * 128)
            score = dot_t(block, qn[g, :, lanes]) + near_bias
            near_s[g, s * span : (s + 1) * span, :] = score
            tops[g, n + s] = jnp.max(score.reshape(span // 8, 8, across_q), axis=0)
            value = svt[g * HEAD_DIM : (g + 1) * HEAD_DIM, :].astype(f32)
            vals[g, s * HEAD_DIM : (s + 1) * HEAD_DIM, 0:near_keys] = jnp.where(
                seq_lane == s, value, 0.0
            ).astype(bf16)
        vals[g, stack : stack + 16, 0:near_keys] = jnp.where(
            ones_at == ones_lane, 1.0, 0.0
        ).astype(bf16)

    slots = n * entries
    entry_row = lax.broadcasted_iota(jnp.int32, (slots, 128), 0)
    entry_half = lax.broadcasted_iota(jnp.int32, (slots, 128), 1) // HEAD_DIM
    entry_seq = (entry_row % entries) // count
    slot_row = lax.broadcasted_iota(jnp.int32, (slots, across_q), 0)
    slot_query = lax.broadcasted_iota(jnp.int32, (slots, across_q), 1) % span
    slot_entry = (slot_row // entries) * count + slot_row % count
    entry_ok = (slot_entry >= 1) & (
        slot_entry * CMP_STRIDE + CMP_STRIDE - 1 <= me * span + slot_query
    )
    entry_bias = jnp.where(entry_ok, 0.0, FAR)
    value_lane = (lax.broadcasted_iota(jnp.int32, (HEAD_DIM, slots), 1) % entries) // count
    total_row = lax.broadcasted_iota(jnp.int32, (16, slots), 0)
    total_lane = (lax.broadcasted_iota(jnp.int32, (16, slots), 1) % entries) // count
    group_row = lax.broadcasted_iota(jnp.int32, (entries, across_q), 0)

    def cmp_part(g):
        part = slice(g * entries, (g + 1) * entries)
        both = ents[:, part, :].reshape(slots, 128).astype(f32)
        twice = jnp.where(entry_half == 0, both, swap(both))
        keys = jnp.concatenate(
            [jnp.where(entry_seq == 2 * p + entry_half, twice, 0.0) for p in range(pairs)], axis=1
        ).astype(bf16)
        score = (dot_t(keys, qn[g]) + entry_bias).reshape(n, entries, across_q)
        top = jnp.max(score, axis=0)
        for step in (1, 2):
            top = jnp.maximum(
                top,
                jnp.where(
                    (group_row // step) % 2 == 0,
                    pltpu.roll(top, entries - step, 0),
                    pltpu.roll(top, step, 0),
                ),
            )
        top = jnp.maximum(top, -1e29)
        w = jnp.exp(score - top[None]).reshape(slots, across_q).astype(bf16)
        value = jnp.transpose(both)[HEAD_DIM:]
        left = [jnp.where(value_lane == s, value, 0.0) for s in range(seqs)]
        left.append(jnp.where(total_row == total_lane, 1.0, 0.0))
        made = dot(jnp.concatenate(left, axis=0).astype(bf16), w)
        for s in range(seqs):
            total = jnp.maximum(made[stack + s : stack + s + 1], 1.0)
            row = g * seqs + s
            factor = gate_buf[row : row + 1, :] / total
            block = slice(s * HEAD_DIM, (s + 1) * HEAD_DIM)
            mix[g, block, :] = made[block] * factor

    def plane_scores(g, plane):
        base = plane * PLANE
        first_lane = value_lanes(plane).start
        left = []
        for i in range(PLANE):
            block = blobs[g, base + i].astype(f32)
            turned = swap(block)
            twice = jnp.where(low, block, turned)
            tiles = []
            for p in range(pairs):
                r0, r1 = 4 * p + g, 4 * p + 2 + g
                flag = jnp.where(
                    low_row, hits[base + i, r0 : r0 + 1], hits[base + i, r1 : r1 + 1]
                )
                tiles.append(twice * flag)
            left.append(jnp.concatenate(tiles, axis=1))
            if i % 2 == 0:
                before = turned
            else:
                value = jnp.where(low, before, block)
                lanes = slice(first_lane + (i - 1) * span, first_lane + (i + 1) * span)
                flags = [
                    jnp.where(low_row, hits[base + i - 1, r : r + 1], hits[base + i, r : r + 1])
                    for r in range(g, 2 * seqs, 2)
                ]
                for s in range(seqs):
                    vals[g, s * HEAD_DIM : (s + 1) * HEAD_DIM, lanes] = (value * flags[s]).astype(
                        bf16
                    )
                flags.append(jnp.zeros((16 - seqs, 128), f32))
                vals[g, stack : stack + 16, lanes] = jnp.concatenate(flags, axis=0).astype(bf16)
        score = dot_t(jnp.concatenate(left, axis=0).astype(bf16), qn[g])
        far_s[g, base * span : base * span + plane_keys, :] = score
        for i in range(PLANE):
            block = score[i * span : (i + 1) * span].reshape(span // 8, 8, across_q)
            tops[g, base + i] = jnp.max(block, axis=0)

    def flag_of(b):
        return jnp.concatenate([hits[b], hits[b]], axis=1) > 0

    def far_base(g):
        blocks = range(PLANE, n)
        refs = {b: jnp.full((1, across_q), 1e30, f32) for b in blocks}
        flags = {b: flag_of(b) for b in blocks}
        for s in range(seqs):
            r = 2 * s + g
            top = tops[g, n + s]
            for b in blocks:
                top = jnp.maximum(top, jnp.where(flags[b][r : r + 1], tops[g, b], FAR))
            top = jnp.max(top, axis=0, keepdims=True)
            base_top[g, s : s + 1, :] = top
            for b in blocks:
                refs[b] = jnp.where(flags[b][r : r + 1], top, refs[b])
            part = slice(s * span, (s + 1) * span)
            probs[part, :] = jnp.exp(near_s[g, part, :] - top).astype(bf16)
        for b in blocks:
            block = jnp.exp(far_s[g, b * span : (b + 1) * span, :] - refs[b]).astype(bf16)
            start = near_keys + (b - PLANE) * span
            probs[start : start + span, :] = block
        known = n * span
        base_sum[g] = dot(vals[g, :, :known], probs[...])

    def far_part(g):
        refs = [jnp.full((1, across_q), 1e30, f32) for _ in range(PLANE)]
        flags = [flag_of(b) for b in range(PLANE)]
        scales = []
        for s in range(seqs):
            r = 2 * s + g
            top = jnp.where(flags[0][r : r + 1], tops[g, 0], FAR)
            for b in range(1, PLANE):
                top = jnp.maximum(top, jnp.where(flags[b][r : r + 1], tops[g, b], FAR))
            before = base_top[g, s : s + 1, :]
            top = jnp.maximum(jnp.max(top, axis=0, keepdims=True), before)
            scales.append(jnp.exp(before - top))
            for b in range(PLANE):
                refs[b] = jnp.where(flags[b][r : r + 1], top, refs[b])
        w = jnp.concatenate(
            [
                jnp.exp(far_s[g, b * span : (b + 1) * span, :] - refs[b]).astype(bf16)
                for b in range(PLANE)
            ],
            axis=0,
        )
        made = dot(vals[g, :, n * span :], w)
        for p in range(pairs):
            tiles = []
            for s in (2 * p, 2 * p + 1):
                row = (2 + g) * seqs + s
                line = slice(stack + s, stack + s + 1)
                total = jnp.maximum(base_sum[g, line, :] * scales[s] + made[line], 1.0)
                factor = gate_buf[row : row + 1, :] / total
                block = slice(s * HEAD_DIM, (s + 1) * HEAD_DIM)
                old = base_sum[g, block, :] * (scales[s] * factor)
                tiles.append(mix[g, block, :] + old + made[block] * factor)
            both = jnp.concatenate(tiles, axis=0)
            for j in range(half // 2):
                lanes = slice(j * 128, (j + 1) * 128)
                flipped = jnp.transpose(both[:, lanes])
                a, b = flipped[:span], flipped[span:]
                part = slice(2 * p * span, (2 * p + 1) * span)
                own[g, part, lanes] = jnp.where(low, a, swap(b)).astype(bf16)
                part = slice((2 * p + 1) * span, (2 * p + 2) * span)
                own[g, part, lanes] = jnp.where(low, swap(a), b).astype(bf16)
            for s in (2 * p, 2 * p + 1):
                piece(g, s).start()

    def piece(g, s):
        part = pl.ds(s * span, span)
        return pltpu.make_async_remote_copy(
            src_ref=own.at[g, part], dst_ref=other.at[g, part], send_sem=half_send.at[0],
            recv_sem=half_recv.at[g * (s + 1)], device_id={"tp": 1 - column}, device_id_type=mesh_id,
        )

    spread = 2 * wg_ref.shape[1]
    logits = dot_t(wg[...].reshape(spread, rows.shape[1]), hidden)
    wide_at = lax.broadcasted_iota(jnp.int32, (1, seqs * span), 1)
    limit = jnp.zeros((1, seqs * span), jnp.int32)
    for s in range(seqs):
        limit = jnp.where(wide_at // span == s, lens[:, s : s + 1], limit)
    live = me * span + wide_at % span < limit
    for branch in range(2):
        base = branch * (spread // 2)
        mine = jnp.where(
            column == 0, logits[base : base + heads], logits[base + heads : base + 2 * heads]
        )
        mine = jnp.where(live, jax.nn.sigmoid(mine), 0.0)
        turned = [mine[:, p * 128 : (p + 1) * 128] for p in range(pairs)]
        swapped = [swap(t) for t in turned]
        for g in range(2):
            for s in range(seqs):
                for j in range(half // 2):
                    one = slice(g * half + 2 * j, g * half + 2 * j + 1)
                    two = slice(g * half + 2 * j + 1, g * half + 2 * j + 2)
                    t, w = turned[s // 2], swapped[s // 2]
                    if s % 2 == 0:
                        row = jnp.where(low_row, t[one], w[two])
                    else:
                        row = jnp.where(low_row, w[one], t[two])
                    line = (branch * 2 + g) * seqs + s
                    gate_buf[line : line + 1, j * 128 : (j + 1) * 128] = row

    for g in range(2):
        near_part(g)
    last = planes - 1
    in_side(0, last - 1)
    in_cross(0, last)
    entries_direct()
    plane_in(0, last)
    for plane in range(last - 2, 0, -1):
        in_side(0, plane)
        in_cross(0, plane + 1)
    in_cross(0, 1)
    export(1)
    entries_beside()
    cmp_part(0)
    for plane in range(last - 1, 1, -1):
        plane_in(0, plane)
    in_side(0, 0)
    in_cross(0, 0)
    plane_in(0, 1)
    far_base(0)
    plane_in(0, 0)
    far_part(0)
    for plane in range(last - 1, 0, -1):
        in_side(1, plane)
    in_cross(1, last)
    for plane in range(last - 1, 0, -1):
        in_cross(1, plane)
    in_side(1, 0)
    in_cross(1, 0)
    pltpu.make_async_copy(weight, weight, load_sem.at[11]).wait()
    cmp_part(1)
    for plane in range(last, 0, -1):
        plane_in(1, plane)
    far_base(1)
    plane_in(1, 0)
    far_part(1)

    squares = jnp.zeros((seqs * span, 1), f32)
    total = jnp.zeros((seqs * span, wide), f32)
    group = half * HEAD_DIM

    def gains(side, g):
        return gain[:, pl.ds(pl.multiple_of(side * depth + g * group, group), group)]

    for g in range(2):
        a = own[g].astype(f32)
        squares = squares + jnp.sum(a * a, axis=1, keepdims=True)
        scaled = (a * gains(column, g)).astype(bf16)
        total = total + dot(scaled, weight[0, g * group : (g + 1) * group, :])
    def all_pieces(ref):
        return pltpu.make_async_remote_copy(
            src_ref=ref, dst_ref=ref, send_sem=half_send.at[0], recv_sem=half_recv.at[0],
            device_id={"tp": 1 - column}, device_id_type=mesh_id,
        )

    for b in range(1, n):
        pl.when(me == b)(lambda b=b: lists_copy(b).wait_send())
    everyone = pl.ds(0, 2 * planes + 1)
    entries_copy(2 * planes + 1, 0).wait_send()
    pltpu.make_async_remote_copy(
        src_ref=blobs.at[:, everyone], dst_ref=blobs.at[:, everyone], send_sem=blob_send.at[0],
        recv_sem=blob_recv.at[0, 0, 0], device_id={"kv": (me + 1) % n}, device_id_type=mesh_id,
    ).wait_send()
    all_pieces(other.at[0]).wait_recv()
    a = other[0].astype(f32)
    squares = squares + jnp.sum(a * a, axis=1, keepdims=True)
    scaled = (a * gains(1 - column, 0)).astype(bf16)
    partial[...] = total + dot(scaled, weight[1, :group, :])
    for s in range(seqs):
        piece(1, s).wait_recv()
        part = slice(s * span, (s + 1) * span)
        a = other[1, part, :].astype(f32)
        square = squares[part] + jnp.sum(a * a, axis=1, keepdims=True)
        row_scale = lax.rsqrt(square / (2 * depth) + norm_eps)
        scaled = (a * gains(1 - column, 1)).astype(bf16)
        done = partial[part, :] + dot(scaled, weight[1, group:, :])
        out_ref[part, :] = (done * row_scale).astype(bf16)

    all_pieces(own).wait_send()


def fused_shards(
    hidden_in,
    w_query,
    w_cmp_key,
    w_cmp_value,
    w_sel_key,
    w_sel_value,
    w_gate,
    cmp_key_in,
    cmp_key_out,
    cmp_value_in,
    cmp_value_out,
    out_gain,
    w_out,
    seq_lengths,
    chosen,
):
    seqs, span, width = hidden_in.shape
    n = lax.axis_size("kv")
    heads = w_query.shape[1] // HEAD_DIM
    total = seqs * span
    entries = total // CMP_STRIDE
    out_width = width // lax.axis_size("tp")
    small = w_sel_key.shape[1]
    half = heads // 2
    stack = seqs * HEAD_DIM
    across_q = half * span
    planes = n // PLANE
    anywhere = pl.BlockSpec(memory_space=pl.ANY)
    gate_rows = jnp.transpose(w_gate, (1, 2, 0))
    picks = chosen[:, 0].reshape(2 * seqs, TOPK)
    key_out, value_out = jnp.transpose(cmp_key_out), jnp.transpose(cmp_value_out)
    lens = seq_lengths[None]
    gain = out_gain[None]
    out = pl.pallas_call(
        functools.partial(layer_kernel, n, seqs, span, heads),
        in_specs=[anywhere] * 15,
        out_specs=pl.BlockSpec(memory_space=pltpu.VMEM),
        out_shape=pltpu.VMEM((total, out_width), bf16),
        scratch_shapes=[
            pltpu.VMEM(picks.shape, jnp.int32),
            pltpu.VMEM((total, width), bf16),
            pltpu.VMEM((width, 4 * small), bf16),
            pltpu.VMEM(key_out.shape, bf16),
            pltpu.VMEM(value_out.shape, bf16),
            pltpu.VMEM(cmp_key_in.shape, bf16),
            pltpu.VMEM(cmp_value_in.shape, bf16),
            pltpu.VMEM(w_query.shape, bf16),
            pltpu.VMEM(gate_rows.shape, bf16),
            pltpu.VMEM(lens.shape, jnp.int32),
            pltpu.VMEM(gain.shape, f32),
            pltpu.VMEM((2, heads * HEAD_DIM, out_width), bf16),
            pltpu.VMEM((2, across_q, stack), bf16),
            pltpu.VMEM((total, small), bf16),
            pltpu.VMEM((small, total), bf16),
            pltpu.VMEM((2, total, small), f32),
            pltpu.VMEM((4 * seqs, across_q), f32),
            pltpu.VMEM((n, 2 * seqs, 128), f32),
            pltpu.VMEM((n,) + picks.shape, jnp.int32),
            pltpu.VMEM((n, 2 * entries, 128), bf16),
            pltpu.VMEM((2, n, span, 128), bf16),
            pltpu.VMEM((2, total, across_q), f32),
            pltpu.VMEM((2, n * span, across_q), f32),
            pltpu.VMEM((2, n + seqs, 8, across_q), f32),
            pltpu.VMEM((2, 8, across_q), f32),
            pltpu.VMEM((n * span, across_q), bf16),
            pltpu.VMEM((2, stack + 16, across_q), f32),
            pltpu.VMEM((2, stack + 16, total + n * span), bf16),
            pltpu.VMEM((2, stack, across_q), f32),
            pltpu.VMEM((2, total, half * HEAD_DIM), bf16),
            pltpu.VMEM((2, total, half * HEAD_DIM), bf16),
            pltpu.VMEM((total, out_width), f32),
            pltpu.SemaphoreType.DMA((12,)),
            pltpu.SemaphoreType.DMA((1,)),
            pltpu.SemaphoreType.DMA((1,)),
            pltpu.SemaphoreType.DMA((1,)),
            pltpu.SemaphoreType.DMA((2,)),
            pltpu.SemaphoreType.DMA((1,)),
            pltpu.SemaphoreType.DMA((2, planes, 3)),
            pltpu.SemaphoreType.DMA((1,)),
            pltpu.SemaphoreType.DMA((1 + seqs,)),
        ],
        compiler_params=pltpu.CompilerParams(
            collective_id=0, has_side_effects=True, vmem_limit_bytes=VMEM_BYTES
        ),
        name="layer",
    )(
        picks, hidden_in.reshape(total, width), w_sel_key, w_sel_value, w_cmp_key, w_cmp_value,
        key_out, value_out, cmp_key_in, cmp_value_in, w_query, gate_rows, lens, gain, w_out,
    )
    return out.reshape(seqs, span, out_width)


def fits(mesh):
    n = mesh.shape["kv"]
    return mesh.shape["tp"] == 2 and n % PLANE == 0 and 3 * PLANE <= n <= 32


def solution(mesh):
    placed = (
        P(None, "kv", None),
        P(None, "tp"),
        P(None, "tp"),
        P(None, "tp"),
        P(None, "tp"),
        P(None, "tp"),
        P(),
        P(),
        P(),
        P(),
        P(),
        P(),
        P(),
        P(),
        P(None, "kv", "tp", None),
    )
    return jax.shard_map(
        fused_shards if fits(mesh) else shards, mesh=mesh, in_specs=placed, out_specs=P(None, "kv", "tp"), check_vma=False
    )
```

```python
import functools
import math

import jax
import jax.numpy as jnp
from jax import lax
from jax.experimental import pallas as pl
from jax.experimental.pallas import tpu as pltpu
from jax.sharding import PartitionSpec as P

HEADS = 16
HEAD_DIM = 64
CMP_STRIDE = 16
CMP_BLOCK = 32
TOPK = 16


theta_base = 500000.0
norm_eps = 1e-06


def rotate(values, positions):
    width = values.shape[-1]
    half = width // 2
    inverse = jnp.exp(
        -jnp.log(jnp.float32(theta_base)) * jnp.arange(0, width, 2).astype(jnp.float32) / width
    )
    angle = positions.astype(jnp.float32)[:, None] * inverse[None, :]
    cosine = jnp.cos(angle)[:, None, :]
    sine = jnp.sin(angle)[:, None, :]
    first = values[..., :half]
    second = values[..., half:]
    return jnp.concatenate(
        [first * cosine - second * sine, second * cosine + first * sine], axis=-1
    )


def masked_weights(scores, valid):
    top = jnp.max(jnp.where(valid, scores, -1e30), axis=-1, keepdims=True)
    expd = jnp.where(valid, jnp.exp(scores - top), 0.0)
    total = jnp.sum(expd, axis=-1, keepdims=True)
    return (expd / jnp.maximum(total, 1.0)).astype(jnp.bfloat16)


def compress(raw, prior, weight_in, weight_out):
    seqs, span, groups, width = raw.shape
    extended = jnp.concatenate([prior, raw], axis=1)
    count = span // CMP_STRIDE
    front = extended[:, :span].reshape(seqs, count, CMP_STRIDE, groups, width)
    back = extended[:, CMP_STRIDE:].reshape(seqs, count, CMP_STRIDE, groups, width)
    window = jnp.concatenate([front, back], axis=2).transpose(0, 1, 3, 2, 4)
    window = window.reshape(seqs * count * groups, CMP_BLOCK * width)
    inner = jax.nn.gelu(jnp.dot(window, weight_in, preferred_element_type=jnp.float32)).astype(
        jnp.bfloat16
    )
    return jnp.dot(inner, weight_out, preferred_element_type=jnp.float32).reshape(
        seqs, count, groups, width
    )


def shards(
    hidden_in,
    w_query,
    w_cmp_key,
    w_cmp_value,
    w_sel_key,
    w_sel_value,
    w_gate,
    cmp_key_in,
    cmp_key_out,
    cmp_value_in,
    cmp_value_out,
    out_gain,
    w_out,
    seq_lengths,
    chosen,
):
    seqs, span, width = hidden_in.shape
    block_list = lax.axis_size("kv")
    place = lax.axis_index("kv")
    column = lax.axis_index("tp")
    local_heads = w_query.shape[1] // HEAD_DIM
    local_groups = w_sel_key.shape[1] // HEAD_DIM
    per_group = local_heads // local_groups
    count = span // CMP_STRIDE
    scale = HEAD_DIM ** (-0.5)
    rows = hidden_in.reshape(seqs * span, width)
    positions = place * span + jnp.arange(span, dtype=jnp.int32)

    def project(weight_matrix, heads):
        return jnp.dot(rows, weight_matrix, preferred_element_type=jnp.float32).reshape(
            seqs, span, heads, HEAD_DIM
        )

    queries = rotate(project(w_query, local_heads), positions).astype(jnp.bfloat16)
    sel_pairs = jnp.concatenate(
        [rotate(project(w_sel_key, local_groups), positions), project(w_sel_value, local_groups)],
        axis=-1,
    ).astype(jnp.bfloat16)
    raw_pairs = jnp.concatenate(
        [project(w_cmp_key, local_groups), project(w_cmp_value, local_groups)], axis=-1
    ).astype(jnp.bfloat16)
    prior = jnp.zeros((seqs, CMP_STRIDE, local_groups, HEAD_DIM), jnp.bfloat16)
    ends = place * span + jnp.arange(count, dtype=jnp.int32) * CMP_STRIDE + CMP_STRIDE - 1
    cmp_keys = rotate(compress(raw_pairs[..., :HEAD_DIM], prior, cmp_key_in, cmp_key_out), ends)
    cmp_values = compress(raw_pairs[..., HEAD_DIM:], prior, cmp_value_in, cmp_value_out)
    cmp_piece = jnp.concatenate(
        [cmp_keys.astype(jnp.bfloat16), cmp_values.astype(jnp.bfloat16)], axis=-1
    )[:, None]
    picks = chosen[:, 0]
    every_list = lax.all_gather(picks[None, :, :, 1:], "kv", axis=0, tiled=True)
    named = jnp.any(every_list == place, axis=(0, 3)).astype(jnp.int32)
    seq_ids = jnp.arange(seqs, dtype=jnp.int32)[:, None]
    exported_seq = jnp.sum(named * seq_ids, axis=0)
    selector = seq_ids == exported_seq[None, :]
    export = jnp.sum(
        jnp.where(selector[:, None, :, None], sel_pairs, jnp.zeros((), jnp.bfloat16)), axis=0
    )
    export = export[None]
    remote_pairs, remote_entries = (
        lax.all_gather(export, "kv", axis=0, tiled=True),
        lax.all_gather(cmp_piece, "kv", axis=1, tiled=True),
    )
    gate_all = jnp.dot(rows, w_gate.reshape(width, 2 * HEADS), preferred_element_type=jnp.float32)
    gate_all = gate_all.reshape(seqs, span, 2, HEADS)
    gates = jax.nn.sigmoid(lax.dynamic_slice_in_dim(gate_all, column * local_heads, local_heads, 3))
    entry = jnp.arange(block_list * count, dtype=jnp.int32)
    entry_end = entry * CMP_STRIDE + CMP_STRIDE - 1
    cmp_valid = ((entry >= 1)[None, :] & (entry_end[None, :] <= positions[:, None]))[None, None]
    key_pos = jnp.arange(span, dtype=jnp.int32)
    own_valid = key_pos[None, :] <= key_pos[:, None]

    def one_sequence(args):
        seq_queries, seq_entries, seq_picks, seq_pairs, seq_gates, seq_length = args
        block_q = seq_queries.reshape(span, local_groups, per_group, HEAD_DIM)
        entries = seq_entries.reshape(block_list * count, local_groups, 2 * HEAD_DIM)
        scores = (
            jnp.einsum(
                "qghd,egd->ghqe",
                block_q,
                entries[..., :HEAD_DIM],
                preferred_element_type=jnp.float32,
            )
            * scale
        )
        weights = masked_weights(scores, cmp_valid)
        cmp_out = jnp.einsum(
            "ghqe,egd->qghd", weights, entries[..., HEAD_DIM:], preferred_element_type=jnp.float32
        )
        far = jnp.maximum(seq_picks[:, 1:], 0)
        fetched = jax.vmap(lambda table, index: table[index], in_axes=(2, 0))(remote_pairs, far)
        near = jnp.transpose(seq_pairs, (1, 0, 2))[:, None]
        pairs = jnp.concatenate([near, fetched], axis=1).reshape(
            local_groups, TOPK * span, 2 * HEAD_DIM
        )
        far_live = jnp.broadcast_to(
            (seq_picks[:, 1:] >= 0)[:, None, :, None], (local_groups, span, TOPK - 1, span)
        )
        near_live = jnp.broadcast_to(own_valid[None, :, None, :], (local_groups, span, 1, span))
        sel_valid = jnp.concatenate([near_live, far_live], axis=2).reshape(
            local_groups, 1, span, TOPK * span
        )
        scores_s = (
            jnp.einsum(
                "qghd,gmd->ghqm", block_q, pairs[..., :HEAD_DIM], preferred_element_type=jnp.float32
            )
            * scale
        )
        weights_s = masked_weights(scores_s, sel_valid)
        sel_out = jnp.einsum(
            "ghqm,gmd->qghd", weights_s, pairs[..., HEAD_DIM:], preferred_element_type=jnp.float32
        )
        split = seq_gates.reshape(span, 2, local_groups, per_group, 1)
        mixed = split[:, 0] * cmp_out + split[:, 1] * sel_out
        mixed = jnp.where((positions < seq_length)[:, None, None, None], mixed, 0.0)
        return mixed.reshape(span, local_heads * HEAD_DIM).astype(jnp.bfloat16)

    mixed = lax.map(one_sequence, (queries, remote_entries, picks, sel_pairs, gates, seq_lengths))
    mixed = mixed.reshape(seqs * span, local_heads * HEAD_DIM)
    out_width = width // lax.axis_size("tp")
    own_columns = lax.dynamic_slice_in_dim(w_out, column * out_width, out_width, 1)
    piece_wide = lax.all_gather(mixed, "tp", axis=1, tiled=True).astype(jnp.float32)
    scaled_piece = (piece_wide * out_gain[None, :]).astype(jnp.bfloat16)
    total = jnp.dot(scaled_piece, own_columns, preferred_element_type=jnp.float32)
    squares = jnp.sum(piece_wide * piece_wide, axis=-1)
    row_scale = lax.rsqrt(squares / (HEADS * HEAD_DIM) + norm_eps)
    return (total * row_scale[:, None]).astype(jnp.bfloat16).reshape(seqs, span, out_width)


FAR = -1e30
PLANE = 4
VMEM_BYTES = 60 * 1024 * 1024
f32 = jnp.float32
bf16 = jnp.bfloat16


def dot(a, b):
    return jnp.dot(a, b, preferred_element_type=f32)


def dot_t(a, b):
    return lax.dot_general(a, b, (((1,), (1,)), ((), ())), preferred_element_type=f32)


def swap(values):
    return pltpu.roll(values, HEAD_DIM, 1)


def turn(values, cosine, sine):
    lane = lax.broadcasted_iota(jnp.int32, values.shape, 1)
    other = jnp.where(
        lane % HEAD_DIM < HEAD_DIM // 2,
        pltpu.roll(values, 128 - HEAD_DIM // 2, 1),
        pltpu.roll(values, HEAD_DIM // 2, 1),
    )
    return values * cosine + other * sine


def gelu(x):
    return 0.5 * x * (1.0 + jnp.tanh(0.7978845608028654 * (x + 0.044715 * (x * x * x))))


def layer_kernel(
    n, seqs, span, heads,
    picks_ref, rows_ref, wsk_ref, wsv_ref, wck_ref, wcv_ref, kout_ref, vout_ref, kin_ref, vin_ref,
    wq_ref, wg_ref, lens_ref, gain_ref, wout_ref,
    out_ref,
    picks, rows, ws, kout, vout, kin, vin, wq, wg, lens, gain, weight,
    qn, sk_buf, svt, raw, gate_buf, hits, lists, ents, blobs, near_s, far_s, tops, base_top,
    probs, base_sum, vals, mix, own, other, partial,
    load_sem, pick_send, pick_recv, ent_send, ent_recv, blob_send, blob_recv, half_send, half_recv,
):
    me = lax.axis_index("kv")
    column = lax.axis_index("tp")
    planes = n // PLANE
    z, x, c = me // PLANE, (me // 2) % 2, me % 2
    depth = heads * HEAD_DIM
    wide = out_ref.shape[1]
    count = span // CMP_STRIDE
    entries = seqs * count
    half = heads // 2
    stack = seqs * HEAD_DIM
    across_q = half * span
    pairs = seqs // 2
    mesh_id = pl.DeviceIdType.MESH

    barrier = pltpu.get_barrier_semaphore()
    for d in range(1, n):
        pl.semaphore_signal(
            barrier, inc=1, device_id={"kv": (me + d) % n}, device_id_type=mesh_id
        )
    pl.semaphore_signal(barrier, inc=1, device_id={"tp": 1 - column}, device_id_type=mesh_id)

    jobs = [(picks_ref, picks), (rows_ref, rows)]
    for i, ref in enumerate((wsk_ref, wsv_ref, wck_ref, wcv_ref)):
        jobs.append((ref, ws.at[:, i * 128 : (i + 1) * 128]))
    jobs += [(kout_ref, kout), (vout_ref, vout), (kin_ref, kin), (vin_ref, vin)]
    jobs += [(wq_ref, wq), (wg_ref, wg), (lens_ref, lens), (gain_ref, gain)]
    for i in range(2):
        side = column if i == 0 else 1 - column
        block = wout_ref.at[
            pl.ds(pl.multiple_of(side * depth, depth), depth),
            pl.ds(pl.multiple_of(column * wide, wide), wide),
        ]
        jobs.append((block, weight.at[i]))
    shared = [0, 1, 2, 2, 2, 2, 3, 4, 5, 6, 7, 8, 9, 10, 11, 11]
    loads = [pltpu.make_async_copy(a, b, load_sem.at[i]) for i, (a, b) in zip(shared, jobs)]
    for load in loads:
        load.start()

    lane = lax.broadcasted_iota(jnp.int32, (span, 128), 1)
    low = lane < HEAD_DIM
    low_e = low[:entries]
    low_row = low[:1]
    at = lax.broadcasted_iota(jnp.int32, (span, 128), 0)
    sign = jnp.where(lane % HEAD_DIM < HEAD_DIM // 2, -1.0, 1.0)
    power = (lane % (HEAD_DIM // 2) * 2).astype(f32)
    freq = jnp.exp(-math.log(theta_base) * power / HEAD_DIM)
    angle = (me * span + at).astype(f32) * freq
    cosine = jnp.cos(angle)
    sine = jnp.sin(angle) * sign
    end = me * span + (at[:entries] % count) * CMP_STRIDE + CMP_STRIDE - 1
    angle = end.astype(f32) * freq[:entries]
    cosine_e = jnp.cos(angle)
    sine_e = jnp.sin(angle) * sign[:entries]

    near_keys = seqs * span
    plane_keys = PLANE * span

    def value_lanes(plane):
        start = near_keys + (plane + planes - 1) % planes * plane_keys
        return slice(start, start + plane_keys)

    for plane in range(1, planes):
        @pl.when(plane > z)
        def _():
            for i in range(PLANE):
                ents[plane * PLANE + i] = jnp.zeros((2 * entries, 128), bf16)
            keys = slice(plane * plane_keys, (plane + 1) * plane_keys)
            lanes = value_lanes(plane)
            for g in range(2):
                far_s[g, keys, :] = jnp.zeros((plane_keys, across_q), f32)
                vals[g, :, lanes] = jnp.zeros((stack + 16, plane_keys), bf16)
                tops[g, plane * PLANE : (plane + 1) * PLANE] = jnp.zeros(
                    (PLANE, 8, across_q), f32
                )

    loads[0].wait()
    pl.semaphore_wait(barrier, n)
    def send(src, dst, ssem, rsem, target, when=None):
        copy = pltpu.make_async_remote_copy(
            src_ref=src, dst_ref=dst, send_sem=ssem, recv_sem=rsem,
            device_id=target, device_id_type=mesh_id,
        )
        if when is None:
            copy.start()
        else:
            pl.when(when)(copy.start)

    for d in range(n - 1, 0, -1):
        send(
            picks, lists.at[me], pick_send.at[0], pick_recv.at[0], {"kv": (me + n - d) % n},
            me >= d,
        )

    def lists_copy(amount):
        ref = lists.at[pl.ds(0, amount)]
        return pltpu.make_async_remote_copy(
            src_ref=ref, dst_ref=ref, send_sem=pick_send.at[0], recv_sem=pick_recv.at[0],
            device_id={"kv": (me + 1) % n}, device_id_type=mesh_id,
        )

    slot_at = lax.broadcasted_iota(jnp.int32, (2 * seqs, TOPK), 1)
    listed = jnp.where(slot_at == 0, -1, picks[...])
    for b in range(n):
        hit = jnp.max(jnp.where(listed == b, 1.0, 0.0), axis=1, keepdims=True)
        hits[b] = jnp.broadcast_to(hit, (2 * seqs, 128))

    loads[1].wait()
    pltpu.make_async_copy(ws, ws, load_sem.at[2]).wait()
    made = dot(rows[...], ws[...])
    sv = []
    for s in range(seqs):
        part = slice(s * span, (s + 1) * span)
        sk_buf[part, :] = turn(made[part, :128], cosine, sine).astype(bf16)
    svt[...] = jnp.transpose(made[:, 128:256]).astype(bf16)
    raw[0] = made[:, 256:384].astype(bf16).astype(f32)
    raw[1] = made[:, 384:512].astype(bf16).astype(f32)
    first = at[:entries] % count == 0
    mid = CMP_STRIDE * HEAD_DIM
    results = []
    for load in loads[6:10]:
        load.wait()
    for branch, inner_weight, outer in ((0, kin, kout), (1, vin, vout)):
        left, right = [], []
        for j in range(0, CMP_STRIDE, 2):
            a = raw[branch, pl.ds(j, entries, stride=CMP_STRIDE), :]
            b = raw[branch, pl.ds(j + 1, entries, stride=CMP_STRIDE), :]
            left.append(jnp.where(low_e, a, swap(b)))
            right.append(jnp.where(low_e, swap(a), b))
        window = jnp.concatenate(
            [jnp.concatenate(left, axis=1), jnp.concatenate(right, axis=1)], axis=0
        ).astype(bf16)
        front = dot(window, inner_weight[:mid])
        back = dot(window, inner_weight[mid:])
        parts = []
        for g in range(2):
            shifted = pltpu.roll(front[g * entries : (g + 1) * entries], 1, 0)
            parts.append(back[g * entries : (g + 1) * entries] + jnp.where(first, 0.0, shifted))
        inner = gelu(jnp.concatenate(parts, axis=0)).astype(bf16)
        results.append(dot_t(inner, jnp.concatenate([outer[...], outer[...]], axis=0)))
    for g in range(2):
        part = slice(g * entries, (g + 1) * entries)
        key = turn(results[0][part], cosine_e, sine_e)
        ents[me, part, :] = jnp.where(low_e, key, results[1][part]).astype(bf16)
    across = z * PLANE + (1 - x) * 2 + c
    beside = z * PLANE + x * 2 + (1 - c)
    side_slot = x * 2 + c
    across_slot = (1 - x) * 2 + c
    def pass_entries(slot, dst, kind, when=None):
        ref = ents.at[slot]
        send(ref, ref, ent_send.at[0], ent_recv.at[kind], {"kv": dst}, when)

    def entries_copy(amount, kind):
        ref = ents.at[pl.ds(0, amount)]
        return pltpu.make_async_remote_copy(
            src_ref=ref, dst_ref=ref, send_sem=ent_send.at[0], recv_sem=ent_recv.at[kind],
            device_id={"kv": (me + 1) % n}, device_id_type=mesh_id,
        )

    for d in range(planes - 1, 0, -1):
        up = jnp.minimum(z + d, planes - 1) * PLANE
        pass_entries(me, up + side_slot, 0, z + d < planes)
        pass_entries(me, up + across_slot, 0, z + d < planes)
    pass_entries(me, across, 0)
    pass_entries(me, beside, 1)

    for load in loads[10:14]:
        load.wait()
    hidden = rows[...]
    for i in range(half):
        made = dot(hidden, wq[:, i * 128 : (i + 1) * 128])
        g, h = (2 * i) // half, (2 * i) % half
        turned = [
            turn(made[s * span : (s + 1) * span], cosine, sine) * (HEAD_DIM**-0.5)
            for s in range(seqs)
        ]
        for p in range(pairs):
            a, b = turned[2 * p], turned[2 * p + 1]
            even, odd = jnp.where(low, a, swap(b)), jnp.where(low, swap(a), b)
            lanes = slice(p * 128, (p + 1) * 128)
            qn[g, h * span : (h + 1) * span, lanes] = even.astype(bf16)
            qn[g, (h + 1) * span : (h + 2) * span, lanes] = odd.astype(bf16)
    for b in range(n - 1):
        pl.when(me == b)(lambda b=b: lists_copy(n - 1 - b).wait_recv())
    named = jnp.zeros((2 * seqs, TOPK), f32)
    for b in range(1, n):
        named = jnp.where((lists[b] == me) & (me < b), 1.0, named)
    named = jnp.max(jnp.where(slot_at == 0, 0.0, named), axis=1, keepdims=True)
    named = jnp.broadcast_to(named, (2 * seqs, 128))
    key = jnp.zeros((span, 128), f32)
    for s in range(seqs):
        flag = jnp.where(low_row, named[2 * s : 2 * s + 1], named[2 * s + 1 : 2 * s + 2])
        key = key + flag * sk_buf[s * span : (s + 1) * span, :].astype(f32)
    for g in range(2):
        value = jnp.zeros((HEAD_DIM, 128), f32)
        for p in range(pairs):
            r0, r1 = 4 * p + g, 4 * p + 2 + g
            flag = jnp.where(low_row, named[r0 : r0 + 1], named[r1 : r1 + 1])
            block = svt[g * HEAD_DIM : (g + 1) * HEAD_DIM, p * 128 : (p + 1) * 128]
            value = value + flag * block.astype(f32)
        value = value + swap(value)
        blobs[g, me] = jnp.where(low, key if g == 0 else swap(key), value).astype(bf16)

    def pass_on(g, slot, dst, kind, when=None):
        ref = blobs.at[g, slot]
        send(ref, ref, blob_send.at[0], blob_recv.at[g, slot // PLANE, kind], {"kv": dst}, when)

    def arrived(g, plane, kind):
        ref = blobs.at[g, pl.ds(0, 2)] if kind == 2 else blobs.at[g, 0]
        pltpu.make_async_remote_copy(
            src_ref=ref, dst_ref=ref, send_sem=blob_send.at[0],
            recv_sem=blob_recv.at[g, plane, kind], device_id={"kv": (me + 1) % n},
            device_id_type=mesh_id,
        ).wait_recv()

    def export(g):
        for d in range(1, planes):
            up = jnp.minimum(z + d, planes - 1) * PLANE
            pass_on(g, me, up + side_slot, 0, z + d < planes)
            pass_on(g, me, up + across_slot, 1, z + d < planes)
        pass_on(g, me, across, 1)
        pass_on(g, me, beside, 2)

    export(0)

    def entries_direct():
        for v in range(planes):
            pl.when(z == v)(lambda v=v: entries_copy(2 * v + 1, 0).wait_recv())
        for plane in range(planes):
            pass_entries(plane * PLANE + side_slot, beside, 1, z > plane)
            pass_entries(plane * PLANE + across_slot, beside, 1, z >= plane)

    def entries_beside():
        for v in range(planes):
            pl.when(z == v)(lambda v=v: entries_copy(2 * v + 2, 1).wait_recv())

    def in_side(g, plane):
        slot = plane * PLANE + side_slot
        pl.when(z > plane)(lambda: arrived(g, plane, 0))
        pass_on(g, slot, beside, 2, z > plane)

    def in_cross(g, plane):
        slot = plane * PLANE + across_slot
        pl.when(z >= plane)(lambda: arrived(g, plane, 1))
        pass_on(g, slot, beside, 2, z >= plane)

    def plane_in(g, plane):
        @pl.when(z >= plane)
        def _():
            arrived(g, plane, 2)
            plane_scores(g, plane)

    key_at = lax.broadcasted_iota(jnp.int32, (span, across_q), 0)
    query_at = lax.broadcasted_iota(jnp.int32, (span, across_q), 1) % span
    near_bias = jnp.where(key_at <= query_at, 0.0, FAR)
    seq_lane = lax.broadcasted_iota(jnp.int32, (HEAD_DIM, seqs * span), 1) // span
    ones_at = lax.broadcasted_iota(jnp.int32, (16, seqs * span), 0)
    ones_lane = lax.broadcasted_iota(jnp.int32, (16, seqs * span), 1) // span

    def near_part(g):
        for s in range(seqs):
            block = sk_buf[s * span : (s + 1) * span, :].astype(f32)
            if g != s % 2:
                block = swap(block)
            block = jnp.where(low if s % 2 == 0 else ~low, block, 0.0).astype(bf16)
            lanes = slice((s // 2) * 128, (s // 2 + 1) * 128)
            score = dot_t(block, qn[g, :, lanes]) + near_bias
            near_s[g, s * span : (s + 1) * span, :] = score
            tops[g, n + s] = jnp.max(score.reshape(span // 8, 8, across_q), axis=0)
            value = svt[g * HEAD_DIM : (g + 1) * HEAD_DIM, :].astype(f32)
            vals[g, s * HEAD_DIM : (s + 1) * HEAD_DIM, 0:near_keys] = jnp.where(
                seq_lane == s, value, 0.0
            ).astype(bf16)
        vals[g, stack : stack + 16, 0:near_keys] = jnp.where(
            ones_at == ones_lane, 1.0, 0.0
        ).astype(bf16)

    slots = n * entries
    entry_row = lax.broadcasted_iota(jnp.int32, (slots, 128), 0)
    entry_half = lax.broadcasted_iota(jnp.int32, (slots, 128), 1) // HEAD_DIM
    entry_seq = (entry_row % entries) // count
    slot_row = lax.broadcasted_iota(jnp.int32, (slots, across_q), 0)
    slot_query = lax.broadcasted_iota(jnp.int32, (slots, across_q), 1) % span
    slot_entry = (slot_row // entries) * count + slot_row % count
    entry_ok = (slot_entry >= 1) & (
        slot_entry * CMP_STRIDE + CMP_STRIDE - 1 <= me * span + slot_query
    )
    entry_bias = jnp.where(entry_ok, 0.0, FAR)
    value_lane = (lax.broadcasted_iota(jnp.int32, (HEAD_DIM, slots), 1) % entries) // count
    total_row = lax.broadcasted_iota(jnp.int32, (16, slots), 0)
    total_lane = (lax.broadcasted_iota(jnp.int32, (16, slots), 1) % entries) // count
    group_row = lax.broadcasted_iota(jnp.int32, (entries, across_q), 0)

    def cmp_part(g):
        part = slice(g * entries, (g + 1) * entries)
        both = ents[:, part, :].reshape(slots, 128).astype(f32)
        twice = jnp.where(entry_half == 0, both, swap(both))
        keys = jnp.concatenate(
            [jnp.where(entry_seq == 2 * p + entry_half, twice, 0.0) for p in range(pairs)], axis=1
        ).astype(bf16)
        score = (dot_t(keys, qn[g]) + entry_bias).reshape(n, entries, across_q)
        top = jnp.max(score, axis=0)
        for step in (1, 2):
            top = jnp.maximum(
                top,
                jnp.where(
                    (group_row // step) % 2 == 0,
                    pltpu.roll(top, entries - step, 0),
                    pltpu.roll(top, step, 0),
                ),
            )
        top = jnp.maximum(top, -1e29)
        w = jnp.exp(score - top[None]).reshape(slots, across_q).astype(bf16)
        value = jnp.transpose(both)[HEAD_DIM:]
        left = [jnp.where(value_lane == s, value, 0.0) for s in range(seqs)]
        left.append(jnp.where(total_row == total_lane, 1.0, 0.0))
        made = dot(jnp.concatenate(left, axis=0).astype(bf16), w)
        for s in range(seqs):
            total = jnp.maximum(made[stack + s : stack + s + 1], 1.0)
            row = g * seqs + s
            factor = gate_buf[row : row + 1, :] / total
            block = slice(s * HEAD_DIM, (s + 1) * HEAD_DIM)
            mix[g, block, :] = made[block] * factor

    def plane_scores(g, plane):
        base = plane * PLANE
        first_lane = value_lanes(plane).start
        left = []
        for i in range(PLANE):
            block = blobs[g, base + i].astype(f32)
            turned = swap(block)
            twice = jnp.where(low, block, turned)
            tiles = []
            for p in range(pairs):
                r0, r1 = 4 * p + g, 4 * p + 2 + g
                flag = jnp.where(
                    low_row, hits[base + i, r0 : r0 + 1], hits[base + i, r1 : r1 + 1]
                )
                tiles.append(twice * flag)
            left.append(jnp.concatenate(tiles, axis=1))
            if i % 2 == 0:
                before = turned
            else:
                value = jnp.where(low, before, block)
                lanes = slice(first_lane + (i - 1) * span, first_lane + (i + 1) * span)
                flags = [
                    jnp.where(low_row, hits[base + i - 1, r : r + 1], hits[base + i, r : r + 1])
                    for r in range(g, 2 * seqs, 2)
                ]
                for s in range(seqs):
                    vals[g, s * HEAD_DIM : (s + 1) * HEAD_DIM, lanes] = (value * flags[s]).astype(
                        bf16
                    )
                flags.append(jnp.zeros((16 - seqs, 128), f32))
                vals[g, stack : stack + 16, lanes] = jnp.concatenate(flags, axis=0).astype(bf16)
        score = dot_t(jnp.concatenate(left, axis=0).astype(bf16), qn[g])
        far_s[g, base * span : base * span + plane_keys, :] = score
        for i in range(PLANE):
            block = score[i * span : (i + 1) * span].reshape(span // 8, 8, across_q)
            tops[g, base + i] = jnp.max(block, axis=0)

    def flag_of(b):
        return jnp.concatenate([hits[b], hits[b]], axis=1) > 0

    def far_base(g):
        blocks = range(PLANE, n)
        refs = {b: jnp.full((1, across_q), 1e30, f32) for b in blocks}
        flags = {b: flag_of(b) for b in blocks}
        for s in range(seqs):
            r = 2 * s + g
            top = tops[g, n + s]
            for b in blocks:
                top = jnp.maximum(top, jnp.where(flags[b][r : r + 1], tops[g, b], FAR))
            top = jnp.max(top, axis=0, keepdims=True)
            base_top[g, s : s + 1, :] = top
            for b in blocks:
                refs[b] = jnp.where(flags[b][r : r + 1], top, refs[b])
            part = slice(s * span, (s + 1) * span)
            probs[part, :] = jnp.exp(near_s[g, part, :] - top).astype(bf16)
        for b in blocks:
            block = jnp.exp(far_s[g, b * span : (b + 1) * span, :] - refs[b]).astype(bf16)
            start = near_keys + (b - PLANE) * span
            probs[start : start + span, :] = block
        known = n * span
        base_sum[g] = dot(vals[g, :, :known], probs[...])

    def far_part(g):
        refs = [jnp.full((1, across_q), 1e30, f32) for _ in range(PLANE)]
        flags = [flag_of(b) for b in range(PLANE)]
        scales = []
        for s in range(seqs):
            r = 2 * s + g
            top = jnp.where(flags[0][r : r + 1], tops[g, 0], FAR)
            for b in range(1, PLANE):
                top = jnp.maximum(top, jnp.where(flags[b][r : r + 1], tops[g, b], FAR))
            before = base_top[g, s : s + 1, :]
            top = jnp.maximum(jnp.max(top, axis=0, keepdims=True), before)
            scales.append(jnp.exp(before - top))
            for b in range(PLANE):
                refs[b] = jnp.where(flags[b][r : r + 1], top, refs[b])
        w = jnp.concatenate(
            [
                jnp.exp(far_s[g, b * span : (b + 1) * span, :] - refs[b]).astype(bf16)
                for b in range(PLANE)
            ],
            axis=0,
        )
        sums = dot(vals[g, stack:, n * span :], w)
        for p in range(pairs):
            tiles = []
            made = dot(vals[g, p * 128 : (p + 1) * 128, n * span :], w)
            for s in (2 * p, 2 * p + 1):
                row = (2 + g) * seqs + s
                line = slice(stack + s, stack + s + 1)
                total = base_sum[g, line, :] * scales[s] + sums[s : s + 1]
                total = jnp.maximum(total, 1.0)
                factor = gate_buf[row : row + 1, :] / total
                block = slice(s * HEAD_DIM, (s + 1) * HEAD_DIM)
                old = base_sum[g, block, :] * (scales[s] * factor)
                fresh = made[(s % 2) * HEAD_DIM : (s % 2 + 1) * HEAD_DIM]
                tiles.append(mix[g, block, :] + old + fresh * factor)
            both = jnp.concatenate(tiles, axis=0)
            for j in range(half // 2):
                lanes = slice(j * 128, (j + 1) * 128)
                flipped = jnp.transpose(both[:, lanes])
                a, b = flipped[:span], flipped[span:]
                part = slice(2 * p * span, (2 * p + 1) * span)
                own[g, part, lanes] = jnp.where(low, a, swap(b)).astype(bf16)
                part = slice((2 * p + 1) * span, (2 * p + 2) * span)
                own[g, part, lanes] = jnp.where(low, swap(a), b).astype(bf16)
            for s in (2 * p, 2 * p + 1):
                piece(g, s).start()

    def piece(g, s):
        part = pl.ds(s * span, span)
        return pltpu.make_async_remote_copy(
            src_ref=own.at[g, part], dst_ref=other.at[g, part], send_sem=half_send.at[0],
            recv_sem=half_recv.at[g * (s + 1)], device_id={"tp": 1 - column}, device_id_type=mesh_id,
        )

    spread = 2 * wg_ref.shape[1]
    logits = dot_t(wg[...].reshape(spread, rows.shape[1]), hidden)
    wide_at = lax.broadcasted_iota(jnp.int32, (1, seqs * span), 1)
    limit = jnp.zeros((1, seqs * span), jnp.int32)
    for s in range(seqs):
        limit = jnp.where(wide_at // span == s, lens[:, s : s + 1], limit)
    live = me * span + wide_at % span < limit
    for branch in range(2):
        base = branch * (spread // 2)
        mine = jnp.where(
            column == 0, logits[base : base + heads], logits[base + heads : base + 2 * heads]
        )
        mine = jnp.where(live, jax.nn.sigmoid(mine), 0.0)
        turned = [mine[:, p * 128 : (p + 1) * 128] for p in range(pairs)]
        swapped = [swap(t) for t in turned]
        for g in range(2):
            for s in range(seqs):
                for j in range(half // 2):
                    one = slice(g * half + 2 * j, g * half + 2 * j + 1)
                    two = slice(g * half + 2 * j + 1, g * half + 2 * j + 2)
                    t, w = turned[s // 2], swapped[s // 2]
                    if s % 2 == 0:
                        row = jnp.where(low_row, t[one], w[two])
                    else:
                        row = jnp.where(low_row, w[one], t[two])
                    line = (branch * 2 + g) * seqs + s
                    gate_buf[line : line + 1, j * 128 : (j + 1) * 128] = row

    for g in range(2):
        near_part(g)
    last = planes - 1
    in_side(0, last - 1)
    in_cross(0, last)
    entries_direct()
    plane_in(0, last)
    for plane in range(last - 2, 0, -1):
        in_side(0, plane)
        in_cross(0, plane + 1)
    in_cross(0, 1)
    export(1)
    entries_beside()
    cmp_part(0)
    for plane in range(last - 1, 1, -1):
        plane_in(0, plane)
    in_side(0, 0)
    in_cross(0, 0)
    plane_in(0, 1)
    far_base(0)
    plane_in(0, 0)
    far_part(0)
    for plane in range(last - 1, 0, -1):
        in_side(1, plane)
    in_cross(1, last)
    for plane in range(last - 1, 0, -1):
        in_cross(1, plane)
    in_side(1, 0)
    in_cross(1, 0)
    pltpu.make_async_copy(weight, weight, load_sem.at[11]).wait()
    cmp_part(1)
    for plane in range(last, 0, -1):
        plane_in(1, plane)
    far_base(1)
    plane_in(1, 0)
    far_part(1)

    squares = jnp.zeros((seqs * span, 1), f32)
    total = jnp.zeros((seqs * span, wide), f32)
    group = half * HEAD_DIM

    def gains(side, g):
        return gain[:, pl.ds(pl.multiple_of(side * depth + g * group, group), group)]

    for g in range(2):
        a = own[g].astype(f32)
        squares = squares + jnp.sum(a * a, axis=1, keepdims=True)
        scaled = (a * gains(column, g)).astype(bf16)
        total = total + dot(scaled, weight[0, g * group : (g + 1) * group, :])
    def all_pieces(ref):
        return pltpu.make_async_remote_copy(
            src_ref=ref, dst_ref=ref, send_sem=half_send.at[0], recv_sem=half_recv.at[0],
            device_id={"tp": 1 - column}, device_id_type=mesh_id,
        )

    for b in range(1, n):
        pl.when(me == b)(lambda b=b: lists_copy(b).wait_send())
    everyone = pl.ds(0, 2 * planes + 1)
    entries_copy(2 * planes + 1, 0).wait_send()
    pltpu.make_async_remote_copy(
        src_ref=blobs.at[:, everyone], dst_ref=blobs.at[:, everyone], send_sem=blob_send.at[0],
        recv_sem=blob_recv.at[0, 0, 0], device_id={"kv": (me + 1) % n}, device_id_type=mesh_id,
    ).wait_send()
    all_pieces(other.at[0]).wait_recv()
    a = other[0].astype(f32)
    squares = squares + jnp.sum(a * a, axis=1, keepdims=True)
    scaled = (a * gains(1 - column, 0)).astype(bf16)
    partial[...] = total + dot(scaled, weight[1, :group, :])
    for s in range(seqs):
        piece(1, s).wait_recv()
        part = slice(s * span, (s + 1) * span)
        a = other[1, part, :].astype(f32)
        square = squares[part] + jnp.sum(a * a, axis=1, keepdims=True)
        row_scale = lax.rsqrt(square / (2 * depth) + norm_eps)
        scaled = (a * gains(1 - column, 1)).astype(bf16)
        done = partial[part, :] + dot(scaled, weight[1, group:, :])
        out_ref[part, :] = (done * row_scale).astype(bf16)

    all_pieces(own).wait_send()


def fused_shards(
    hidden_in,
    w_query,
    w_cmp_key,
    w_cmp_value,
    w_sel_key,
    w_sel_value,
    w_gate,
    cmp_key_in,
    cmp_key_out,
    cmp_value_in,
    cmp_value_out,
    out_gain,
    w_out,
    seq_lengths,
    chosen,
):
    seqs, span, width = hidden_in.shape
    n = lax.axis_size("kv")
    heads = w_query.shape[1] // HEAD_DIM
    total = seqs * span
    entries = total // CMP_STRIDE
    out_width = width // lax.axis_size("tp")
    small = w_sel_key.shape[1]
    half = heads // 2
    stack = seqs * HEAD_DIM
    across_q = half * span
    planes = n // PLANE
    anywhere = pl.BlockSpec(memory_space=pl.ANY)
    gate_rows = jnp.transpose(w_gate, (1, 2, 0))
    picks = chosen[:, 0].reshape(2 * seqs, TOPK)
    key_out, value_out = jnp.transpose(cmp_key_out), jnp.transpose(cmp_value_out)
    lens = seq_lengths[None]
    gain = out_gain[None]
    out = pl.pallas_call(
        functools.partial(layer_kernel, n, seqs, span, heads),
        in_specs=[anywhere] * 15,
        out_specs=pl.BlockSpec(memory_space=pltpu.VMEM),
        out_shape=pltpu.VMEM((total, out_width), bf16),
        scratch_shapes=[
            pltpu.VMEM(picks.shape, jnp.int32),
            pltpu.VMEM((total, width), bf16),
            pltpu.VMEM((width, 4 * small), bf16),
            pltpu.VMEM(key_out.shape, bf16),
            pltpu.VMEM(value_out.shape, bf16),
            pltpu.VMEM(cmp_key_in.shape, bf16),
            pltpu.VMEM(cmp_value_in.shape, bf16),
            pltpu.VMEM(w_query.shape, bf16),
            pltpu.VMEM(gate_rows.shape, bf16),
            pltpu.VMEM(lens.shape, jnp.int32),
            pltpu.VMEM(gain.shape, f32),
            pltpu.VMEM((2, heads * HEAD_DIM, out_width), bf16),
            pltpu.VMEM((2, across_q, stack), bf16),
            pltpu.VMEM((total, small), bf16),
            pltpu.VMEM((small, total), bf16),
            pltpu.VMEM((2, total, small), f32),
            pltpu.VMEM((4 * seqs, across_q), f32),
            pltpu.VMEM((n, 2 * seqs, 128), f32),
            pltpu.VMEM((n,) + picks.shape, jnp.int32),
            pltpu.VMEM((n, 2 * entries, 128), bf16),
            pltpu.VMEM((2, n, span, 128), bf16),
            pltpu.VMEM((2, total, across_q), f32),
            pltpu.VMEM((2, n * span, across_q), f32),
            pltpu.VMEM((2, n + seqs, 8, across_q), f32),
            pltpu.VMEM((2, 8, across_q), f32),
            pltpu.VMEM((n * span, across_q), bf16),
            pltpu.VMEM((2, stack + 16, across_q), f32),
            pltpu.VMEM((2, stack + 16, total + n * span), bf16),
            pltpu.VMEM((2, stack, across_q), f32),
            pltpu.VMEM((2, total, half * HEAD_DIM), bf16),
            pltpu.VMEM((2, total, half * HEAD_DIM), bf16),
            pltpu.VMEM((total, out_width), f32),
            pltpu.SemaphoreType.DMA((12,)),
            pltpu.SemaphoreType.DMA((1,)),
            pltpu.SemaphoreType.DMA((1,)),
            pltpu.SemaphoreType.DMA((1,)),
            pltpu.SemaphoreType.DMA((2,)),
            pltpu.SemaphoreType.DMA((1,)),
            pltpu.SemaphoreType.DMA((2, planes, 3)),
            pltpu.SemaphoreType.DMA((1,)),
            pltpu.SemaphoreType.DMA((1 + seqs,)),
        ],
        compiler_params=pltpu.CompilerParams(
            collective_id=0, has_side_effects=True, vmem_limit_bytes=VMEM_BYTES
        ),
        name="layer",
    )(
        picks, hidden_in.reshape(total, width), w_sel_key, w_sel_value, w_cmp_key, w_cmp_value,
        key_out, value_out, cmp_key_in, cmp_value_in, w_query, gate_rows, lens, gain, w_out,
    )
    return out.reshape(seqs, span, out_width)


def fits(mesh):
    n = mesh.shape["kv"]
    return mesh.shape["tp"] == 2 and n % PLANE == 0 and 3 * PLANE <= n <= 32


def solution(mesh):
    placed = (
        P(None, "kv", None),
        P(None, "tp"),
        P(None, "tp"),
        P(None, "tp"),
        P(None, "tp"),
        P(None, "tp"),
        P(),
        P(),
        P(),
        P(),
        P(),
        P(),
        P(),
        P(),
        P(None, "kv", "tp", None),
    )
    return jax.shard_map(
        fused_shards if fits(mesh) else shards, mesh=mesh, in_specs=placed, out_specs=P(None, "kv", "tp"), check_vma=False
    )
```
